32 devices in a mesh: sp: 8 (over z, y), tp: 4 (over x, core).
Axes of the slice: x: 2, y: 2, z: 4, core: 2. Of those that a mesh axis runs over, the one named last changes fastest.
Arguments:
- grad_out: bfloat16 [2048, 2048], P('sp'), may hold values from -6 to 6
- resid: bfloat16 [2048, 2048], P('sp'), may hold values from -6 to 6
- norm_gain: float32 [2048], replicated, may hold values from 0.1 to 1.9
- routes: int32 [2048, 2], P('sp'), may hold values from 0 to 7, all different within a row; in each aligned block of 256 rows (0 to 255, 256 to 511, ...) at most 96 rows name the same one
- route_weights: float32 [2048, 2], P('sp'), may hold values from 0.05 to 1
- gate_weight: bfloat16 [8, 2048, 1536], P('sp', None, 'tp'), may hold values from -0.375 to 0.375
- up_weight: bfloat16 [8, 2048, 1536], P('sp', None, 'tp'), may hold values from -0.375 to 0.375
- down_weight: bfloat16 [8, 1536, 2048], P('sp', 'tp'), may hold values from -0.15625 to 0.15625
- proj_weight: bfloat16 [2048, 512], P(None, 'tp'), may hold values from -0.25 to 0.25
- conv_sum: bfloat16 [2048, 512], P('sp', 'tp'), may hold values from -6 to 6
- conv_gain: float32 [512], P('tp'), may hold values from 0.1 to 1.9
- conv_taps: float32 [31, 512], P(None, 'tp'), may hold values from -1 to 1
- conv_value: bfloat16 [2048, 512], P('sp', 'tp'), may hold values from -6 to 6
- conv_gate: bfloat16 [2048, 512], P('sp', 'tp'), may hold values from -6 to 6
Outputs:
- gate_weight_grad: bfloat16 [8, 2048, 1536], P('sp', None, 'tp')
- up_weight_grad: bfloat16 [8, 2048, 1536], P('sp', None, 'tp')
- down_weight_grad: bfloat16 [8, 1536, 2048], P('sp', 'tp')
- proj_grad: float32 [2048, 512], P('sp', 'tp')
- value_grad: bfloat16 [2048, 512], P('sp', 'tp')
- gate_input_grad: bfloat16 [2048, 512], P('sp', 'tp')
The draws below stay inside these ranges and needn't reach their ends.
Inputs may be any that keep to these rules, and one draw needn't show every extreme that they name: In each aligned block of 256 tokens no expert is named by more than 96 routes, and in some block one expert is named exactly 96 times; a token's two routes name different experts.
All inputs are finite; a program needn't handle non-finite values.
Results may differ from the reference program's by a relative error of at most 0.028.
Values may be sent and summed in bfloat16 or wider, within the bound.
A program may use at most 128 MiB of HBM per device.

```python
import math
import jax
import jax.numpy as jnp
import numpy as np
from jax import lax

D = 2048
F = 1536
CH = 512
CONV_K = 31
TOK_DEV = 256
GROUP = 128
EXPERTS = 8
CAP = 96
TOKENS = 2048
N_SP = 8
N_TP = 4


def raised(result, rng, source, target, blocks, factor):
    owner, partner = [(jnp.arange(result.shape[axis_at]) // (result.shape[axis_at] // blocks)).reshape([-1 if axis == axis_at else 1 for axis in range(result.ndim)]) for axis_at in (source, target)]
    chosen = jax.random.permutation(rng, blocks)[partner]
    strong = (owner == chosen) | (owner == (partner + blocks // 2) % blocks)
    return jnp.where(strong, factor * result, result)


def block_levels(key, extent, pieces, smallest, high):
    loudness = 1.0
    for dim, parts in pieces:
        heights = jax.random.uniform(jax.random.fold_in(jax.random.fold_in(key, 6), dim), (parts,), jnp.float32, smallest / len(pieces), high / len(pieces))
        loudness = loudness * jnp.repeat(jnp.exp(heights), extent[dim] // parts).reshape((-1,) + (1,) * (len(extent) - 1 - dim))
    return loudness


def deal_out(own_key, own, number, rows, number_of, top, reach, skew):
    order = jax.random.permutation(own_key, number_of)
    crowded, ordinary = shares(number_of, rows * top, reach, skew, True), shares(number_of, rows * top, reach, skew, False)
    places = jnp.arange(number_of)

    def named(lengths, rotation):
        used = int((lengths > 0).sum())
        fixed = max(1, used // 4)
        passed = fixed + (places - fixed + rotation * (used - fixed)) % max(1, number_of - fixed)
        return jnp.zeros((number_of,), jnp.int32).at[order[jnp.where(places < fixed, places, passed)]].set(jnp.asarray(lengths, jnp.int32))

    lengths = jnp.where(number % 4 == 0, named(crowded, number // 4), named(ordinary, number - number // 4 - 1))
    mixed = jax.random.permutation(jax.random.fold_in(own, 3), number_of)
    giver, receiver = mixed[0:number_of // 2 * 2:2], mixed[1:number_of // 2 * 2:2]
    room = jnp.minimum(lengths[giver] - 1, reach - lengths[receiver]) // 2
    room = jnp.where((giver == order[0]) | (receiver == order[0]) | (lengths[receiver] == 0), 0, jnp.maximum(room, 0))
    passed = jax.random.randint(jax.random.fold_in(own, 4), (number_of // 2,), 0, 1 << 20) % (room + 1)
    lengths = lengths.at[giver].add(-passed).at[receiver].add(passed)
    items = jnp.searchsorted(jnp.cumsum(lengths), jnp.arange(rows * top), side="right").astype(jnp.int32)
    grid = items.reshape(top, rows).T
    grid = grid[jax.random.permutation(jax.random.fold_in(own, 1), rows)]
    rotation = jax.random.randint(jax.random.fold_in(own, 2), (rows, 1), 0, top)
    return jnp.take_along_axis(grid, (jnp.arange(top)[None, :] + rotation) % top, axis=1)


def shares(amount, total, limit, lean, full):
    portions = [(1 << 20) // math.isqrt(standing ** lean) + 1 for standing in range(1, amount + 1)]
    largest = limit if full else min(limit, max(-(-total // amount), total * portions[0] // sum(portions)))
    least = 1 if total - largest >= amount - 1 else 0
    holding, spare = [largest] + [least] * (amount - 1), total - largest - least * (amount - 1)
    while spare > 0:
        candidates = [i for i in range(1, amount) if holding[i] < largest] or [i for i in range(1, amount) if holding[i] < limit]
        pool, remaining = sum([portions[i] for i in candidates]), spare
        for i in candidates:
            addition = min(limit - holding[i], max(1, remaining * portions[i] // pool), spare)
            holding[i] = holding[i] + addition
            spare = spare - addition
    return np.array(holding)


def gaussian(key, extent, deviation, bound, shards=(), held_as=jnp.bfloat16):
    values = deviation * jax.random.normal(key, extent, jnp.float32)
    if shards:
        values = values * block_levels(key, extent, shards, -0.22, 0.18)
    return jnp.clip(values, -bound, bound).astype(held_as)


def noise_with(rng, dims, deviation, limit, split, heavy, kind=jnp.bfloat16):
    drawn = deviation * jax.random.normal(rng, dims, jnp.float32)
    if split:
        drawn = drawn * block_levels(rng, dims, split, -0.22, 0.18)
    return jnp.clip(raised(drawn, jax.random.fold_in(rng, 3), *heavy), -limit, limit).astype(kind)


def setup_inputs(seed: int = 0) -> dict:
    streams_of = jax.random.split(jax.random.key(seed), 15)
    grad_out = noise_with(streams_of[0], (TOKENS, D), 1.0, 6.0, ((0, 8),), (0, 1, 8, 2.0))
    resid = gaussian(streams_of[1], (TOKENS, D), 1.0, 6.0, ((0, 8),))
    norm_gain = jnp.clip(1.0 + 0.18 * jax.random.normal(streams_of[2], (D,), jnp.float32), 0.1, 1.9)
    routes_keys = jax.random.split(jax.random.fold_in(streams_of[3], 1), TOKENS // TOK_DEV)
    routes_turns = jax.random.permutation(jax.random.fold_in(streams_of[3], 3), TOKENS // TOK_DEV)
    routes = jax.vmap(lambda own, number: deal_out(jax.random.fold_in(streams_of[3], 2), own, number, TOK_DEV, EXPERTS, 2, CAP, 1))(routes_keys, routes_turns).reshape((TOKENS, 2))
    route_weights = jnp.clip(0.05 + 0.95 * jax.random.uniform(streams_of[4], (TOKENS, 2), jnp.float32) ** block_levels(streams_of[4], (TOKENS, 2), ((0, 8),), -0.2, 0.2), 0.05, 1.0)
    gate_weight = gaussian(streams_of[5], (EXPERTS, D, F), (D // 9) ** -0.5, 0.375, ((0, 8), (2, 4)))
    up_weight = gaussian(streams_of[6], (EXPERTS, D, F), (D // 9) ** -0.5, 0.375, ((0, 8), (2, 4)))
    down_weight = gaussian(streams_of[7], (EXPERTS, F, D), F ** -0.5, 0.15625, ((0, 8), (1, 4)))
    proj_weight = gaussian(streams_of[8], (D, CH), CH ** -0.5, 0.25, ((1, 4),))
    conv_sum = gaussian(streams_of[9], (TOKENS, CH), 1.0, 6.0, ((0, 8), (1, 4)))
    conv_gain = jnp.clip(1.0 + 0.18 * jax.random.normal(streams_of[10], (CH,), jnp.float32), 0.1, 1.9)
    conv_taps = gaussian(streams_of[11], (CONV_K, CH), CONV_K ** -0.5, 1.0, ((1, 4),), jnp.float32)
    conv_value = gaussian(streams_of[12], (TOKENS, CH), 1.0, 6.0, ((0, 8), (1, 4)))
    conv_gate = gaussian(streams_of[13], (TOKENS, CH), 1.0, 6.0, ((0, 8), (1, 4)))
    return dict(grad_out=grad_out, resid=resid, norm_gain=norm_gain, routes=routes, route_weights=route_weights, gate_weight=gate_weight, up_weight=up_weight, down_weight=down_weight, proj_weight=proj_weight, conv_sum=conv_sum, conv_gain=conv_gain, conv_taps=conv_taps, conv_value=conv_value, conv_gate=conv_gate)


CLAMP_LIMIT = 7.0
SLOPE_ALPHA = 1.702

def contract_rows(left_side, right_side):
    return lax.dot_general(left_side, right_side, (((0,), (0,)), ((), ())), preferred_element_type=jnp.float32)

def contract_cols(left_side, right_side):
    return lax.dot_general(left_side, right_side, (((1,), (1,)), ((), ())), preferred_element_type=jnp.float32)

def expert_backward(routed_rows, routed_cots, w_gate, w_up, w_down):
    gate_pre = jnp.dot(routed_rows, w_gate, preferred_element_type=jnp.float32)
    up_pre = jnp.dot(routed_rows, w_up, preferred_element_type=jnp.float32)
    gate_clamped = jnp.minimum(gate_pre, CLAMP_LIMIT)
    up_clamped = jnp.clip(up_pre, -CLAMP_LIMIT, CLAMP_LIMIT)
    sigma = jax.nn.sigmoid(SLOPE_ALPHA * gate_clamped)
    gated = gate_clamped * sigma
    act = ((up_clamped + 1.0) * gated).astype(jnp.bfloat16)
    down_grad = contract_rows(act, routed_cots).astype(jnp.bfloat16)
    act_grad = contract_cols(routed_cots, w_down)
    inside = (up_pre > -CLAMP_LIMIT) & (up_pre < CLAMP_LIMIT)
    up_pre_grad = jnp.where(inside, act_grad * gated, 0.0).astype(jnp.bfloat16)
    slope = sigma + SLOPE_ALPHA * gate_clamped * sigma * (1.0 - sigma)
    gate_pre_grad = jnp.where(gate_pre < CLAMP_LIMIT, act_grad * (up_clamped + 1.0) * slope, 0.0).astype(jnp.bfloat16)
    gate_grad = contract_rows(routed_rows, gate_pre_grad).astype(jnp.bfloat16)
    up_grad = contract_rows(routed_rows, up_pre_grad).astype(jnp.bfloat16)
    partial_value = contract_cols(gate_pre_grad, w_gate) + contract_cols(up_pre_grad, w_up)
    return (gate_grad, up_grad, down_grad, partial_value)

def reference(grad_out, resid, norm_gain, routes, route_weights, gate_weight, up_weight, down_weight, proj_weight, conv_sum, conv_gain, conv_taps, conv_value, conv_gate):
    resid_f = resid.astype(jnp.float32)
    inv_rms = lax.rsqrt(lax.optimization_barrier(jnp.mean(resid_f * resid_f, axis=-1, keepdims=True)) + 1e-06)
    normed = (resid_f * inv_rms * norm_gain).astype(jnp.bfloat16)
    scaled = (route_weights[:, :, None] * grad_out.astype(jnp.float32)[:, None, :]).astype(jnp.bfloat16)
    scaled = scaled.reshape(2 * TOKENS, D)
    route_ids = routes.reshape(N_SP, 2 * TOK_DEV)
    one_hot = (route_ids[:, :, None] == jnp.arange(EXPERTS, dtype=jnp.int32)[None, None, :]).astype(jnp.int32)
    slot_rank = lax.optimization_barrier(jnp.sum(jnp.cumsum(one_hot, axis=1) * one_hot, axis=2)) - 1
    slot_index = route_ids * (N_SP * CAP) + jnp.arange(N_SP, dtype=jnp.int32)[:, None] * CAP + slot_rank
    slot_table = jnp.full((EXPERTS * N_SP * CAP,), 2 * TOKENS, jnp.int32)
    slot_table = slot_table.at[slot_index.reshape(-1)].set(jnp.arange(2 * TOKENS, dtype=jnp.int32))
    slot_table = slot_table.reshape(EXPERTS, N_SP * CAP)
    normed_pad = jnp.concatenate([normed, jnp.zeros((1, D), jnp.bfloat16)], axis=0)
    scaled_pad = jnp.concatenate([scaled, jnp.zeros((1, D), jnp.bfloat16)], axis=0)
    block_width = F // N_TP

    def one_expert(route_store, inputs):
        table_row, w_gate, w_up, w_down = inputs
        routed_rows = normed_pad[table_row // 2]
        routed_cots = scaled_pad[table_row]
        gate_parts, up_parts, down_parts = ([], [], [])
        row_total = jnp.zeros((N_SP * CAP, D), jnp.float32)
        for block_number in range(N_TP):
            first_col = block_number * block_width
            gate_grad, up_grad, down_grad, partial_value = expert_backward(routed_rows, routed_cots, w_gate[:, first_col:first_col + block_width], w_up[:, first_col:first_col + block_width], w_down[first_col:first_col + block_width, :])
            gate_parts.append(gate_grad)
            up_parts.append(up_grad)
            down_parts.append(down_grad)
            rounded = lax.optimization_barrier(partial_value.astype(jnp.bfloat16))
            row_total = row_total + rounded.astype(jnp.float32)
        route_store = route_store.at[table_row].set(row_total.astype(jnp.bfloat16))
        return (route_store, (jnp.concatenate(gate_parts, axis=1), jnp.concatenate(up_parts, axis=1), jnp.concatenate(down_parts, axis=0)))
    route_store = jnp.zeros((2 * TOKENS + 1, D), jnp.bfloat16)
    route_store, (gate_weight_grad, up_weight_grad, down_weight_grad) = lax.scan(one_expert, route_store, (slot_table, gate_weight, up_weight, down_weight))
    normed_grad = route_store[:2 * TOKENS].astype(jnp.float32).reshape(TOKENS, 2, D).sum(axis=1).astype(jnp.bfloat16)
    feature_grad = normed_grad.astype(jnp.float32) * norm_gain
    cubed = inv_rms * inv_rms * inv_rms
    resid_grad = (grad_out.astype(jnp.float32) + inv_rms * feature_grad - resid_f * cubed * lax.optimization_barrier(jnp.mean(resid_f * feature_grad, axis=-1, keepdims=True))).astype(jnp.bfloat16)
    summed = conv_sum.astype(jnp.float32).reshape(TOKENS, CH // GROUP, GROUP)
    centre = summed - lax.optimization_barrier(jnp.mean(summed, axis=-1, keepdims=True))
    inv_std = lax.rsqrt(lax.optimization_barrier(jnp.mean(centre * centre, axis=-1, keepdims=True)) + 1e-05)
    grouped = centre * inv_std
    chan_normed = grouped.reshape(TOKENS, CH)
    pre_act = chan_normed * conv_gain
    sigma_conv = jax.nn.sigmoid(pre_act)
    conv_out = (pre_act * sigma_conv).astype(jnp.bfloat16)
    proj_grad = contract_rows(resid_grad, conv_out)
    out_grad = jnp.dot(resid_grad, proj_weight, preferred_element_type=jnp.float32)
    normal_grad = (out_grad * sigma_conv * (1.0 + pre_act * (1.0 - sigma_conv)) * conv_gain).reshape(TOKENS, CH // GROUP, GROUP)
    sum_grad = inv_std * (normal_grad - lax.optimization_barrier(jnp.mean(normal_grad, axis=-1, keepdims=True)) - grouped * lax.optimization_barrier(jnp.mean(normal_grad * grouped, axis=-1, keepdims=True)))
    sum_grad = sum_grad.reshape(TOKENS, CH)
    extended = jnp.concatenate([sum_grad, jnp.zeros((CONV_K - 1, CH), jnp.float32)], axis=0)
    gated_grad = lax.conv_general_dilated(extended[None], conv_taps[::-1][:, None, :], (1,), ((0, 0),), dimension_numbers=('NWC', 'WIO', 'NWC'), feature_group_count=CH, precision=lax.Precision.HIGHEST)[0]
    sigma_gate = jax.nn.sigmoid(conv_gate.astype(jnp.float32))
    value_grad = (gated_grad * sigma_gate).astype(jnp.bfloat16)
    gate_input_grad = (gated_grad * conv_value.astype(jnp.float32) * sigma_gate * (1.0 - sigma_gate)).astype(jnp.bfloat16)
    return (gate_weight_grad, up_weight_grad, down_weight_grad, proj_grad, value_grad, gate_input_grad)
```

```python
import functools

import jax
import jax.numpy as jnp
from jax import lax
from jax.experimental import pallas as pl
from jax.experimental.pallas import tpu as pltpu
from jax.sharding import PartitionSpec as P

CONV_K = 31
GROUP = 128
MESH = pl.DeviceIdType.MESH


CLAMP_LIMIT = 7.0
SLOPE_ALPHA = 1.702


def passed_along(block, axis, distance):
    devices = range(lax.axis_size(axis))
    route = [(i - distance, i) for i in devices if i - distance in devices]
    return lax.ppermute(block, axis, route)


def tp_places():
    mine = lax.axis_index("tp")
    near = mine + 1 - 2 * (mine % 2)
    far = (mine + 2) % 4
    diag = (near + 2) % 4
    return mine, near, far, diag


def meet(steps, over_sp, near, far):
    s, t = lax.axis_index("sp"), lax.axis_index("tp")
    barrier = pltpu.get_barrier_semaphore()
    pl.semaphore_signal(barrier, inc=1, device_id=(s, near), device_id_type=MESH)
    pl.semaphore_signal(barrier, inc=1, device_id=(s, far), device_id_type=MESH)
    total = 2
    if over_sp:

        def greet(d, carry):
            pl.semaphore_signal(
                barrier, inc=1, device_id=((s + d) % steps, t), device_id_type=MESH
            )
            return carry

        lax.fori_loop(1, steps, greet, 0)
        total += steps - 1
    pl.semaphore_wait(barrier, total)


def crossing_first(steps, k):
    return steps // 2 + ((k + 1) // 2) * (2 * (k % 2) - 1)


def looped(first, last, body):
    def step(k, carry):
        body(k)
        return carry

    lax.fori_loop(first, last, step, 0)


def spread_kernel(count, steps, over_sp, in_lanes, absolute, beside, sp_count, *refs):
    refs = list(refs)
    sends, refs = refs[:count], refs[count:]
    fulls, refs = (refs[:count], refs[count:]) if over_sp else (None, refs)
    side, refs = (refs[0], refs[1:]) if beside else (None, refs)
    outs, refs = refs[:count], refs[count:]
    side_out, refs = (refs[0], refs[1:]) if beside else (None, refs)
    own_sem, a_send, a_recv, b_send, f_send, c_send, near_recv, fwd_recv, far_recv = refs[:9]
    s = lax.axis_index("sp")
    t, near, far, _ = tp_places()
    width = sends[0].shape[-1]

    def place(c, d, q):
        if in_lanes:
            return outs[c].at[d, :, pl.ds(pl.multiple_of(q * width, width), width)]
        return outs[c].at[d, q]

    def source(c, d):
        return sends[c].at[(s + d) % steps if absolute else d]

    def own(c, d):
        if over_sp:
            return pltpu.make_async_copy(fulls[c], outs[c].at[0], own_sem.at[c, 0])
        return pltpu.make_async_copy(source(c, d), place(c, d, t), own_sem.at[c, d])

    def to_sp(c, d):
        return pltpu.make_async_remote_copy(
            src_ref=source(c, d),
            dst_ref=place(c, d, t),
            send_sem=a_send.at[c, d],
            recv_sem=a_recv.at[c, d],
            device_id=((s + d) % steps, t),
            device_id_type=MESH,
        )

    def to_tp(c, d, q, target, send_sem, recv_sem):
        return pltpu.make_async_remote_copy(
            src_ref=place(c, d, q),
            dst_ref=place(c, d, q),
            send_sem=send_sem.at[c, d],
            recv_sem=recv_sem.at[c, d],
            device_id=(s, target),
            device_id_type=MESH,
        )

    def near_copy(c, d):
        return to_tp(c, d, t, near, b_send, near_recv)

    def far_copy(c, d):
        return to_tp(c, d, t, far, f_send, far_recv)

    def fwd_copy(c, d):
        return to_tp(c, d, far, near, c_send, fwd_recv)

    def side_copy(d):
        side_send, side_recv = refs[10:12]
        return pltpu.make_async_remote_copy(
            src_ref=side,
            dst_ref=side_out.at[d],
            send_sem=side_send.at[d],
            recv_sem=side_recv.at[d],
            device_id=((s + d) % sp_count, t),
            device_id_type=MESH,
        )

    def own_side():
        return pltpu.make_async_copy(side, side_out.at[0], refs[9].at[0])

    def share(c, d):
        far_copy(c, d).start()
        near_copy(c, d).start()

    def forward(c, d):
        far_copy(c, d).wait_recv()
        fwd_copy(c, d).start()

    def finish(c, d):
        near_copy(c, d).wait()
        far_copy(c, d).wait_send()
        fwd_copy(c, d).wait()

    def loop(first, last, body):
        def each(k):
            d = k + 1 if over_sp else k
            for c in range(count):
                body(c, d)

        looped(first, last, each)

    meet(sp_count, over_sp or beside, near, far)
    if over_sp:
        loop(0, steps - 1, lambda c, d: to_sp(c, d).start())
        for c in range(count):
            own(c, 0).start()

        def pass_on(k):
            for c in range(count):
                d = k + 1
                to_sp(c, d).wait_recv()
                share(c, d)

        def pass_on_twice(k):
            pass_on(k)
            for c in range(count):
                forward(c, k)

        pass_on(0)
        looped(1, steps - 1, pass_on_twice)
        loop(steps - 2, steps - 1, forward)
        loop(0, steps - 1, finish)
        loop(0, steps - 1, lambda c, d: to_sp(c, d).wait_send())
        for c in range(count):
            own(c, 0).wait()
    else:
        loop(0, steps, lambda c, d: own(c, d).start())
        if beside:
            looped(0, sp_count - 1, lambda k: side_copy(crossing_first(sp_count, k)).start())
            own_side().start()

        def share_own(c, d):
            own(c, d).wait()
            share(c, d)

        loop(0, steps, share_own)
        loop(0, steps, forward)
        loop(0, steps, finish)
        if beside:
            looped(0, sp_count - 1, lambda k: side_copy(crossing_first(sp_count, k)).wait())
            own_side().wait()


def spread(sends, fulls, side, in_lanes, absolute, collective_id):
    count = len(sends)
    steps, rows, width = sends[0].shape
    tp_count, sp_count = lax.axis_size("tp"), lax.axis_size("sp")
    over_sp, beside = fulls is not None, side is not None
    shape = (steps, rows, tp_count * width) if in_lanes else (steps, tp_count, rows, width)
    out_shape = [jax.ShapeDtypeStruct(shape, x.dtype) for x in sends]
    operands = list(sends) + (list(fulls) if over_sp else []) + ([side] if beside else [])
    scratch = [pltpu.SemaphoreType.DMA((count, steps))] * 9
    if beside:
        out_shape.append(jax.ShapeDtypeStruct((sp_count,) + side.shape, side.dtype))
        scratch += [pltpu.SemaphoreType.DMA((1,))] + [pltpu.SemaphoreType.DMA((sp_count,))] * 2
    return pl.pallas_call(
        functools.partial(
            spread_kernel, count, steps, over_sp, in_lanes, absolute, beside, sp_count
        ),
        out_shape=tuple(out_shape),
        in_specs=[pl.BlockSpec(memory_space=pltpu.VMEM)] * len(operands),
        out_specs=tuple(pl.BlockSpec(memory_space=pltpu.VMEM) for _ in out_shape),
        scratch_shapes=scratch,
        compiler_params=pltpu.CompilerParams(
            collective_id=collective_id, has_side_effects=True, vmem_limit_bytes=40 << 20
        ),
    )(*operands)


def combine_kernel(
    steps, part, out, near_in, pair, far_in, total,
    n0_send, n0_recv, n1_send, n1_recv, f_send, f_recv, a_send, a_recv,
):
    s = lax.axis_index("sp")
    t, near, far, diag = tp_places()
    width = out.shape[-1]

    def lanes(q):
        return pl.ds(pl.multiple_of(q * width, width), width)

    def near_copy(d, which, q, send_sem, recv_sem):
        return pltpu.make_async_remote_copy(
            src_ref=part.at[d, :, lanes(q)],
            dst_ref=near_in.at[which, d],
            send_sem=send_sem.at[d],
            recv_sem=recv_sem.at[d],
            device_id=(s, near),
            device_id_type=MESH,
        )

    def for_near(d):
        return near_copy(d, 0, near, n0_send, n0_recv)

    def for_diag(d):
        return near_copy(d, 1, diag, n1_send, n1_recv)

    def far_copy(d):
        return pltpu.make_async_remote_copy(
            src_ref=pair.at[d],
            dst_ref=far_in.at[d],
            send_sem=f_send.at[d],
            recv_sem=f_recv.at[d],
            device_id=(s, far),
            device_id_type=MESH,
        )

    def back(d):
        return pltpu.make_async_remote_copy(
            src_ref=total.at[d],
            dst_ref=out.at[d],
            send_sem=a_send.at[d],
            recv_sem=a_recv.at[d],
            device_id=((s + steps - d) % steps, t),
            device_id_type=MESH,
        )

    meet(steps, True, near, far)

    def open_up(d):
        for_diag(d).start()
        for_near(d).start()

    def add_pair(d):
        for_diag(d).wait_recv()
        mine = part[d, :, lanes(far)].astype(jnp.float32)
        pair[d] = (mine + near_in[1, d].astype(jnp.float32)).astype(pair.dtype)
        far_copy(d).start()

    def whole(d):
        for_near(d).wait_recv()
        far_copy(d).wait_recv()
        mine = part[d, :, lanes(t)].astype(jnp.float32)
        both = mine + near_in[0, d].astype(jnp.float32)
        return (both + far_in[d].astype(jnp.float32)).astype(out.dtype)

    def send_back(d):
        total[d] = whole(d)
        back(d).start()

    def at(k):
        return crossing_first(steps, k)

    lag = min(3, steps - 1)
    looped(0, steps - 1, lambda k: open_up(at(k)))
    open_up(0)
    looped(0, lag, lambda k: add_pair(at(k)))

    def middle(k):
        add_pair(at(k))
        send_back(at(k - lag))

    looped(lag, steps - 1, middle)
    add_pair(0)
    looped(steps - 1 - lag, steps - 1, lambda k: send_back(at(k)))
    out[0] = whole(0)

    def finish(d):
        for_near(d).wait_send()
        for_diag(d).wait_send()
        far_copy(d).wait_send()

    looped(0, steps, finish)
    looped(1, steps, lambda d: back(d).wait())


def combine(part, collective_id):
    steps, rows, all_width = part.shape
    width = all_width // lax.axis_size("tp")
    block = (steps, rows, width)
    return pl.pallas_call(
        functools.partial(combine_kernel, steps),
        out_shape=jax.ShapeDtypeStruct(block, part.dtype),
        in_specs=[pl.BlockSpec(memory_space=pltpu.VMEM)],
        out_specs=pl.BlockSpec(memory_space=pltpu.VMEM),
        scratch_shapes=[
            pltpu.VMEM((2,) + block, part.dtype),
            pltpu.VMEM(block, part.dtype),
            pltpu.VMEM(block, part.dtype),
            pltpu.VMEM(block, part.dtype),
        ]
        + [pltpu.SemaphoreType.DMA((steps,))] * 8,
        compiler_params=pltpu.CompilerParams(
            collective_id=collective_id, has_side_effects=True, vmem_limit_bytes=40 << 20
        ),
    )(part)


def contract_rows(left_side, right_side):
    return lax.dot_general(
        left_side, right_side, (((0,), (0,)), ((), ())), preferred_element_type=jnp.float32
    )


def contract_cols(left_side, right_side):
    return lax.dot_general(
        left_side, right_side, (((1,), (1,)), ((), ())), preferred_element_type=jnp.float32
    )


def expert_backward(routed_rows, routed_cots, w_gate, w_up, w_down):
    gate_pre = jnp.dot(routed_rows, w_gate, preferred_element_type=jnp.float32)
    up_pre = jnp.dot(routed_rows, w_up, preferred_element_type=jnp.float32)
    gate_clamped = jnp.minimum(gate_pre, CLAMP_LIMIT)
    up_clamped = jnp.clip(up_pre, -CLAMP_LIMIT, CLAMP_LIMIT)
    sigma = jax.nn.sigmoid(SLOPE_ALPHA * gate_clamped)
    gated = gate_clamped * sigma
    act = ((up_clamped + 1.0) * gated).astype(jnp.bfloat16)
    down_grad = contract_rows(act, routed_cots).astype(jnp.bfloat16)
    act_grad = contract_cols(routed_cots, w_down)
    inside = (up_pre > -CLAMP_LIMIT) & (up_pre < CLAMP_LIMIT)
    up_pre_grad = jnp.where(inside, act_grad * gated, 0.0).astype(jnp.bfloat16)
    slope = sigma + SLOPE_ALPHA * gate_clamped * sigma * (1.0 - sigma)
    gate_pre_grad = jnp.where(
        gate_pre < CLAMP_LIMIT, act_grad * (up_clamped + 1.0) * slope, 0.0
    ).astype(jnp.bfloat16)
    gate_grad = contract_rows(routed_rows, gate_pre_grad).astype(jnp.bfloat16)
    up_grad = contract_rows(routed_rows, up_pre_grad).astype(jnp.bfloat16)
    partial_value = contract_cols(gate_pre_grad, w_gate) + contract_cols(up_pre_grad, w_up)
    return (gate_grad, up_grad, down_grad, partial_value)


def routed_kernel(
    steps, send_rows, send_cots, own_rows, own_cots, w_gate, w_up, w_down,
    gate_grad, up_grad, down_grad, out,
    rows, cots, act, gate_pg, up_pg, part, near_in, pair, far_in, total,
    own_sem, a_send, a_recv, b_send, f_send, c_send, near_recv, fwd_recv, far_recv,
    n0_send, n0_recv, n1_send, n1_recv, g_send, g_recv, r_send, r_recv,
):
    s = lax.axis_index("sp")
    t, near, far, diag = tp_places()
    sends, fulls, held = (send_rows, send_cots), (own_rows, own_cots), (rows, cots)
    width = send_rows.shape[-1]
    hidden = w_gate.shape[1]
    both = (0, 1)

    def lanes(q):
        return pl.ds(pl.multiple_of(q * width, width), width)

    def own(c):
        return pltpu.make_async_copy(fulls[c], held[c].at[0], own_sem.at[c])

    def to_sp(c, d):
        return pltpu.make_async_remote_copy(
            src_ref=sends[c].at[d],
            dst_ref=held[c].at[d, :, lanes(t)],
            send_sem=a_send.at[c, d],
            recv_sem=a_recv.at[c, d],
            device_id=((s + d) % steps, t),
            device_id_type=MESH,
        )

    def to_tp(c, d, q, target, send_sem, recv_sem):
        return pltpu.make_async_remote_copy(
            src_ref=held[c].at[d, :, lanes(q)],
            dst_ref=held[c].at[d, :, lanes(q)],
            send_sem=send_sem.at[c, d],
            recv_sem=recv_sem.at[c, d],
            device_id=(s, target),
            device_id_type=MESH,
        )

    def near_copy(c, d):
        return to_tp(c, d, t, near, b_send, near_recv)

    def far_copy(c, d):
        return to_tp(c, d, t, far, f_send, far_recv)

    def fwd_copy(c, d):
        return to_tp(c, d, far, near, c_send, fwd_recv)

    def part_copy(d, which, q, send_sem, recv_sem):
        return pltpu.make_async_remote_copy(
            src_ref=part.at[d, :, lanes(q)],
            dst_ref=near_in.at[which, d],
            send_sem=send_sem.at[d],
            recv_sem=recv_sem.at[d],
            device_id=(s, near),
            device_id_type=MESH,
        )

    def for_near(d):
        return part_copy(d, 0, near, n0_send, n0_recv)

    def for_diag(d):
        return part_copy(d, 1, diag, n1_send, n1_recv)

    def pair_copy(d):
        return pltpu.make_async_remote_copy(
            src_ref=pair.at[d],
            dst_ref=far_in.at[d],
            send_sem=g_send.at[d],
            recv_sem=g_recv.at[d],
            device_id=(s, far),
            device_id_type=MESH,
        )

    def back(d):
        return pltpu.make_async_remote_copy(
            src_ref=total.at[d],
            dst_ref=out.at[d],
            send_sem=r_send.at[d],
            recv_sem=r_recv.at[d],
            device_id=((s + steps - d) % steps, t),
            device_id_type=MESH,
        )

    def share(d):
        for c in both:
            to_sp(c, d).wait_recv()
            far_copy(c, d).start()
            near_copy(c, d).start()

    def forward(d):
        for c in both:
            far_copy(c, d).wait_recv()
            fwd_copy(c, d).start()

    def arrived(d):
        for c in both:
            near_copy(c, d).wait_recv()
            fwd_copy(c, d).wait_recv()

    def experts(d):
        gate_pre = jnp.dot(rows[d], w_gate[...], preferred_element_type=jnp.float32)
        up_pre = jnp.dot(rows[d], w_up[...], preferred_element_type=jnp.float32)
        act_grad = contract_cols(cots[d], w_down[...])
        gate_clamped = jnp.minimum(gate_pre, CLAMP_LIMIT)
        up_clamped = jnp.clip(up_pre, -CLAMP_LIMIT, CLAMP_LIMIT)
        sigma = jax.nn.sigmoid(SLOPE_ALPHA * gate_clamped)
        gated = gate_clamped * sigma
        act[d] = ((up_clamped + 1.0) * gated).astype(jnp.bfloat16)
        inside = (up_pre > -CLAMP_LIMIT) & (up_pre < CLAMP_LIMIT)
        up_g = jnp.where(inside, act_grad * gated, 0.0).astype(jnp.bfloat16)
        slope = sigma + SLOPE_ALPHA * gate_clamped * sigma * (1.0 - sigma)
        gate_g = jnp.where(
            gate_pre < CLAMP_LIMIT, act_grad * (up_clamped + 1.0) * slope, 0.0
        ).astype(jnp.bfloat16)
        gate_pg[d] = gate_g
        up_pg[d] = up_g
        for q in range(part.shape[-1] // width):
            mine = pl.ds(q * width, width)
            value = contract_cols(gate_g, w_gate[mine, :]) + contract_cols(up_g, w_up[mine, :])
            part[d, :, mine] = value.astype(part.dtype)

    def open_up(d):
        for_diag(d).start()
        for_near(d).start()

    def add_pair(d):
        for_diag(d).wait_recv()
        mine = part[d, :, lanes(far)].astype(jnp.float32)
        pair[d] = (mine + near_in[1, d].astype(jnp.float32)).astype(pair.dtype)
        pair_copy(d).start()

    def whole(d):
        for_near(d).wait_recv()
        pair_copy(d).wait_recv()
        mine = part[d, :, lanes(t)].astype(jnp.float32)
        summed = mine + near_in[0, d].astype(jnp.float32)
        return (summed + far_in[d].astype(jnp.float32)).astype(out.dtype)

    def flat(ref, cols):
        return ref[:, :, cols].reshape(-1, cols.size)

    every = pl.ds(0, hidden)

    def row_grads(k):
        cols = pl.ds(pl.multiple_of(k * 256, 256), 256)
        left = flat(rows, cols)
        gate_grad[cols, :] = contract_rows(left, flat(gate_pg, every)).astype(gate_grad.dtype)
        up_grad[cols, :] = contract_rows(left, flat(up_pg, every)).astype(up_grad.dtype)

    def act_grads(k):
        cols = pl.ds(pl.multiple_of(k * 512, 512), 512)
        down_grad[:, cols] = contract_rows(flat(act, every), flat(cots, cols)).astype(
            down_grad.dtype
        )

    meet(steps, True, near, far)

    def send(k):
        for c in both:
            to_sp(c, k).start()

    looped(1, steps, send)
    for c in both:
        own(c).start()
    for c in both:
        own(c).wait()

    def step(k):
        @pl.when(k < steps)
        def _():
            share(k)

        @pl.when((k >= 2) & (k < steps + 1))
        def _():
            forward(k - 1)

        @pl.when(k >= 3)
        def _():
            arrived(k - 2)

        @pl.when(k >= 2)
        def _():
            experts(k - 2)
            open_up(k - 2)

        @pl.when(k >= 3)
        def _():
            add_pair(k - 3)

        @pl.when(k >= 5)
        def _():
            d = k - 4
            total[d] = whole(d)
            back(d).start()

    looped(1, steps + 2, step)
    last = steps - 1
    half = rows.shape[-1] // 512
    looped(0, half, row_grads)
    add_pair(last)
    total[last - 1] = whole(last - 1)
    back(last - 1).start()
    looped(half, 2 * half, row_grads)
    total[last] = whole(last)
    back(last).start()
    out[0] = whole(0)
    looped(0, half, act_grads)

    def finish(d):
        for_near(d).wait_send()
        for_diag(d).wait_send()
        pair_copy(d).wait_send()

    def finish_remote(d):
        for c in both:
            to_sp(c, d).wait_send()
            near_copy(c, d).wait_send()
            far_copy(c, d).wait_send()
            fwd_copy(c, d).wait_send()
        back(d).wait()

    looped(0, steps, finish)
    looped(1, steps, finish_remote)


def routed_experts(send_rows, send_cots, own_rows, own_cots, w_gate, w_up, w_down, collective_id):
    steps, count, width = send_rows.shape
    model_width, hidden = w_gate.shape
    kind = send_rows.dtype
    block = (steps, count, width)
    outs = [
        jax.ShapeDtypeStruct((model_width, hidden), kind),
        jax.ShapeDtypeStruct((model_width, hidden), kind),
        jax.ShapeDtypeStruct((hidden, model_width), kind),
        jax.ShapeDtypeStruct(block, kind),
    ]
    pairs = pltpu.SemaphoreType.DMA((2, steps))
    ones = pltpu.SemaphoreType.DMA((steps,))
    return pl.pallas_call(
        functools.partial(routed_kernel, steps),
        out_shape=tuple(outs),
        in_specs=[pl.BlockSpec(memory_space=pltpu.VMEM)] * 7,
        out_specs=tuple(pl.BlockSpec(memory_space=pltpu.VMEM) for _ in outs),
        scratch_shapes=[pltpu.VMEM((steps, count, model_width), kind)] * 2
        + [pltpu.VMEM((steps, count, hidden), kind)] * 3
        + [pltpu.VMEM((steps, count, model_width), kind), pltpu.VMEM((2,) + block, kind)]
        + [pltpu.VMEM(block, kind)] * 3
        + [pltpu.SemaphoreType.DMA((2,))]
        + [pairs] * 8
        + [ones] * 8,
        compiler_params=pltpu.CompilerParams(
            collective_id=collective_id, has_side_effects=True, vmem_limit_bytes=36 << 20
        ),
    )(send_rows, send_cots, own_rows, own_cots, w_gate, w_up, w_down)


def local(
    grad_out,
    resid,
    norm_gain,
    routes,
    route_weights,
    gate_weight,
    up_weight,
    down_weight,
    proj_weight,
    conv_sum,
    conv_gain,
    conv_taps,
    conv_value,
    conv_gate,
):
    tok_rows, model_width = resid.shape
    sp_count = lax.axis_size("sp")
    tp_count = lax.axis_size("tp")
    capacity = 3 * tok_rows // sp_count
    col_count = model_width // tp_count
    resid_f = resid.astype(jnp.float32)
    inv_rms = lax.rsqrt(jnp.mean(resid_f * resid_f, axis=-1, keepdims=True) + 1e-06)
    normed = (resid_f * inv_rms * norm_gain).astype(jnp.bfloat16)
    my_sp = lax.axis_index("sp")
    away = (routes - my_sp) % sp_count
    steps_away = jnp.arange(sp_count, dtype=jnp.int32)
    named = away[:, :, None] == steps_away[None, None, :]
    chosen = jnp.any(named, axis=1)
    weight_of = jnp.sum(jnp.where(named, route_weights[:, :, None], 0.0), axis=1)
    token_ids = jnp.arange(tok_rows, dtype=jnp.int32)
    earlier = (token_ids[None, :] < token_ids[:, None]).astype(jnp.bfloat16)
    rank = jnp.dot(earlier, chosen.astype(jnp.bfloat16), preferred_element_type=jnp.float32)
    rank = jnp.where(chosen, rank, -1.0).astype(jnp.int32)
    slots = jnp.arange(capacity, dtype=jnp.int32)
    held = rank.T[:, None, :] == slots[None, :, None]
    slot_weight = jnp.sum(jnp.where(held, weight_of.T[:, None, :], 0.0), axis=2)
    pick = held.astype(jnp.bfloat16).reshape(sp_count * capacity, tok_rows)
    first_col = lax.axis_index("tp") * col_count
    normed_part = lax.dynamic_slice_in_dim(normed, first_col, col_count, 1)
    cots_part = lax.dynamic_slice_in_dim(grad_out, first_col, col_count, 1)
    slot_weight = slot_weight.reshape(-1, 1)
    send_rows = jnp.dot(pick, normed_part, preferred_element_type=jnp.float32).astype(jnp.bfloat16)
    send_cots = jnp.dot(pick, cots_part, preferred_element_type=jnp.float32)
    send_cots = (send_cots * slot_weight).astype(jnp.bfloat16)
    own_pick = pick[:capacity]
    own_rows = jnp.dot(own_pick, normed, preferred_element_type=jnp.float32).astype(jnp.bfloat16)
    own_cots = jnp.dot(own_pick, grad_out, preferred_element_type=jnp.float32)
    own_cots = (own_cots * slot_weight[:capacity]).astype(jnp.bfloat16)
    if capacity % 16 == 0 and model_width % 512 == 0:
        gate_grad, up_grad, down_grad, returned = routed_experts(
            send_rows.reshape(sp_count, capacity, col_count),
            send_cots.reshape(sp_count, capacity, col_count),
            own_rows,
            own_cots,
            gate_weight[0],
            up_weight[0],
            down_weight[0],
            4,
        )
        returned = returned.reshape(sp_count * capacity, col_count)
    else:
        routed_rows, routed_cots = spread(
            (
                send_rows.reshape(sp_count, capacity, col_count),
                send_cots.reshape(sp_count, capacity, col_count),
            ),
            (own_rows, own_cots),
            None,
            True,
            False,
            0,
        )
        routed_rows = routed_rows.reshape(sp_count * capacity, model_width)
        routed_cots = routed_cots.reshape(sp_count * capacity, model_width)
        gate_grad, up_grad, down_grad, partial_value = expert_backward(
            routed_rows, routed_cots, gate_weight[0], up_weight[0], down_weight[0]
        )
        returned = combine(
            partial_value.reshape(sp_count, capacity, model_width).astype(jnp.bfloat16), 1
        ).reshape(sp_count * capacity, col_count)
    normed_part_grad = contract_rows(pick, returned).astype(jnp.bfloat16)
    channels = conv_sum.shape[1]
    summed = conv_sum.astype(jnp.float32).reshape(tok_rows, channels // GROUP, GROUP)
    centre = summed - jnp.mean(summed, axis=-1, keepdims=True)
    inv_std = lax.rsqrt(jnp.mean(centre * centre, axis=-1, keepdims=True) + 1e-05)
    grouped = centre * inv_std
    chan_normed = grouped.reshape(tok_rows, channels)
    pre_act = chan_normed * conv_gain
    sigma_conv = jax.nn.sigmoid(pre_act)
    conv_out = (pre_act * sigma_conv).astype(jnp.bfloat16)
    chunks = 4
    normed_grad, all_out = spread(
        (normed_part_grad.reshape(chunks, tok_rows // chunks, col_count),),
        None,
        conv_out,
        True,
        False,
        2,
    )
    normed_grad = normed_grad.reshape(tok_rows, model_width)
    feature_grad = normed_grad.astype(jnp.float32) * norm_gain
    cubed = inv_rms * inv_rms * inv_rms
    resid_grad = (
        grad_out.astype(jnp.float32)
        + inv_rms * feature_grad
        - resid_f * cubed * jnp.mean(resid_f * feature_grad, axis=-1, keepdims=True)
    ).astype(jnp.bfloat16)
    share = tok_rows // tp_count
    feat_rows = model_width // sp_count
    tokens_part = lax.dynamic_slice_in_dim(resid_grad, lax.axis_index("tp") * share, share, 0)
    by_feature = tokens_part.reshape(share, sp_count, feat_rows).transpose(1, 0, 2)
    own_features = lax.dynamic_slice_in_dim(resid_grad, my_sp * feat_rows, feat_rows, 1)
    (feature_cols,) = spread(
        (by_feature,), (own_features.reshape(tp_count, share, feat_rows),), None, False, True, 3
    )
    proj_grad = contract_rows(
        feature_cols.reshape(sp_count * tok_rows, feat_rows),
        all_out.reshape(sp_count * tok_rows, channels),
    )
    out_grad = jnp.dot(resid_grad, proj_weight, preferred_element_type=jnp.float32)
    normal_grad = (
        out_grad * sigma_conv * (1.0 + pre_act * (1.0 - sigma_conv)) * conv_gain
    ).reshape(tok_rows, channels // GROUP, GROUP)
    sum_grad = inv_std * (
        normal_grad
        - jnp.mean(normal_grad, axis=-1, keepdims=True)
        - grouped * jnp.mean(normal_grad * grouped, axis=-1, keepdims=True)
    )
    sum_grad = sum_grad.reshape(tok_rows, channels)
    following = passed_along(sum_grad[: CONV_K - 1], "sp", -1)
    extended = jnp.concatenate([sum_grad, following], axis=0)
    gated_grad = lax.conv_general_dilated(
        extended[None],
        conv_taps[::-1][:, None, :],
        (1,),
        ((0, 0),),
        dimension_numbers=("NWC", "WIO", "NWC"),
        feature_group_count=channels,
        precision=lax.Precision.HIGHEST,
    )[0]
    sigma_gate = jax.nn.sigmoid(conv_gate.astype(jnp.float32))
    value_grad = (gated_grad * sigma_gate).astype(jnp.bfloat16)
    gate_input_grad = (
        gated_grad * conv_value.astype(jnp.float32) * sigma_gate * (1.0 - sigma_gate)
    ).astype(jnp.bfloat16)
    return (gate_grad[None], up_grad[None], down_grad[None], proj_grad, value_grad, gate_input_grad)


def solution(mesh):
    in_specs = (
        P("sp", None),
        P("sp", None),
        P(),
        P("sp", None),
        P("sp", None),
        P("sp", None, "tp"),
        P("sp", None, "tp"),
        P("sp", "tp", None),
        P(None, "tp"),
        P("sp", "tp"),
        P("tp"),
        P(None, "tp"),
        P("sp", "tp"),
        P("sp", "tp"),
    )
    out_specs = (
        P("sp", None, "tp"),
        P("sp", None, "tp"),
        P("sp", "tp", None),
        P("sp", "tp"),
        P("sp", "tp"),
        P("sp", "tp"),
    )
    return jax.shard_map(local, mesh=mesh, in_specs=in_specs, out_specs=out_specs, check_vma=False)
```

```python
import functools

import jax
import jax.numpy as jnp
from jax import lax
from jax.experimental import pallas as pl
from jax.experimental.pallas import tpu as pltpu
from jax.sharding import PartitionSpec as P

CONV_K = 31
GROUP = 128
MESH = pl.DeviceIdType.MESH


CLAMP_LIMIT = 7.0
SLOPE_ALPHA = 1.702


def passed_along(block, axis, distance):
    devices = range(lax.axis_size(axis))
    route = [(i - distance, i) for i in devices if i - distance in devices]
    return lax.ppermute(block, axis, route)


def tp_places():
    mine = lax.axis_index("tp")
    near = mine + 1 - 2 * (mine % 2)
    far = (mine + 2) % 4
    diag = (near + 2) % 4
    return mine, near, far, diag


def meet(steps, over_sp, near, far):
    s, t = lax.axis_index("sp"), lax.axis_index("tp")
    barrier = pltpu.get_barrier_semaphore()
    pl.semaphore_signal(barrier, inc=1, device_id=(s, near), device_id_type=MESH)
    pl.semaphore_signal(barrier, inc=1, device_id=(s, far), device_id_type=MESH)
    total = 2
    if over_sp:

        def greet(d, carry):
            pl.semaphore_signal(
                barrier, inc=1, device_id=((s + d) % steps, t), device_id_type=MESH
            )
            return carry

        lax.fori_loop(1, steps, greet, 0)
        total += steps - 1
    pl.semaphore_wait(barrier, total)


def crossing_first(steps, k):
    return steps // 2 + ((k + 1) // 2) * (2 * (k % 2) - 1)


def looped(first, last, body):
    def step(k, carry):
        body(k)
        return carry

    lax.fori_loop(first, last, step, 0)


def spread_kernel(count, steps, over_sp, in_lanes, absolute, beside, sp_count, *refs):
    refs = list(refs)
    sends, refs = refs[:count], refs[count:]
    fulls, refs = (refs[:count], refs[count:]) if over_sp else (None, refs)
    side, refs = (refs[0], refs[1:]) if beside else (None, refs)
    outs, refs = refs[:count], refs[count:]
    side_out, refs = (refs[0], refs[1:]) if beside else (None, refs)
    own_sem, a_send, a_recv, b_send, f_send, c_send, near_recv, fwd_recv, far_recv = refs[:9]
    s = lax.axis_index("sp")
    t, near, far, _ = tp_places()
    width = sends[0].shape[-1]

    def place(c, d, q):
        if in_lanes:
            return outs[c].at[d, :, pl.ds(pl.multiple_of(q * width, width), width)]
        return outs[c].at[d, q]

    def source(c, d):
        return sends[c].at[(s + d) % steps if absolute else d]

    def own(c, d):
        if over_sp:
            return pltpu.make_async_copy(fulls[c], outs[c].at[0], own_sem.at[c, 0])
        return pltpu.make_async_copy(source(c, d), place(c, d, t), own_sem.at[c, d])

    def to_sp(c, d):
        return pltpu.make_async_remote_copy(
            src_ref=source(c, d),
            dst_ref=place(c, d, t),
            send_sem=a_send.at[c, d],
            recv_sem=a_recv.at[c, d],
            device_id=((s + d) % steps, t),
            device_id_type=MESH,
        )

    def to_tp(c, d, q, target, send_sem, recv_sem):
        return pltpu.make_async_remote_copy(
            src_ref=place(c, d, q),
            dst_ref=place(c, d, q),
            send_sem=send_sem.at[c, d],
            recv_sem=recv_sem.at[c, d],
            device_id=(s, target),
            device_id_type=MESH,
        )

    def near_copy(c, d):
        return to_tp(c, d, t, near, b_send, near_recv)

    def far_copy(c, d):
        return to_tp(c, d, t, far, f_send, far_recv)

    def fwd_copy(c, d):
        return to_tp(c, d, far, near, c_send, fwd_recv)

    def side_copy(d):
        side_send, side_recv = refs[10:12]
        return pltpu.make_async_remote_copy(
            src_ref=side,
            dst_ref=side_out.at[d],
            send_sem=side_send.at[d],
            recv_sem=side_recv.at[d],
            device_id=((s + d) % sp_count, t),
            device_id_type=MESH,
        )

    def own_side():
        return pltpu.make_async_copy(side, side_out.at[0], refs[9].at[0])

    def share(c, d):
        far_copy(c, d).start()
        near_copy(c, d).start()

    def forward(c, d):
        far_copy(c, d).wait_recv()
        fwd_copy(c, d).start()

    def finish(c, d):
        near_copy(c, d).wait()
        far_copy(c, d).wait_send()
        fwd_copy(c, d).wait()

    def loop(first, last, body):
        def each(k):
            d = k + 1 if over_sp else k
            for c in range(count):
                body(c, d)

        looped(first, last, each)

    meet(sp_count, over_sp or beside, near, far)
    if over_sp:
        loop(0, steps - 1, lambda c, d: to_sp(c, d).start())
        for c in range(count):
            own(c, 0).start()

        def pass_on(k):
            for c in range(count):
                d = k + 1
                to_sp(c, d).wait_recv()
                share(c, d)

        def pass_on_twice(k):
            pass_on(k)
            for c in range(count):
                forward(c, k)

        pass_on(0)
        looped(1, steps - 1, pass_on_twice)
        loop(steps - 2, steps - 1, forward)
        loop(0, steps - 1, finish)
        loop(0, steps - 1, lambda c, d: to_sp(c, d).wait_send())
        for c in range(count):
            own(c, 0).wait()
    else:
        loop(0, steps, lambda c, d: own(c, d).start())
        if beside:
            looped(0, sp_count - 1, lambda k: side_copy(crossing_first(sp_count, k)).start())
            own_side().start()

        def share_own(c, d):
            own(c, d).wait()
            share(c, d)

        loop(0, steps, share_own)
        loop(0, steps, forward)
        loop(0, steps, finish)
        if beside:
            looped(0, sp_count - 1, lambda k: side_copy(crossing_first(sp_count, k)).wait())
            own_side().wait()


def spread(sends, fulls, side, in_lanes, absolute, collective_id):
    count = len(sends)
    steps, rows, width = sends[0].shape
    tp_count, sp_count = lax.axis_size("tp"), lax.axis_size("sp")
    over_sp, beside = fulls is not None, side is not None
    shape = (steps, rows, tp_count * width) if in_lanes else (steps, tp_count, rows, width)
    out_shape = [jax.ShapeDtypeStruct(shape, x.dtype) for x in sends]
    operands = list(sends) + (list(fulls) if over_sp else []) + ([side] if beside else [])
    scratch = [pltpu.SemaphoreType.DMA((count, steps))] * 9
    if beside:
        out_shape.append(jax.ShapeDtypeStruct((sp_count,) + side.shape, side.dtype))
        scratch += [pltpu.SemaphoreType.DMA((1,))] + [pltpu.SemaphoreType.DMA((sp_count,))] * 2
    return pl.pallas_call(
        functools.partial(
            spread_kernel, count, steps, over_sp, in_lanes, absolute, beside, sp_count
        ),
        out_shape=tuple(out_shape),
        in_specs=[pl.BlockSpec(memory_space=pltpu.VMEM)] * len(operands),
        out_specs=tuple(pl.BlockSpec(memory_space=pltpu.VMEM) for _ in out_shape),
        scratch_shapes=scratch,
        compiler_params=pltpu.CompilerParams(
            collective_id=collective_id, has_side_effects=True, vmem_limit_bytes=40 << 20
        ),
    )(*operands)


def combine_kernel(
    steps, part, out, near_in, pair, far_in, total,
    n0_send, n0_recv, n1_send, n1_recv, f_send, f_recv, a_send, a_recv,
):
    s = lax.axis_index("sp")
    t, near, far, diag = tp_places()
    width = out.shape[-1]

    def lanes(q):
        return pl.ds(pl.multiple_of(q * width, width), width)

    def near_copy(d, which, q, send_sem, recv_sem):
        return pltpu.make_async_remote_copy(
            src_ref=part.at[d, :, lanes(q)],
            dst_ref=near_in.at[which, d],
            send_sem=send_sem.at[d],
            recv_sem=recv_sem.at[d],
            device_id=(s, near),
            device_id_type=MESH,
        )

    def for_near(d):
        return near_copy(d, 0, near, n0_send, n0_recv)

    def for_diag(d):
        return near_copy(d, 1, diag, n1_send, n1_recv)

    def far_copy(d):
        return pltpu.make_async_remote_copy(
            src_ref=pair.at[d],
            dst_ref=far_in.at[d],
            send_sem=f_send.at[d],
            recv_sem=f_recv.at[d],
            device_id=(s, far),
            device_id_type=MESH,
        )

    def back(d):
        return pltpu.make_async_remote_copy(
            src_ref=total.at[d],
            dst_ref=out.at[d],
            send_sem=a_send.at[d],
            recv_sem=a_recv.at[d],
            device_id=((s + steps - d) % steps, t),
            device_id_type=MESH,
        )

    meet(steps, True, near, far)

    def open_up(d):
        for_diag(d).start()
        for_near(d).start()

    def add_pair(d):
        for_diag(d).wait_recv()
        mine = part[d, :, lanes(far)].astype(jnp.float32)
        pair[d] = (mine + near_in[1, d].astype(jnp.float32)).astype(pair.dtype)
        far_copy(d).start()

    def whole(d):
        for_near(d).wait_recv()
        far_copy(d).wait_recv()
        mine = part[d, :, lanes(t)].astype(jnp.float32)
        both = mine + near_in[0, d].astype(jnp.float32)
        return (both + far_in[d].astype(jnp.float32)).astype(out.dtype)

    def send_back(d):
        total[d] = whole(d)
        back(d).start()

    def at(k):
        return crossing_first(steps, k)

    lag = min(3, steps - 1)
    looped(0, steps - 1, lambda k: open_up(at(k)))
    open_up(0)
    looped(0, lag, lambda k: add_pair(at(k)))

    def middle(k):
        add_pair(at(k))
        send_back(at(k - lag))

    looped(lag, steps - 1, middle)
    add_pair(0)
    looped(steps - 1 - lag, steps - 1, lambda k: send_back(at(k)))
    out[0] = whole(0)

    def finish(d):
        for_near(d).wait_send()
        for_diag(d).wait_send()
        far_copy(d).wait_send()

    looped(0, steps, finish)
    looped(1, steps, lambda d: back(d).wait())


def combine(part, collective_id):
    steps, rows, all_width = part.shape
    width = all_width // lax.axis_size("tp")
    block = (steps, rows, width)
    return pl.pallas_call(
        functools.partial(combine_kernel, steps),
        out_shape=jax.ShapeDtypeStruct(block, part.dtype),
        in_specs=[pl.BlockSpec(memory_space=pltpu.VMEM)],
        out_specs=pl.BlockSpec(memory_space=pltpu.VMEM),
        scratch_shapes=[
            pltpu.VMEM((2,) + block, part.dtype),
            pltpu.VMEM(block, part.dtype),
            pltpu.VMEM(block, part.dtype),
            pltpu.VMEM(block, part.dtype),
        ]
        + [pltpu.SemaphoreType.DMA((steps,))] * 8,
        compiler_params=pltpu.CompilerParams(
            collective_id=collective_id, has_side_effects=True, vmem_limit_bytes=40 << 20
        ),
    )(part)


def contract_rows(left_side, right_side):
    return lax.dot_general(
        left_side, right_side, (((0,), (0,)), ((), ())), preferred_element_type=jnp.float32
    )


def contract_cols(left_side, right_side):
    return lax.dot_general(
        left_side, right_side, (((1,), (1,)), ((), ())), preferred_element_type=jnp.float32
    )


def expert_backward(routed_rows, routed_cots, w_gate, w_up, w_down):
    gate_pre = jnp.dot(routed_rows, w_gate, preferred_element_type=jnp.float32)
    up_pre = jnp.dot(routed_rows, w_up, preferred_element_type=jnp.float32)
    gate_clamped = jnp.minimum(gate_pre, CLAMP_LIMIT)
    up_clamped = jnp.clip(up_pre, -CLAMP_LIMIT, CLAMP_LIMIT)
    sigma = jax.nn.sigmoid(SLOPE_ALPHA * gate_clamped)
    gated = gate_clamped * sigma
    act = ((up_clamped + 1.0) * gated).astype(jnp.bfloat16)
    down_grad = contract_rows(act, routed_cots).astype(jnp.bfloat16)
    act_grad = contract_cols(routed_cots, w_down)
    inside = (up_pre > -CLAMP_LIMIT) & (up_pre < CLAMP_LIMIT)
    up_pre_grad = jnp.where(inside, act_grad * gated, 0.0).astype(jnp.bfloat16)
    slope = sigma + SLOPE_ALPHA * gate_clamped * sigma * (1.0 - sigma)
    gate_pre_grad = jnp.where(
        gate_pre < CLAMP_LIMIT, act_grad * (up_clamped + 1.0) * slope, 0.0
    ).astype(jnp.bfloat16)
    gate_grad = contract_rows(routed_rows, gate_pre_grad).astype(jnp.bfloat16)
    up_grad = contract_rows(routed_rows, up_pre_grad).astype(jnp.bfloat16)
    partial_value = contract_cols(gate_pre_grad, w_gate) + contract_cols(up_pre_grad, w_up)
    return (gate_grad, up_grad, down_grad, partial_value)


def routed_kernel(
    steps, send_rows, send_cots, own_rows, own_cots, w_gate, w_up, w_down, side,
    gate_grad, up_grad, down_grad, out, side_out,
    rows, cots, act, gate_pg, up_pg, part, near_in, pair, far_in, total,
    own_sem, a_send, a_recv, b_send, f_send, c_send, near_recv, fwd_recv, far_recv,
    n0_send, n0_recv, n1_send, n1_recv, g_send, g_recv, r_send, r_recv, s_send, s_recv,
):
    s = lax.axis_index("sp")
    t, near, far, diag = tp_places()
    sends, fulls, held = (send_rows, send_cots), (own_rows, own_cots), (rows, cots)
    width = send_rows.shape[-1]
    hidden = w_gate.shape[1]
    both = (0, 1)

    def lanes(q):
        return pl.ds(pl.multiple_of(q * width, width), width)

    def own(c):
        return pltpu.make_async_copy(fulls[c], held[c].at[0], own_sem.at[c])

    def to_sp(c, d):
        return pltpu.make_async_remote_copy(
            src_ref=sends[c].at[d],
            dst_ref=held[c].at[d, :, lanes(t)],
            send_sem=a_send.at[c, d],
            recv_sem=a_recv.at[c, d],
            device_id=((s + d) % steps, t),
            device_id_type=MESH,
        )

    def to_tp(c, d, q, target, send_sem, recv_sem):
        return pltpu.make_async_remote_copy(
            src_ref=held[c].at[d, :, lanes(q)],
            dst_ref=held[c].at[d, :, lanes(q)],
            send_sem=send_sem.at[c, d],
            recv_sem=recv_sem.at[c, d],
            device_id=(s, target),
            device_id_type=MESH,
        )

    def near_copy(c, d):
        return to_tp(c, d, t, near, b_send, near_recv)

    def far_copy(c, d):
        return to_tp(c, d, t, far, f_send, far_recv)

    def fwd_copy(c, d):
        return to_tp(c, d, far, near, c_send, fwd_recv)

    def part_copy(d, which, q, send_sem, recv_sem):
        return pltpu.make_async_remote_copy(
            src_ref=part.at[d, :, lanes(q)],
            dst_ref=near_in.at[which, d],
            send_sem=send_sem.at[d],
            recv_sem=recv_sem.at[d],
            device_id=(s, near),
            device_id_type=MESH,
        )

    def for_near(d):
        return part_copy(d, 0, near, n0_send, n0_recv)

    def for_diag(d):
        return part_copy(d, 1, diag, n1_send, n1_recv)

    def pair_copy(d):
        return pltpu.make_async_remote_copy(
            src_ref=pair.at[d],
            dst_ref=far_in.at[d],
            send_sem=g_send.at[d],
            recv_sem=g_recv.at[d],
            device_id=(s, far),
            device_id_type=MESH,
        )

    def back(d):
        return pltpu.make_async_remote_copy(
            src_ref=total.at[d],
            dst_ref=out.at[d],
            send_sem=r_send.at[d],
            recv_sem=r_recv.at[d],
            device_id=((s + steps - d) % steps, t),
            device_id_type=MESH,
        )

    def own_side():
        return pltpu.make_async_copy(side, side_out.at[0], own_sem.at[2])

    def side_copy(d):
        return pltpu.make_async_remote_copy(
            src_ref=side,
            dst_ref=side_out.at[d],
            send_sem=s_send.at[d],
            recv_sem=s_recv.at[d],
            device_id=((s + d) % steps, t),
            device_id_type=MESH,
        )

    def share(d):
        for c in both:
            to_sp(c, d).wait_recv()
            far_copy(c, d).start()
            near_copy(c, d).start()

    def forward(d):
        for c in both:
            far_copy(c, d).wait_recv()
            fwd_copy(c, d).start()

    def arrived(d):
        for c in both:
            near_copy(c, d).wait_recv()
            fwd_copy(c, d).wait_recv()

    def experts(d):
        gate_pre = jnp.dot(rows[d], w_gate[...], preferred_element_type=jnp.float32)
        up_pre = jnp.dot(rows[d], w_up[...], preferred_element_type=jnp.float32)
        act_grad = contract_cols(cots[d], w_down[...])
        gate_clamped = jnp.minimum(gate_pre, CLAMP_LIMIT)
        up_clamped = jnp.clip(up_pre, -CLAMP_LIMIT, CLAMP_LIMIT)
        sigma = jax.nn.sigmoid(SLOPE_ALPHA * gate_clamped)
        gated = gate_clamped * sigma
        act[d] = ((up_clamped + 1.0) * gated).astype(jnp.bfloat16)
        inside = (up_pre > -CLAMP_LIMIT) & (up_pre < CLAMP_LIMIT)
        up_g = jnp.where(inside, act_grad * gated, 0.0).astype(jnp.bfloat16)
        slope = sigma + SLOPE_ALPHA * gate_clamped * sigma * (1.0 - sigma)
        gate_g = jnp.where(
            gate_pre < CLAMP_LIMIT, act_grad * (up_clamped + 1.0) * slope, 0.0
        ).astype(jnp.bfloat16)
        gate_pg[d] = gate_g
        up_pg[d] = up_g
        for q in range(part.shape[-1] // width):
            mine = pl.ds(q * width, width)
            value = contract_cols(gate_g, w_gate[mine, :]) + contract_cols(up_g, w_up[mine, :])
            part[d, :, mine] = value.astype(part.dtype)

    def open_up(d):
        for_diag(d).start()
        for_near(d).start()

    def add_pair(d):
        for_diag(d).wait_recv()
        mine = part[d, :, lanes(far)].astype(jnp.float32)
        pair[d] = (mine + near_in[1, d].astype(jnp.float32)).astype(pair.dtype)
        pair_copy(d).start()

    def whole(d):
        for_near(d).wait_recv()
        pair_copy(d).wait_recv()
        mine = part[d, :, lanes(t)].astype(jnp.float32)
        summed = mine + near_in[0, d].astype(jnp.float32)
        return (summed + far_in[d].astype(jnp.float32)).astype(out.dtype)

    def flat(ref, cols):
        return ref[:, :, cols].reshape(-1, cols.size)

    every = pl.ds(0, hidden)

    def row_grads(k):
        cols = pl.ds(pl.multiple_of(k * 256, 256), 256)
        left = flat(rows, cols)
        gate_grad[cols, :] = contract_rows(left, flat(gate_pg, every)).astype(gate_grad.dtype)
        up_grad[cols, :] = contract_rows(left, flat(up_pg, every)).astype(up_grad.dtype)

    def act_grads(k):
        cols = pl.ds(pl.multiple_of(k * 512, 512), 512)
        down_grad[:, cols] = contract_rows(flat(act, every), flat(cots, cols)).astype(
            down_grad.dtype
        )

    meet(steps, True, near, far)

    def send(k):
        for c in both:
            to_sp(c, k).start()

    looped(1, steps, send)
    own_side().start()
    for c in both:
        own(c).start()
    for c in both:
        own(c).wait()

    def step(k):
        @pl.when(k < steps)
        def _():
            share(k)
            side_copy(k).start()

        @pl.when((k >= 2) & (k < steps + 1))
        def _():
            forward(k - 1)

        @pl.when(k >= 3)
        def _():
            arrived(k - 2)

        @pl.when(k >= 2)
        def _():
            experts(k - 2)
            open_up(k - 2)

        @pl.when(k >= 3)
        def _():
            add_pair(k - 3)

        @pl.when(k >= 5)
        def _():
            d = k - 4
            total[d] = whole(d)
            back(d).start()

    looped(1, steps + 2, step)
    last = steps - 1
    half = rows.shape[-1] // 512
    looped(0, half, row_grads)
    add_pair(last)
    total[last - 1] = whole(last - 1)
    back(last - 1).start()
    looped(half, 2 * half, row_grads)
    total[last] = whole(last)
    back(last).start()
    out[0] = whole(0)
    looped(0, half, act_grads)

    def finish(d):
        for_near(d).wait_send()
        for_diag(d).wait_send()
        pair_copy(d).wait_send()

    def finish_remote(d):
        for c in both:
            to_sp(c, d).wait_send()
            near_copy(c, d).wait_send()
            far_copy(c, d).wait_send()
            fwd_copy(c, d).wait_send()
        back(d).wait()
        side_copy(d).wait()

    own_side().wait()
    looped(0, steps, finish)
    looped(1, steps, finish_remote)


def routed_experts(
    send_rows, send_cots, own_rows, own_cots, w_gate, w_up, w_down, side, collective_id
):
    steps, count, width = send_rows.shape
    model_width, hidden = w_gate.shape
    kind = send_rows.dtype
    block = (steps, count, width)
    outs = [
        jax.ShapeDtypeStruct((model_width, hidden), kind),
        jax.ShapeDtypeStruct((model_width, hidden), kind),
        jax.ShapeDtypeStruct((hidden, model_width), kind),
        jax.ShapeDtypeStruct(block, kind),
        jax.ShapeDtypeStruct((steps,) + side.shape, side.dtype),
    ]
    pairs = pltpu.SemaphoreType.DMA((2, steps))
    ones = pltpu.SemaphoreType.DMA((steps,))
    return pl.pallas_call(
        functools.partial(routed_kernel, steps),
        out_shape=tuple(outs),
        in_specs=[pl.BlockSpec(memory_space=pltpu.VMEM)] * 8,
        out_specs=tuple(pl.BlockSpec(memory_space=pltpu.VMEM) for _ in outs),
        scratch_shapes=[pltpu.VMEM((steps, count, model_width), kind)] * 2
        + [pltpu.VMEM((steps, count, hidden), kind)] * 3
        + [pltpu.VMEM((steps, count, model_width), kind), pltpu.VMEM((2,) + block, kind)]
        + [pltpu.VMEM(block, kind)] * 3
        + [pltpu.SemaphoreType.DMA((3,))]
        + [pairs] * 8
        + [ones] * 10,
        compiler_params=pltpu.CompilerParams(
            collective_id=collective_id, has_side_effects=True, vmem_limit_bytes=36 << 20
        ),
    )(send_rows, send_cots, own_rows, own_cots, w_gate, w_up, w_down, side)


def settle_kernel(
    steps, part_grad, grad_out, resid, inv_rms, norm_gain, proj_weight,
    conv_sum, conv_gain, conv_taps, conv_value, conv_gate,
    feature_cols, value_grad, gate_input_grad,
    full, grads, extended, far_send, far_recv, near_send, near_recv, fwd_send, fwd_recv,
    own_sem, x_send, x_recv, xf_send, xf_recv, xn_send, xn_recv, xw_send, xw_recv,
    h_send, h_recv,
):
    s = lax.axis_index("sp")
    t, near, far, diag = tp_places()
    tok_rows, width = part_grad.shape
    chunks, share = feature_cols.shape[1], feature_cols.shape[2]
    feat_rows = feature_cols.shape[3]
    overlap = conv_taps.shape[0] - 1

    def rows_of(j):
        return pl.ds(pl.multiple_of(j * share, share), share)

    def lanes(q):
        return pl.ds(pl.multiple_of(q * width, width), width)

    def mine_at(j):
        return full.at[rows_of(j), lanes(t)]

    def own_copy():
        return pltpu.make_async_copy(part_grad, full.at[:, lanes(t)], own_sem.at[0])

    def gather(j, q, src, target, send_sem, recv_sem):
        return pltpu.make_async_remote_copy(
            src_ref=src,
            dst_ref=full.at[rows_of(j), lanes(q)],
            send_sem=send_sem.at[j],
            recv_sem=recv_sem.at[j],
            device_id=(s, target),
            device_id_type=MESH,
        )

    def to_far(j):
        return gather(j, t, part_grad.at[rows_of(j), :], far, far_send, far_recv)

    def to_near(j):
        return gather(j, t, part_grad.at[rows_of(j), :], near, near_send, near_recv)

    def pass_near(j):
        return gather(j, far, full.at[rows_of(j), lanes(far)], near, fwd_send, fwd_recv)

    def spread_out(d):
        feats = pl.ds(pl.multiple_of(((s + d) % steps) * feat_rows, feat_rows), feat_rows)
        return pltpu.make_async_remote_copy(
            src_ref=grads.at[rows_of(t), feats],
            dst_ref=feature_cols.at[d, t],
            send_sem=x_send.at[d],
            recv_sem=x_recv.at[d],
            device_id=((s + d) % steps, t),
            device_id_type=MESH,
        )

    def beside(d, q, target, send_sem, recv_sem):
        return pltpu.make_async_remote_copy(
            src_ref=feature_cols.at[d, q],
            dst_ref=feature_cols.at[d, q],
            send_sem=send_sem.at[d],
            recv_sem=recv_sem.at[d],
            device_id=(s, target),
            device_id_type=MESH,
        )

    def x_far(d):
        return beside(d, t, far, xf_send, xf_recv)

    def x_near(d):
        return beside(d, t, near, xn_send, xn_recv)

    def x_pass(d):
        return beside(d, far, near, xw_send, xw_recv)

    def halo():
        return pltpu.make_async_remote_copy(
            src_ref=extended.at[pl.ds(0, overlap + 2)],
            dst_ref=extended.at[pl.ds(tok_rows, overlap + 2)],
            send_sem=h_send.at[0],
            recv_sem=h_recv.at[0],
            device_id=((s + steps - 1) % steps, t),
            device_id_type=MESH,
        )

    gain = norm_gain[...]

    def settle(j):
        here = rows_of(j)
        feature_grad = full[here, :].astype(jnp.float32) * gain
        x = resid[here, :].astype(jnp.float32)
        scale = inv_rms[here, :]
        cubed = scale * scale * scale
        mean = jnp.mean(x * feature_grad, axis=-1, keepdims=True)
        value = grad_out[here, :].astype(jnp.float32) + scale * feature_grad - x * cubed * mean
        grads[here, :] = value.astype(grads.dtype)

    def crossing(k):
        return crossing_first(steps, k)

    meet(steps, True, near, far)
    for j in (far, diag, t, near):
        to_far(j).start()
    for j in (near, t, diag, far):
        to_near(j).start()
    own_copy().start()
    summed = conv_sum[...].astype(jnp.float32)
    centre = summed - jnp.mean(summed, axis=-1, keepdims=True)
    inv_std = lax.rsqrt(jnp.mean(centre * centre, axis=-1, keepdims=True) + 1e-05)
    grouped = centre * inv_std
    pre_act = grouped * conv_gain[...]
    sigma = jax.nn.sigmoid(pre_act)
    slope = sigma * (1.0 + pre_act * (1.0 - sigma)) * conv_gain[...]
    own_copy().wait()

    def arrive(j):
        to_far(j).wait_recv()
        pass_near(j).start()

    def whole(j):
        to_near(j).wait_recv()
        pass_near(j).wait_recv()

    arrive(t)
    arrive(near)
    whole(t)
    settle(t)
    looped(0, steps - 1, lambda k: spread_out(crossing(k)).start())
    arrive(far)
    arrive(diag)
    for j in (near, far, diag):
        whole(j)
        settle(j)
    feats = pl.ds(pl.multiple_of(s * feat_rows, feat_rows), feat_rows)
    feature_cols[0] = grads[:, feats].reshape(chunks, share, feat_rows)
    out_grad = jnp.dot(grads[...], proj_weight[...], preferred_element_type=jnp.float32)
    normal = out_grad * slope
    sum_grad = inv_std * (
        normal
        - jnp.mean(normal, axis=-1, keepdims=True)
        - grouped * jnp.mean(normal * grouped, axis=-1, keepdims=True)
    )
    extended[pl.ds(0, tok_rows), :] = sum_grad
    halo().start()

    def share_out(d):
        spread_out(d).wait_recv()
        x_far(d).start()
        x_near(d).start()

    def pass_on(d):
        x_far(d).wait_recv()
        x_pass(d).start()

    def both(k):
        share_out(crossing(k))
        pass_on(crossing(k - 1))

    share_out(crossing(0))
    looped(1, steps - 1, both)
    halo().wait()

    @pl.when(s == steps - 1)
    def _():
        extended[pl.ds(tok_rows, overlap + 2), :] = jnp.zeros(
            (overlap + 2, extended.shape[1]), extended.dtype
        )

    gated_grad = extended[pl.ds(overlap, tok_rows), :] * conv_taps[pl.ds(0, 1), :]
    for j in range(1, overlap + 1):
        gated_grad += extended[pl.ds(overlap - j, tok_rows), :] * conv_taps[pl.ds(j, 1), :]
    sigma_gate = jax.nn.sigmoid(conv_gate[...].astype(jnp.float32))
    value_grad[...] = (gated_grad * sigma_gate).astype(value_grad.dtype)
    gate_input_grad[...] = (
        gated_grad * conv_value[...].astype(jnp.float32) * sigma_gate * (1.0 - sigma_gate)
    ).astype(gate_input_grad.dtype)
    pass_on(crossing(steps - 2))

    def finish(k):
        d = crossing(k)
        spread_out(d).wait_send()
        x_near(d).wait()
        x_far(d).wait_send()
        x_pass(d).wait()

    looped(0, steps - 1, finish)

    def finish_gather(j):
        to_far(j).wait_send()
        to_near(j).wait_send()
        pass_near(j).wait_send()

    looped(0, chunks, finish_gather)


def settle_tokens(operands, collective_id):
    part_grad, resid, conv_sum = operands[0], operands[2], operands[6]
    overlap = operands[8].shape[0] - 1
    steps, tp_count = lax.axis_size("sp"), lax.axis_size("tp")
    tok_rows, model_width = resid.shape
    channels = conv_sum.shape[1]
    kind = resid.dtype
    outs = [
        jax.ShapeDtypeStruct((steps, tp_count, tok_rows // tp_count, model_width // steps), kind),
        jax.ShapeDtypeStruct((tok_rows, channels), kind),
        jax.ShapeDtypeStruct((tok_rows, channels), kind),
    ]
    fours = pltpu.SemaphoreType.DMA((tp_count,))
    ones = pltpu.SemaphoreType.DMA((steps,))
    single = pltpu.SemaphoreType.DMA((1,))
    return pl.pallas_call(
        functools.partial(settle_kernel, steps),
        out_shape=tuple(outs),
        in_specs=[pl.BlockSpec(memory_space=pltpu.VMEM)] * len(operands),
        out_specs=tuple(pl.BlockSpec(memory_space=pltpu.VMEM) for _ in outs),
        scratch_shapes=[
            pltpu.VMEM((tok_rows, model_width), kind),
            pltpu.VMEM((tok_rows, model_width), kind),
            pltpu.VMEM((tok_rows + overlap + 2, channels), jnp.float32),
        ]
        + [fours] * 6
        + [single]
        + [ones] * 8
        + [single] * 2,
        compiler_params=pltpu.CompilerParams(
            collective_id=collective_id, has_side_effects=True, vmem_limit_bytes=24 << 20
        ),
    )(*operands)


def last_kernel(feature_cols, all_out, gate_in, up_in, down_in, proj, gate_out, up_out, down_out, sem):
    moves = [
        pltpu.make_async_copy(a, b, sem.at[i])
        for i, (a, b) in enumerate(((gate_in, gate_out), (up_in, up_out), (down_in, down_out)))
    ]
    for move in moves:
        move.start()
    proj[...] = contract_rows(feature_cols[...], all_out[...])
    for move in moves:
        move.wait()


def last_stage(feature_cols, all_out, grads):
    held = [pl.BlockSpec(memory_space=pltpu.VMEM)]
    outside = [pl.BlockSpec(memory_space=pl.ANY)]
    shape = (feature_cols.shape[1], all_out.shape[1])
    outs = [jax.ShapeDtypeStruct(shape, jnp.float32)]
    outs += [jax.ShapeDtypeStruct(g.shape, g.dtype) for g in grads]
    return pl.pallas_call(
        last_kernel,
        out_shape=tuple(outs),
        in_specs=held * 5,
        out_specs=tuple(held + outside * 3),
        scratch_shapes=[pltpu.SemaphoreType.DMA((3,))],
        compiler_params=pltpu.CompilerParams(vmem_limit_bytes=16 << 20),
    )(feature_cols, all_out, *grads)


def local(
    grad_out,
    resid,
    norm_gain,
    routes,
    route_weights,
    gate_weight,
    up_weight,
    down_weight,
    proj_weight,
    conv_sum,
    conv_gain,
    conv_taps,
    conv_value,
    conv_gate,
):
    tok_rows, model_width = resid.shape
    sp_count = lax.axis_size("sp")
    tp_count = lax.axis_size("tp")
    capacity = 3 * tok_rows // sp_count
    col_count = model_width // tp_count
    resid_f = resid.astype(jnp.float32)
    inv_rms = lax.rsqrt(jnp.mean(resid_f * resid_f, axis=-1, keepdims=True) + 1e-06)
    normed = (resid_f * inv_rms * norm_gain).astype(jnp.bfloat16)
    my_sp = lax.axis_index("sp")
    away = (routes - my_sp) % sp_count
    steps_away = jnp.arange(sp_count, dtype=jnp.int32)
    named = away[:, :, None] == steps_away[None, None, :]
    chosen = jnp.any(named, axis=1)
    weight_of = jnp.sum(jnp.where(named, route_weights[:, :, None], 0.0), axis=1)
    token_ids = jnp.arange(tok_rows, dtype=jnp.int32)
    earlier = (token_ids[None, :] < token_ids[:, None]).astype(jnp.bfloat16)
    rank = jnp.dot(earlier, chosen.astype(jnp.bfloat16), preferred_element_type=jnp.float32)
    rank = jnp.where(chosen, rank, -1.0).astype(jnp.int32)
    slots = jnp.arange(capacity, dtype=jnp.int32)
    held = rank.T[:, None, :] == slots[None, :, None]
    slot_weight = jnp.sum(jnp.where(held, weight_of.T[:, None, :], 0.0), axis=2)
    pick = held.astype(jnp.bfloat16).reshape(sp_count * capacity, tok_rows)
    first_col = lax.axis_index("tp") * col_count
    normed_part = lax.dynamic_slice_in_dim(normed, first_col, col_count, 1)
    cots_part = lax.dynamic_slice_in_dim(grad_out, first_col, col_count, 1)
    slot_weight = slot_weight.reshape(-1, 1)
    send_rows = jnp.dot(pick, normed_part, preferred_element_type=jnp.float32).astype(jnp.bfloat16)
    send_cots = jnp.dot(pick, cots_part, preferred_element_type=jnp.float32)
    send_cots = (send_cots * slot_weight).astype(jnp.bfloat16)
    own_pick = pick[:capacity]
    own_rows = jnp.dot(own_pick, normed, preferred_element_type=jnp.float32).astype(jnp.bfloat16)
    own_cots = jnp.dot(own_pick, grad_out, preferred_element_type=jnp.float32)
    own_cots = (own_cots * slot_weight[:capacity]).astype(jnp.bfloat16)
    channels = conv_sum.shape[1]
    summed = conv_sum.astype(jnp.float32).reshape(tok_rows, channels // GROUP, GROUP)
    centre = summed - jnp.mean(summed, axis=-1, keepdims=True)
    inv_std = lax.rsqrt(jnp.mean(centre * centre, axis=-1, keepdims=True) + 1e-05)
    grouped = centre * inv_std
    chan_normed = grouped.reshape(tok_rows, channels)
    pre_act = chan_normed * conv_gain
    sigma_conv = jax.nn.sigmoid(pre_act)
    conv_out = (pre_act * sigma_conv).astype(jnp.bfloat16)
    aligned = capacity % 16 == 0 and model_width % (128 * sp_count) == 0 and channels == GROUP
    if aligned:
        gate_grad, up_grad, down_grad, returned, all_out = routed_experts(
            send_rows.reshape(sp_count, capacity, col_count),
            send_cots.reshape(sp_count, capacity, col_count),
            own_rows,
            own_cots,
            gate_weight[0],
            up_weight[0],
            down_weight[0],
            conv_out,
            4,
        )
        returned = returned.reshape(sp_count * capacity, col_count)
    else:
        routed_rows, routed_cots = spread(
            (
                send_rows.reshape(sp_count, capacity, col_count),
                send_cots.reshape(sp_count, capacity, col_count),
            ),
            (own_rows, own_cots),
            None,
            True,
            False,
            0,
        )
        routed_rows = routed_rows.reshape(sp_count * capacity, model_width)
        routed_cots = routed_cots.reshape(sp_count * capacity, model_width)
        gate_grad, up_grad, down_grad, partial_value = expert_backward(
            routed_rows, routed_cots, gate_weight[0], up_weight[0], down_weight[0]
        )
        returned = combine(
            partial_value.reshape(sp_count, capacity, model_width).astype(jnp.bfloat16), 1
        ).reshape(sp_count * capacity, col_count)
    normed_part_grad = contract_rows(pick, returned).astype(jnp.bfloat16)
    if aligned:
        operands = (
            normed_part_grad,
            grad_out,
            resid,
            inv_rms,
            norm_gain[None],
            proj_weight,
            conv_sum,
            conv_gain[None],
            conv_taps,
            conv_value,
            conv_gate,
        )
        feature_cols, value_grad, gate_input_grad = settle_tokens(operands, 5)
        feat_rows = model_width // sp_count
        proj_grad, gate_grad, up_grad, down_grad = last_stage(
            feature_cols.reshape(sp_count * tok_rows, feat_rows),
            all_out.reshape(sp_count * tok_rows, channels),
            (gate_grad, up_grad, down_grad),
        )
        weight_grads = (gate_grad[None], up_grad[None], down_grad[None])
        return weight_grads + (proj_grad, value_grad, gate_input_grad)
    chunks = 4
    normed_grad, all_out = spread(
        (normed_part_grad.reshape(chunks, tok_rows // chunks, col_count),),
        None,
        conv_out,
        True,
        False,
        2,
    )
    normed_grad = normed_grad.reshape(tok_rows, model_width)
    feature_grad = normed_grad.astype(jnp.float32) * norm_gain
    cubed = inv_rms * inv_rms * inv_rms
    resid_grad = (
        grad_out.astype(jnp.float32)
        + inv_rms * feature_grad
        - resid_f * cubed * jnp.mean(resid_f * feature_grad, axis=-1, keepdims=True)
    ).astype(jnp.bfloat16)
    share = tok_rows // tp_count
    feat_rows = model_width // sp_count
    tokens_part = lax.dynamic_slice_in_dim(resid_grad, lax.axis_index("tp") * share, share, 0)
    by_feature = tokens_part.reshape(share, sp_count, feat_rows).transpose(1, 0, 2)
    own_features = lax.dynamic_slice_in_dim(resid_grad, my_sp * feat_rows, feat_rows, 1)
    (feature_cols,) = spread(
        (by_feature,), (own_features.reshape(tp_count, share, feat_rows),), None, False, True, 3
    )
    proj_grad = contract_rows(
        feature_cols.reshape(sp_count * tok_rows, feat_rows),
        all_out.reshape(sp_count * tok_rows, channels),
    )
    out_grad = jnp.dot(resid_grad, proj_weight, preferred_element_type=jnp.float32)
    normal_grad = (
        out_grad * sigma_conv * (1.0 + pre_act * (1.0 - sigma_conv)) * conv_gain
    ).reshape(tok_rows, channels // GROUP, GROUP)
    sum_grad = inv_std * (
        normal_grad
        - jnp.mean(normal_grad, axis=-1, keepdims=True)
        - grouped * jnp.mean(normal_grad * grouped, axis=-1, keepdims=True)
    )
    sum_grad = sum_grad.reshape(tok_rows, channels)
    following = passed_along(sum_grad[: CONV_K - 1], "sp", -1)
    extended = jnp.concatenate([sum_grad, following], axis=0)
    gated_grad = lax.conv_general_dilated(
        extended[None],
        conv_taps[::-1][:, None, :],
        (1,),
        ((0, 0),),
        dimension_numbers=("NWC", "WIO", "NWC"),
        feature_group_count=channels,
        precision=lax.Precision.HIGHEST,
    )[0]
    sigma_gate = jax.nn.sigmoid(conv_gate.astype(jnp.float32))
    value_grad = (gated_grad * sigma_gate).astype(jnp.bfloat16)
    gate_input_grad = (
        gated_grad * conv_value.astype(jnp.float32) * sigma_gate * (1.0 - sigma_gate)
    ).astype(jnp.bfloat16)
    return (gate_grad[None], up_grad[None], down_grad[None], proj_grad, value_grad, gate_input_grad)


def solution(mesh):
    in_specs = (
        P("sp", None),
        P("sp", None),
        P(),
        P("sp", None),
        P("sp", None),
        P("sp", None, "tp"),
        P("sp", None, "tp"),
        P("sp", "tp", None),
        P(None, "tp"),
        P("sp", "tp"),
        P("tp"),
        P(None, "tp"),
        P("sp", "tp"),
        P("sp", "tp"),
    )
    out_specs = (
        P("sp", None, "tp"),
        P("sp", None, "tp"),
        P("sp", "tp", None),
        P("sp", "tp"),
        P("sp", "tp"),
        P("sp", "tp"),
    )
    return jax.shard_map(local, mesh=mesh, in_specs=in_specs, out_specs=out_specs, check_vma=False)
```

```python
import functools

import jax
import jax.numpy as jnp
from jax import lax
from jax.experimental import pallas as pl
from jax.experimental.pallas import tpu as pltpu
from jax.sharding import PartitionSpec as P

CONV_K = 31
GROUP = 128
MESH = pl.DeviceIdType.MESH


CLAMP_LIMIT = 7.0
SLOPE_ALPHA = 1.702


def passed_along(block, axis, distance):
    devices = range(lax.axis_size(axis))
    route = [(i - distance, i) for i in devices if i - distance in devices]
    return lax.ppermute(block, axis, route)


def tp_places():
    mine = lax.axis_index("tp")
    near = mine + 1 - 2 * (mine % 2)
    far = (mine + 2) % 4
    diag = (near + 2) % 4
    return mine, near, far, diag


def meet(steps, over_sp, near, far):
    s, t = lax.axis_index("sp"), lax.axis_index("tp")
    barrier = pltpu.get_barrier_semaphore()
    pl.semaphore_signal(barrier, inc=1, device_id=(s, near), device_id_type=MESH)
    pl.semaphore_signal(barrier, inc=1, device_id=(s, far), device_id_type=MESH)
    total = 2
    if over_sp:

        def greet(d, carry):
            pl.semaphore_signal(
                barrier, inc=1, device_id=((s + d) % steps, t), device_id_type=MESH
            )
            return carry

        lax.fori_loop(1, steps, greet, 0)
        total += steps - 1
    pl.semaphore_wait(barrier, total)


def crossing_first(steps, k):
    return steps // 2 + ((k + 1) // 2) * (2 * (k % 2) - 1)


def looped(first, last, body):
    def step(k, carry):
        body(k)
        return carry

    lax.fori_loop(first, last, step, 0)


def spread_kernel(count, steps, over_sp, in_lanes, absolute, beside, sp_count, *refs):
    refs = list(refs)
    sends, refs = refs[:count], refs[count:]
    fulls, refs = (refs[:count], refs[count:]) if over_sp else (None, refs)
    side, refs = (refs[0], refs[1:]) if beside else (None, refs)
    outs, refs = refs[:count], refs[count:]
    side_out, refs = (refs[0], refs[1:]) if beside else (None, refs)
    own_sem, a_send, a_recv, b_send, f_send, c_send, near_recv, fwd_recv, far_recv = refs[:9]
    s = lax.axis_index("sp")
    t, near, far, _ = tp_places()
    width = sends[0].shape[-1]

    def place(c, d, q):
        if in_lanes:
            return outs[c].at[d, :, pl.ds(pl.multiple_of(q * width, width), width)]
        return outs[c].at[d, q]

    def source(c, d):
        return sends[c].at[(s + d) % steps if absolute else d]

    def own(c, d):
        if over_sp:
            return pltpu.make_async_copy(fulls[c], outs[c].at[0], own_sem.at[c, 0])
        return pltpu.make_async_copy(source(c, d), place(c, d, t), own_sem.at[c, d])

    def to_sp(c, d):
        return pltpu.make_async_remote_copy(
            src_ref=source(c, d),
            dst_ref=place(c, d, t),
            send_sem=a_send.at[c, d],
            recv_sem=a_recv.at[c, d],
            device_id=((s + d) % steps, t),
            device_id_type=MESH,
        )

    def to_tp(c, d, q, target, send_sem, recv_sem):
        return pltpu.make_async_remote_copy(
            src_ref=place(c, d, q),
            dst_ref=place(c, d, q),
            send_sem=send_sem.at[c, d],
            recv_sem=recv_sem.at[c, d],
            device_id=(s, target),
            device_id_type=MESH,
        )

    def near_copy(c, d):
        return to_tp(c, d, t, near, b_send, near_recv)

    def far_copy(c, d):
        return to_tp(c, d, t, far, f_send, far_recv)

    def fwd_copy(c, d):
        return to_tp(c, d, far, near, c_send, fwd_recv)

    def side_copy(d):
        side_send, side_recv = refs[10:12]
        return pltpu.make_async_remote_copy(
            src_ref=side,
            dst_ref=side_out.at[d],
            send_sem=side_send.at[d],
            recv_sem=side_recv.at[d],
            device_id=((s + d) % sp_count, t),
            device_id_type=MESH,
        )

    def own_side():
        return pltpu.make_async_copy(side, side_out.at[0], refs[9].at[0])

    def share(c, d):
        far_copy(c, d).start()
        near_copy(c, d).start()

    def forward(c, d):
        far_copy(c, d).wait_recv()
        fwd_copy(c, d).start()

    def finish(c, d):
        near_copy(c, d).wait()
        far_copy(c, d).wait_send()
        fwd_copy(c, d).wait()

    def loop(first, last, body):
        def each(k):
            d = k + 1 if over_sp else k
            for c in range(count):
                body(c, d)

        looped(first, last, each)

    meet(sp_count, over_sp or beside, near, far)
    if over_sp:
        loop(0, steps - 1, lambda c, d: to_sp(c, d).start())
        for c in range(count):
            own(c, 0).start()

        def pass_on(k):
            for c in range(count):
                d = k + 1
                to_sp(c, d).wait_recv()
                share(c, d)

        def pass_on_twice(k):
            pass_on(k)
            for c in range(count):
                forward(c, k)

        pass_on(0)
        looped(1, steps - 1, pass_on_twice)
        loop(steps - 2, steps - 1, forward)
        loop(0, steps - 1, finish)
        loop(0, steps - 1, lambda c, d: to_sp(c, d).wait_send())
        for c in range(count):
            own(c, 0).wait()
    else:
        loop(0, steps, lambda c, d: own(c, d).start())
        if beside:
            looped(0, sp_count - 1, lambda k: side_copy(crossing_first(sp_count, k)).start())
            own_side().start()

        def share_own(c, d):
            own(c, d).wait()
            share(c, d)

        loop(0, steps, share_own)
        loop(0, steps, forward)
        loop(0, steps, finish)
        if beside:
            looped(0, sp_count - 1, lambda k: side_copy(crossing_first(sp_count, k)).wait())
            own_side().wait()


def spread(sends, fulls, side, in_lanes, absolute, collective_id):
    count = len(sends)
    steps, rows, width = sends[0].shape
    tp_count, sp_count = lax.axis_size("tp"), lax.axis_size("sp")
    over_sp, beside = fulls is not None, side is not None
    shape = (steps, rows, tp_count * width) if in_lanes else (steps, tp_count, rows, width)
    out_shape = [jax.ShapeDtypeStruct(shape, x.dtype) for x in sends]
    operands = list(sends) + (list(fulls) if over_sp else []) + ([side] if beside else [])
    scratch = [pltpu.SemaphoreType.DMA((count, steps))] * 9
    if beside:
        out_shape.append(jax.ShapeDtypeStruct((sp_count,) + side.shape, side.dtype))
        scratch += [pltpu.SemaphoreType.DMA((1,))] + [pltpu.SemaphoreType.DMA((sp_count,))] * 2
    return pl.pallas_call(
        functools.partial(
            spread_kernel, count, steps, over_sp, in_lanes, absolute, beside, sp_count
        ),
        out_shape=tuple(out_shape),
        in_specs=[pl.BlockSpec(memory_space=pltpu.VMEM)] * len(operands),
        out_specs=tuple(pl.BlockSpec(memory_space=pltpu.VMEM) for _ in out_shape),
        scratch_shapes=scratch,
        compiler_params=pltpu.CompilerParams(
            collective_id=collective_id, has_side_effects=True, vmem_limit_bytes=40 << 20
        ),
    )(*operands)


def combine_kernel(
    steps, part, out, near_in, pair, far_in, total,
    n0_send, n0_recv, n1_send, n1_recv, f_send, f_recv, a_send, a_recv,
):
    s = lax.axis_index("sp")
    t, near, far, diag = tp_places()
    width = out.shape[-1]

    def lanes(q):
        return pl.ds(pl.multiple_of(q * width, width), width)

    def near_copy(d, which, q, send_sem, recv_sem):
        return pltpu.make_async_remote_copy(
            src_ref=part.at[d, :, lanes(q)],
            dst_ref=near_in.at[which, d],
            send_sem=send_sem.at[d],
            recv_sem=recv_sem.at[d],
            device_id=(s, near),
            device_id_type=MESH,
        )

    def for_near(d):
        return near_copy(d, 0, near, n0_send, n0_recv)

    def for_diag(d):
        return near_copy(d, 1, diag, n1_send, n1_recv)

    def far_copy(d):
        return pltpu.make_async_remote_copy(
            src_ref=pair.at[d],
            dst_ref=far_in.at[d],
            send_sem=f_send.at[d],
            recv_sem=f_recv.at[d],
            device_id=(s, far),
            device_id_type=MESH,
        )

    def back(d):
        return pltpu.make_async_remote_copy(
            src_ref=total.at[d],
            dst_ref=out.at[d],
            send_sem=a_send.at[d],
            recv_sem=a_recv.at[d],
            device_id=((s + steps - d) % steps, t),
            device_id_type=MESH,
        )

    meet(steps, True, near, far)

    def open_up(d):
        for_diag(d).start()
        for_near(d).start()

    def add_pair(d):
        for_diag(d).wait_recv()
        mine = part[d, :, lanes(far)].astype(jnp.float32)
        pair[d] = (mine + near_in[1, d].astype(jnp.float32)).astype(pair.dtype)
        far_copy(d).start()

    def whole(d):
        for_near(d).wait_recv()
        far_copy(d).wait_recv()
        mine = part[d, :, lanes(t)].astype(jnp.float32)
        both = mine + near_in[0, d].astype(jnp.float32)
        return (both + far_in[d].astype(jnp.float32)).astype(out.dtype)

    def send_back(d):
        total[d] = whole(d)
        back(d).start()

    def at(k):
        return crossing_first(steps, k)

    lag = min(3, steps - 1)
    looped(0, steps - 1, lambda k: open_up(at(k)))
    open_up(0)
    looped(0, lag, lambda k: add_pair(at(k)))

    def middle(k):
        add_pair(at(k))
        send_back(at(k - lag))

    looped(lag, steps - 1, middle)
    add_pair(0)
    looped(steps - 1 - lag, steps - 1, lambda k: send_back(at(k)))
    out[0] = whole(0)

    def finish(d):
        for_near(d).wait_send()
        for_diag(d).wait_send()
        far_copy(d).wait_send()

    looped(0, steps, finish)
    looped(1, steps, lambda d: back(d).wait())


def combine(part, collective_id):
    steps, rows, all_width = part.shape
    width = all_width // lax.axis_size("tp")
    block = (steps, rows, width)
    return pl.pallas_call(
        functools.partial(combine_kernel, steps),
        out_shape=jax.ShapeDtypeStruct(block, part.dtype),
        in_specs=[pl.BlockSpec(memory_space=pltpu.VMEM)],
        out_specs=pl.BlockSpec(memory_space=pltpu.VMEM),
        scratch_shapes=[
            pltpu.VMEM((2,) + block, part.dtype),
            pltpu.VMEM(block, part.dtype),
            pltpu.VMEM(block, part.dtype),
            pltpu.VMEM(block, part.dtype),
        ]
        + [pltpu.SemaphoreType.DMA((steps,))] * 8,
        compiler_params=pltpu.CompilerParams(
            collective_id=collective_id, has_side_effects=True, vmem_limit_bytes=40 << 20
        ),
    )(part)


def contract_rows(left_side, right_side):
    return lax.dot_general(
        left_side, right_side, (((0,), (0,)), ((), ())), preferred_element_type=jnp.float32
    )


def contract_cols(left_side, right_side):
    return lax.dot_general(
        left_side, right_side, (((1,), (1,)), ((), ())), preferred_element_type=jnp.float32
    )


def expert_backward(routed_rows, routed_cots, w_gate, w_up, w_down):
    gate_pre = jnp.dot(routed_rows, w_gate, preferred_element_type=jnp.float32)
    up_pre = jnp.dot(routed_rows, w_up, preferred_element_type=jnp.float32)
    gate_clamped = jnp.minimum(gate_pre, CLAMP_LIMIT)
    up_clamped = jnp.clip(up_pre, -CLAMP_LIMIT, CLAMP_LIMIT)
    sigma = jax.nn.sigmoid(SLOPE_ALPHA * gate_clamped)
    gated = gate_clamped * sigma
    act = ((up_clamped + 1.0) * gated).astype(jnp.bfloat16)
    down_grad = contract_rows(act, routed_cots).astype(jnp.bfloat16)
    act_grad = contract_cols(routed_cots, w_down)
    inside = (up_pre > -CLAMP_LIMIT) & (up_pre < CLAMP_LIMIT)
    up_pre_grad = jnp.where(inside, act_grad * gated, 0.0).astype(jnp.bfloat16)
    slope = sigma + SLOPE_ALPHA * gate_clamped * sigma * (1.0 - sigma)
    gate_pre_grad = jnp.where(
        gate_pre < CLAMP_LIMIT, act_grad * (up_clamped + 1.0) * slope, 0.0
    ).astype(jnp.bfloat16)
    gate_grad = contract_rows(routed_rows, gate_pre_grad).astype(jnp.bfloat16)
    up_grad = contract_rows(routed_rows, up_pre_grad).astype(jnp.bfloat16)
    partial_value = contract_cols(gate_pre_grad, w_gate) + contract_cols(up_pre_grad, w_up)
    return (gate_grad, up_grad, down_grad, partial_value)


def relay_kernel(
    steps, info, grad_out, resid, norm_gain, gate_held, up_held, down_held, conv_sum, conv_gain,
    gate_grad, up_grad, down_grad, part_grad, side_out,
    w_gate, w_up, w_down, normed, infos, ranks, weights, before, picks,
    tok, over, cross, cross_far, held, act, gate_pg, up_pg, part,
    near_in, pair, far_in, total, ret, side,
    own_sem, info_send, info_recv, line_send, line_recv, end_send, cross_recv,
    across_send, afar_send, arr_recv, b_send, f_send, c_send, near_recv, fwd_recv, far_recv,
    n0_send, n0_recv, n1_send, n1_recv, g_send, g_recv, r_send, r_recv, s_send, s_recv,
):
    s = lax.axis_index("sp")
    t, near, far, diag = tp_places()
    line = steps // 2
    z, y = s // 2, s % 2
    across = s + 1 - 2 * y
    tok_rows, width = part_grad.shape
    count = cross.shape[2]
    hidden = w_gate.shape[1]
    model_width = resid.shape[1]
    both = (0, 1)
    kind = held.dtype
    sources = (grad_out, normed)

    def lanes(q):
        return pl.ds(pl.multiple_of(q * width, width), width)

    def remote(src, dst, send_sem, recv_sem, sp_to, tp_to):
        return pltpu.make_async_remote_copy(
            src_ref=src,
            dst_ref=dst,
            send_sem=send_sem,
            recv_sem=recv_sem,
            device_id=(sp_to, tp_to),
            device_id_type=MESH,
        )

    def weight_copies():
        pairs = ((gate_held, w_gate), (up_held, w_up), (down_held, w_down))
        return [pltpu.make_async_copy(a, b, own_sem.at[i]) for i, (a, b) in enumerate(pairs)]

    def info_copy(dz):
        peer = ((z + dz) % line) * 2 + y
        return remote(info, infos.at[z], info_send.at[dz], info_recv.at[z], peer, t)

    def info_from(zb):
        return remote(info, infos.at[zb], info_send.at[0], info_recv.at[zb], across, t)

    def line_copy(a, zb, src, up):
        to = s + 2 if up else s - 2
        return remote(src, tok.at[a, zb], line_send.at[a, up, zb], line_recv.at[a, zb], to, t)

    def end_copy(a, zb, col, up):
        to = s + 2 if up else s - 2
        j = 2 * zb + y
        if col == 0:
            dst, recv = held.at[a, j, :, lanes(t)], arr_recv.at[a, j]
        else:
            dst, recv = cross.at[a, zb], cross_recv.at[a, zb]
        return remote(over.at[a, zb, col], dst, end_send.at[a, col, zb], recv, to, t)

    def across_copy(a, zb):
        j = 2 * zb + y
        dst = held.at[a, j, :, lanes(t)]
        return remote(cross.at[a, zb], dst, across_send.at[a, zb], arr_recv.at[a, j], across, t)

    def across_far(a):
        dst = held.at[a, s, :, lanes(far)]
        return remote(cross_far.at[a], dst, afar_send.at[a], far_recv.at[a, s], across, t)

    def arrival(a, j):
        place = held.at[a, j, :, lanes(t)]
        return remote(place, place, f_send.at[a, j], arr_recv.at[a, j], s, far)

    def to_tp(a, j, q, target, send_sem, recv_sem):
        place = held.at[a, j, :, lanes(q)]
        return remote(place, place, send_sem.at[a, j], recv_sem.at[a, j], s, target)

    def near_copy(a, j):
        return to_tp(a, j, t, near, b_send, near_recv)

    def far_copy(a, j):
        return to_tp(a, j, t, far, f_send, far_recv)

    def fwd_copy(a, j):
        return to_tp(a, j, far, near, c_send, fwd_recv)

    def part_copy(j, which, q, send_sem, recv_sem):
        src, dst = part.at[j, :, lanes(q)], near_in.at[which, j]
        return remote(src, dst, send_sem.at[j], recv_sem.at[j], s, near)

    def for_near(j):
        return part_copy(j, 0, near, n0_send, n0_recv)

    def for_diag(j):
        return part_copy(j, 1, diag, n1_send, n1_recv)

    def pair_copy(j):
        return remote(pair.at[j], far_in.at[j], g_send.at[j], g_recv.at[j], s, far)

    def back(j):
        return remote(total.at[j], ret.at[s], r_send.at[j], r_recv.at[s], j, t)

    def back_from(e):
        return remote(total.at[e], ret.at[e], r_send.at[e], r_recv.at[e], e, t)

    def side_copy(d):
        to = (s + d) % steps
        return remote(side, side_out.at[d], s_send.at[d], s_recv.at[d], to, t)

    def table(zb):
        first, second = infos[zb, pl.ds(0, 1), :], infos[zb, pl.ds(1, 1), :]
        ids = lax.broadcasted_iota(jnp.int32, (steps, tok_rows), 0).astype(jnp.float32)
        chosen = (first == ids) | (second == ids)
        ones = jnp.where(chosen, 1.0, 0.0).astype(kind)
        rank = jnp.dot(ones, before[...], preferred_element_type=jnp.float32)
        ranks[zb] = jnp.where(chosen, rank, -1.0)
        weights[zb] = jnp.where(
            first == ids, infos[zb, pl.ds(2, 1), :], infos[zb, pl.ds(3, 1), :]
        )

    def pick(zb, e):
        slots = lax.broadcasted_iota(jnp.int32, (count, tok_rows), 0).astype(jnp.float32)
        return slots == ranks[zb, pl.ds(e, 1), :]

    def selected(a, zb, e, value):
        mask = pick(zb, e)
        hot = jnp.where(mask, 1.0, 0.0).astype(kind)
        out = jnp.dot(hot, value, preferred_element_type=jnp.float32)
        if a == 0:
            scale = jnp.where(mask, weights[zb, pl.ds(e, 1), :], 0.0)
            out = out * jnp.sum(scale, axis=1, keepdims=True)
        return out.astype(kind)

    def to_end(a, zb, value, up):
        end = z + 1 if up else z - 1
        for col in both:
            e = 2 * end + (y if col == 0 else 1 - y)
            over[a, zb, col] = selected(a, zb, e, value)
            end_copy(a, zb, col, up).start()

    def valid(m, up):
        return (z >= m) if up else (z + m < line)

    def block_at(m, up):
        return z - m if up else z + m

    def next_is_end(up):
        return (z + 1 == line - 1) if up else (z == 1)

    def next_is_inner(up):
        return (z + 1 < line - 1) if up else (z >= 2)

    def at_end(up):
        return (z == line - 1) if up else (z == 0)

    def share(a, j):
        far_copy(a, j).start()
        near_copy(a, j).start()

    def read_info(m, up):
        zb = block_at(m, up)

        @pl.when(valid(m, up))
        def _():
            info_from(zb).wait_recv()

        @pl.when(valid(m, up) & jnp.logical_not(at_end(up)))
        def _():
            table(zb)

    def handle(a, m, up):
        zb = block_at(m, up)
        j = 2 * zb + y

        @pl.when(valid(m, up) & at_end(up))
        def _():
            arrival(a, j).wait_recv()
            end_copy(a, zb, 1, up).wait_recv()
            across_copy(a, zb).start()
            share(a, j)

        @pl.when(valid(m, up) & jnp.logical_not(at_end(up)))
        def _():
            line_copy(a, zb, tok.at[a, zb], up).wait_recv()

            @pl.when(next_is_end(up))
            def _():
                to_end(a, zb, tok[a, zb], up)

            @pl.when(next_is_inner(up))
            def _():
                line_copy(a, zb, tok.at[a, zb], up).start()

            cross[a, zb] = selected(a, zb, across, tok[a, zb])
            across_copy(a, zb).start()
            held[a, j, :, lanes(t)] = selected(a, zb, s, tok[a, zb])
            share(a, j)

    def each_block(m, body):
        for up in both:
            ok = valid(m, up) if up else valid(m, up) & (m > 0)

            @pl.when(ok)
            def _():
                body(block_at(m, up))

    def each_chunk(m, body):
        def one(q):
            up, other = q // 2, q % 2
            zb = z + m - 2 * m * up
            ok = (zb >= 0) & (zb < line) & ((m > 0) | (up == 1))

            @pl.when(ok)
            def _():
                body(2 * zb + y + other * (1 - 2 * y))

        looped(0, 4, one)

    def unless_own(j, body):
        @pl.when(j != s)
        def _():
            body()

    def experts(j):
        def settle():
            for a in both:
                near_copy(a, j).wait_recv()
                fwd_copy(a, j).wait_recv()

        unless_own(j, settle)
        gate_pre = jnp.dot(held[1, j], w_gate[...], preferred_element_type=jnp.float32)
        up_pre = jnp.dot(held[1, j], w_up[...], preferred_element_type=jnp.float32)
        act_grad = contract_cols(held[0, j], w_down[...])
        gate_clamped = jnp.minimum(gate_pre, CLAMP_LIMIT)
        up_clamped = jnp.clip(up_pre, -CLAMP_LIMIT, CLAMP_LIMIT)
        sigma = jax.nn.sigmoid(SLOPE_ALPHA * gate_clamped)
        gated = gate_clamped * sigma
        act[j] = ((up_clamped + 1.0) * gated).astype(kind)
        inside = (up_pre > -CLAMP_LIMIT) & (up_pre < CLAMP_LIMIT)
        up_g = jnp.where(inside, act_grad * gated, 0.0).astype(kind)
        slope = sigma + SLOPE_ALPHA * gate_clamped * sigma * (1.0 - sigma)
        gate_g = jnp.where(
            gate_pre < CLAMP_LIMIT, act_grad * (up_clamped + 1.0) * slope, 0.0
        ).astype(kind)
        gate_pg[j] = gate_g
        up_pg[j] = up_g
        for q in range(model_width // width):
            mine = pl.ds(q * width, width)
            value = contract_cols(gate_g, w_gate[mine, :]) + contract_cols(up_g, w_up[mine, :])
            part[j, :, mine] = value.astype(kind)
        for_diag(j).start()
        for_near(j).start()

    def add_pair(j):
        for_diag(j).wait_recv()
        mine = part[j, :, lanes(far)].astype(jnp.float32)
        pair[j] = (mine + near_in[1, j].astype(jnp.float32)).astype(kind)
        pair_copy(j).start()

    def whole(j):
        for_near(j).wait_recv()
        pair_copy(j).wait_recv()
        mine = part[j, :, lanes(t)].astype(jnp.float32)
        summed = mine + near_in[0, j].astype(jnp.float32)
        return (summed + far_in[j].astype(jnp.float32)).astype(kind)

    def send_back(j):
        @pl.when(j == s)
        def _():
            ret[s] = whole(j)

        @pl.when(j != s)
        def _():
            total[j] = whole(j)
            back(j).start()

    def forward(j):
        def run():
            for a in both:
                far_copy(a, j).wait_recv()
                fwd_copy(a, j).start()

        unless_own(j, run)

    def flat(value):
        return value.reshape(-1, value.shape[-1])

    def row_grads(k):
        cols = pl.ds(pl.multiple_of(k * 256, 256), 256)
        left = flat(held[1, :, :, cols])
        gate_grad[cols, :] = contract_rows(left, flat(gate_pg[...])).astype(kind)
        up_grad[cols, :] = contract_rows(left, flat(up_pg[...])).astype(kind)

    def act_grads(k):
        cols = pl.ds(pl.multiple_of(k * 512, 512), 512)
        down_grad[:, cols] = contract_rows(flat(act[...]), flat(held[0, :, :, cols])).astype(kind)

    for copy in weight_copies():
        copy.start()
    meet(steps, True, near, far)

    def start_own(a):
        src = sources[a]
        for up in both:

            @pl.when(next_is_inner(up))
            def _():
                line_copy(a, z, src.at[:, lanes(t)], up).start()

    def end_own(a):
        for up in both:

            @pl.when(next_is_end(up))
            def _():
                to_end(a, z, sources[a][:, lanes(t)], up)

    start_own(0)
    looped(1, line, lambda dz: info_copy(dz).start())
    infos[z] = info[...]
    row_ids = lax.broadcasted_iota(jnp.int32, (tok_rows, tok_rows), 0)
    col_ids = lax.broadcasted_iota(jnp.int32, (tok_rows, tok_rows), 1)
    before[...] = jnp.where(row_ids < col_ids, 1.0, 0.0).astype(kind)
    table(z)
    end_own(0)
    gain = norm_gain[...]

    def normalise(k):
        here = pl.ds(pl.multiple_of(k * 32, 32), 32)
        x = resid[here, :].astype(jnp.float32)
        scale = lax.rsqrt(jnp.mean(x * x, axis=-1, keepdims=True) + 1e-06)
        normed[here, :] = (x * scale * gain).astype(kind)

    looped(0, tok_rows // 32, normalise)
    start_own(1)
    end_own(1)
    for a in both:
        cross[a, z] = selected(a, z, across, sources[a][:, lanes(t)])
        across_copy(a, z).start()
        cross_far[a] = selected(a, z, across, sources[a][:, lanes(far)])
        across_far(a).start()

    def own_chunk(q):
        for a in both:
            held[a, s, :, lanes(q)] = selected(a, z, s, sources[a][:, lanes(q)])

    looped(0, model_width // width, own_chunk)
    summed = conv_sum[...].astype(jnp.float32)
    centre = summed - jnp.mean(summed, axis=-1, keepdims=True)
    inv_std = lax.rsqrt(jnp.mean(centre * centre, axis=-1, keepdims=True) + 1e-05)
    pre_act = centre * inv_std * conv_gain[...]
    conv_out = (pre_act * jax.nn.sigmoid(pre_act)).astype(kind)
    side[...] = conv_out
    side_out[0] = conv_out

    def own_picks(e):
        picks[e] = jnp.where(pick(z, e), 1.0, 0.0).astype(kind)

    looped(0, steps, own_picks)
    for copy in weight_copies():
        copy.wait()

    def step(k):
        @pl.when(k < line)
        def _():
            for up in both:
                read_info(k, up)
            for a in both:
                for up in both:
                    handle(a, k, up)

        @pl.when(k == line - 1)
        def _():
            looped(1, steps, lambda d: side_copy(d).start())

        @pl.when(k == 1)
        def _():
            j = 2 * z + 1 - y
            for a in both:
                arrival(a, j).wait_recv()
                near_copy(a, j).start()

        each_chunk(k - 1, forward)
        each_chunk(k - 1, experts)

        @pl.when(k < line)
        def _():
            def meet_column(zb):
                j = 2 * zb + 1 - y
                for a in both:
                    arrival(a, j).wait_recv()
                    share(a, j)

            each_block(k, meet_column)

        each_chunk(k - 1, add_pair)

        @pl.when(k >= 2)
        def _():
            each_chunk(k - 2, send_back)

    looped(1, line + 1, step)
    half = model_width // 512
    looped(0, half, row_grads)
    each_chunk(line - 1, send_back)
    looped(half, 2 * half, row_grads)
    looped(0, half, act_grads)

    def gather_back(d):
        back_from((s + d) % steps).wait_recv()

    looped(1, steps, gather_back)
    part_grad[...] = contract_rows(flat(picks[...]), flat(ret[...])).astype(kind)

    def finish(j):
        for_near(j).wait_send()
        for_diag(j).wait_send()
        pair_copy(j).wait_send()

        @pl.when(j != s)
        def _():
            back(j).wait_send()
            for a in both:
                near_copy(a, j).wait_send()
                fwd_copy(a, j).wait_send()

        @pl.when(j // 2 != z)
        def _():
            for a in both:
                far_copy(a, j).wait_send()

    looped(0, steps, finish)

    def finish_side(d):
        side_copy(d).wait()

    looped(1, steps, finish_side)
    looped(1, line, lambda dz: info_copy(dz).wait_send())

    def finish_line(m):
        for up in both:
            zb = block_at(m, up)

            @pl.when(valid(m, up) & next_is_inner(up))
            def _():
                for a in both:
                    line_copy(a, zb, tok.at[a, zb], up).wait_send()

            @pl.when(valid(m, up) & next_is_end(up))
            def _():
                for a in both:
                    for col in both:
                        end_copy(a, zb, col, up).wait_send()

    looped(0, line, finish_line)

    def finish_across(zb):
        for a in both:
            across_copy(a, zb).wait_send()

    looped(0, line, finish_across)
    for a in both:
        across_far(a).wait_send()


def relay_experts(operands, collective_id):
    info, resid, w_gate, conv_sum = operands[0], operands[2], operands[4], operands[7]
    steps, tp_count = lax.axis_size("sp"), lax.axis_size("tp")
    line = steps // 2
    tok_rows, model_width = resid.shape
    count = 3 * tok_rows // steps
    width = model_width // tp_count
    hidden = w_gate.shape[1]
    kind = resid.dtype
    block = (steps, count, width)
    outs = [
        jax.ShapeDtypeStruct((model_width, hidden), kind),
        jax.ShapeDtypeStruct((model_width, hidden), kind),
        jax.ShapeDtypeStruct((hidden, model_width), kind),
        jax.ShapeDtypeStruct((tok_rows, width), kind),
        jax.ShapeDtypeStruct((steps,) + conv_sum.shape, kind),
    ]
    held = pl.BlockSpec(memory_space=pltpu.VMEM)
    outside = pl.BlockSpec(memory_space=pl.ANY)

    def sems(*shape):
        return pltpu.SemaphoreType.DMA(shape)

    return pl.pallas_call(
        functools.partial(relay_kernel, steps),
        out_shape=tuple(outs),
        in_specs=[held] * 4 + [outside] * 3 + [held] * 2,
        out_specs=tuple(held for _ in outs),
        scratch_shapes=[
            pltpu.VMEM((model_width, hidden), kind),
            pltpu.VMEM((model_width, hidden), kind),
            pltpu.VMEM((hidden, model_width), kind),
            pltpu.VMEM((tok_rows, model_width), kind),
            pltpu.VMEM((line,) + info.shape, jnp.float32),
            pltpu.VMEM((line, steps, tok_rows), jnp.float32),
            pltpu.VMEM((line, steps, tok_rows), jnp.float32),
            pltpu.VMEM((tok_rows, tok_rows), kind),
            pltpu.VMEM((steps, count, tok_rows), kind),
            pltpu.VMEM((2, line, tok_rows, width), kind),
            pltpu.VMEM((2, line, 2, count, width), kind),
            pltpu.VMEM((2, line, count, width), kind),
            pltpu.VMEM((2, count, width), kind),
            pltpu.VMEM((2, steps, count, model_width), kind),
        ]
        + [pltpu.VMEM((steps, count, hidden), kind)] * 3
        + [pltpu.VMEM((steps, count, model_width), kind), pltpu.VMEM((2,) + block, kind)]
        + [pltpu.VMEM(block, kind)] * 4
        + [pltpu.VMEM(conv_sum.shape, kind)]
        + [sems(3), sems(line), sems(line), sems(2, 2, line), sems(2, line), sems(2, 2, line)]
        + [sems(2, line), sems(2, line), sems(2), sems(2, steps)]
        + [sems(2, steps)] * 6
        + [sems(steps)] * 10,
        compiler_params=pltpu.CompilerParams(
            collective_id=collective_id, has_side_effects=True, vmem_limit_bytes=42 << 20
        ),
    )(*operands)


def settle_kernel(
    steps, part_grad, grad_out, resid, norm_gain, proj_weight,
    conv_sum, conv_gain, conv_taps, conv_value, conv_gate,
    feature_cols, value_grad, gate_input_grad,
    full, grads, extended, far_send, far_recv, near_send, near_recv, fwd_send, fwd_recv,
    own_sem, x_send, x_recv, xf_send, xf_recv, xn_send, xn_recv, xw_send, xw_recv,
    h_send, h_recv,
):
    s = lax.axis_index("sp")
    t, near, far, diag = tp_places()
    tok_rows, width = part_grad.shape
    chunks, share = feature_cols.shape[1], feature_cols.shape[2]
    feat_rows = feature_cols.shape[3]
    overlap = conv_taps.shape[0] - 1

    def rows_of(j):
        return pl.ds(pl.multiple_of(j * share, share), share)

    def lanes(q):
        return pl.ds(pl.multiple_of(q * width, width), width)

    def mine_at(j):
        return full.at[rows_of(j), lanes(t)]

    def own_copy():
        return pltpu.make_async_copy(part_grad, full.at[:, lanes(t)], own_sem.at[0])

    def gather(j, q, src, target, send_sem, recv_sem):
        return pltpu.make_async_remote_copy(
            src_ref=src,
            dst_ref=full.at[rows_of(j), lanes(q)],
            send_sem=send_sem.at[j],
            recv_sem=recv_sem.at[j],
            device_id=(s, target),
            device_id_type=MESH,
        )

    def to_far(j):
        return gather(j, t, part_grad.at[rows_of(j), :], far, far_send, far_recv)

    def to_near(j):
        return gather(j, t, part_grad.at[rows_of(j), :], near, near_send, near_recv)

    def pass_near(j):
        return gather(j, far, full.at[rows_of(j), lanes(far)], near, fwd_send, fwd_recv)

    def spread_out(d):
        feats = pl.ds(pl.multiple_of(((s + d) % steps) * feat_rows, feat_rows), feat_rows)
        return pltpu.make_async_remote_copy(
            src_ref=grads.at[rows_of(t), feats],
            dst_ref=feature_cols.at[d, t],
            send_sem=x_send.at[d],
            recv_sem=x_recv.at[d],
            device_id=((s + d) % steps, t),
            device_id_type=MESH,
        )

    def beside(d, q, target, send_sem, recv_sem):
        return pltpu.make_async_remote_copy(
            src_ref=feature_cols.at[d, q],
            dst_ref=feature_cols.at[d, q],
            send_sem=send_sem.at[d],
            recv_sem=recv_sem.at[d],
            device_id=(s, target),
            device_id_type=MESH,
        )

    def x_far(d):
        return beside(d, t, far, xf_send, xf_recv)

    def x_near(d):
        return beside(d, t, near, xn_send, xn_recv)

    def x_pass(d):
        return beside(d, far, near, xw_send, xw_recv)

    def halo():
        return pltpu.make_async_remote_copy(
            src_ref=extended.at[pl.ds(0, overlap + 2)],
            dst_ref=extended.at[pl.ds(tok_rows, overlap + 2)],
            send_sem=h_send.at[0],
            recv_sem=h_recv.at[0],
            device_id=((s + steps - 1) % steps, t),
            device_id_type=MESH,
        )

    gain = norm_gain[...]

    def settle(j):
        here = rows_of(j)
        feature_grad = full[here, :].astype(jnp.float32) * gain
        x = resid[here, :].astype(jnp.float32)
        scale = lax.rsqrt(jnp.mean(x * x, axis=-1, keepdims=True) + 1e-06)
        cubed = scale * scale * scale
        mean = jnp.mean(x * feature_grad, axis=-1, keepdims=True)
        value = grad_out[here, :].astype(jnp.float32) + scale * feature_grad - x * cubed * mean
        grads[here, :] = value.astype(grads.dtype)

    def crossing(k):
        return crossing_first(steps, k)

    meet(steps, True, near, far)
    for j in (far, diag, t, near):
        to_far(j).start()
    for j in (near, t, diag, far):
        to_near(j).start()
    own_copy().start()
    summed = conv_sum[...].astype(jnp.float32)
    centre = summed - jnp.mean(summed, axis=-1, keepdims=True)
    inv_std = lax.rsqrt(jnp.mean(centre * centre, axis=-1, keepdims=True) + 1e-05)
    grouped = centre * inv_std
    pre_act = grouped * conv_gain[...]
    sigma = jax.nn.sigmoid(pre_act)
    slope = sigma * (1.0 + pre_act * (1.0 - sigma)) * conv_gain[...]
    own_copy().wait()

    def arrive(j):
        to_far(j).wait_recv()
        pass_near(j).start()

    def whole(j):
        to_near(j).wait_recv()
        pass_near(j).wait_recv()

    arrive(t)
    arrive(near)
    whole(t)
    settle(t)
    looped(0, steps - 1, lambda k: spread_out(crossing(k)).start())
    arrive(far)
    arrive(diag)
    for j in (near, far, diag):
        whole(j)
        settle(j)
    feats = pl.ds(pl.multiple_of(s * feat_rows, feat_rows), feat_rows)
    feature_cols[0] = grads[:, feats].reshape(chunks, share, feat_rows)
    out_grad = jnp.dot(grads[...], proj_weight[...], preferred_element_type=jnp.float32)
    normal = out_grad * slope
    sum_grad = inv_std * (
        normal
        - jnp.mean(normal, axis=-1, keepdims=True)
        - grouped * jnp.mean(normal * grouped, axis=-1, keepdims=True)
    )
    extended[pl.ds(0, tok_rows), :] = sum_grad
    halo().start()

    def share_out(d):
        spread_out(d).wait_recv()
        x_far(d).start()
        x_near(d).start()

    def pass_on(d):
        x_far(d).wait_recv()
        x_pass(d).start()

    def both(k):
        share_out(crossing(k))
        pass_on(crossing(k - 1))

    share_out(crossing(0))
    looped(1, steps - 1, both)
    halo().wait()

    @pl.when(s == steps - 1)
    def _():
        extended[pl.ds(tok_rows, overlap + 2), :] = jnp.zeros(
            (overlap + 2, extended.shape[1]), extended.dtype
        )

    gated_grad = extended[pl.ds(overlap, tok_rows), :] * conv_taps[pl.ds(0, 1), :]
    for j in range(1, overlap + 1):
        gated_grad += extended[pl.ds(overlap - j, tok_rows), :] * conv_taps[pl.ds(j, 1), :]
    sigma_gate = jax.nn.sigmoid(conv_gate[...].astype(jnp.float32))
    value_grad[...] = (gated_grad * sigma_gate).astype(value_grad.dtype)
    gate_input_grad[...] = (
        gated_grad * conv_value[...].astype(jnp.float32) * sigma_gate * (1.0 - sigma_gate)
    ).astype(gate_input_grad.dtype)
    pass_on(crossing(steps - 2))

    def finish(k):
        d = crossing(k)
        spread_out(d).wait_send()
        x_near(d).wait()
        x_far(d).wait_send()
        x_pass(d).wait()

    looped(0, steps - 1, finish)

    def finish_gather(j):
        to_far(j).wait_send()
        to_near(j).wait_send()
        pass_near(j).wait_send()

    looped(0, chunks, finish_gather)


def settle_tokens(operands, collective_id):
    part_grad, resid, conv_sum = operands[0], operands[2], operands[5]
    overlap = operands[7].shape[0] - 1
    steps, tp_count = lax.axis_size("sp"), lax.axis_size("tp")
    tok_rows, model_width = resid.shape
    channels = conv_sum.shape[1]
    kind = resid.dtype
    outs = [
        jax.ShapeDtypeStruct((steps, tp_count, tok_rows // tp_count, model_width // steps), kind),
        jax.ShapeDtypeStruct((tok_rows, channels), kind),
        jax.ShapeDtypeStruct((tok_rows, channels), kind),
    ]
    fours = pltpu.SemaphoreType.DMA((tp_count,))
    ones = pltpu.SemaphoreType.DMA((steps,))
    single = pltpu.SemaphoreType.DMA((1,))
    return pl.pallas_call(
        functools.partial(settle_kernel, steps),
        out_shape=tuple(outs),
        in_specs=[pl.BlockSpec(memory_space=pltpu.VMEM)] * len(operands),
        out_specs=tuple(pl.BlockSpec(memory_space=pltpu.VMEM) for _ in outs),
        scratch_shapes=[
            pltpu.VMEM((tok_rows, model_width), kind),
            pltpu.VMEM((tok_rows, model_width), kind),
            pltpu.VMEM((tok_rows + overlap + 2, channels), jnp.float32),
        ]
        + [fours] * 6
        + [single]
        + [ones] * 8
        + [single] * 2,
        compiler_params=pltpu.CompilerParams(
            collective_id=collective_id, has_side_effects=True, vmem_limit_bytes=24 << 20
        ),
    )(*operands)


def last_kernel(count, feature_cols, all_out, *refs):
    ins, proj, outs, sem = refs[:count], refs[count], refs[count + 1 : -1], refs[-1]
    moves = [pltpu.make_async_copy(a, b, sem.at[i]) for i, (a, b) in enumerate(zip(ins, outs))]
    for move in moves:
        move.start()
    proj[...] = contract_rows(feature_cols[...], all_out[...])
    for move in moves:
        move.wait()


def last_stage(feature_cols, all_out, grads):
    held = [pl.BlockSpec(memory_space=pltpu.VMEM)]
    outside = [pl.BlockSpec(memory_space=pl.ANY)]
    shape = (feature_cols.shape[1], all_out.shape[1])
    outs = [jax.ShapeDtypeStruct(shape, jnp.float32)]
    outs += [jax.ShapeDtypeStruct(g.shape, g.dtype) for g in grads]
    return pl.pallas_call(
        functools.partial(last_kernel, len(grads)),
        out_shape=tuple(outs),
        in_specs=held * (2 + len(grads)),
        out_specs=tuple(held + outside * len(grads)),
        scratch_shapes=[pltpu.SemaphoreType.DMA((len(grads),))],
        compiler_params=pltpu.CompilerParams(vmem_limit_bytes=16 << 20),
    )(feature_cols, all_out, *grads)


def local(
    grad_out,
    resid,
    norm_gain,
    routes,
    route_weights,
    gate_weight,
    up_weight,
    down_weight,
    proj_weight,
    conv_sum,
    conv_gain,
    conv_taps,
    conv_value,
    conv_gate,
):
    tok_rows, model_width = resid.shape
    sp_count = lax.axis_size("sp")
    tp_count = lax.axis_size("tp")
    capacity = 3 * tok_rows // sp_count
    col_count = model_width // tp_count
    channels = conv_sum.shape[1]
    aligned = capacity % 16 == 0 and model_width % (128 * sp_count) == 0 and channels == GROUP
    if aligned and sp_count % 4 == 0:
        side_rows = (routes.T.astype(jnp.float32), route_weights.T)
        info = jnp.pad(jnp.concatenate(side_rows, axis=0), ((0, 4), (0, 0)))
        operands = (
            info,
            grad_out,
            resid,
            norm_gain[None],
            gate_weight[0],
            up_weight[0],
            down_weight[0],
            conv_sum,
            conv_gain[None],
        )
        gate_grad, up_grad, down_grad, part_grad, all_out = relay_experts(operands, 4)
        operands = (
            part_grad,
            grad_out,
            resid,
            norm_gain[None],
            proj_weight,
            conv_sum,
            conv_gain[None],
            conv_taps,
            conv_value,
            conv_gate,
        )
        feature_cols, value_grad, gate_input_grad = settle_tokens(operands, 5)
        proj_grad, *ends = last_stage(
            feature_cols.reshape(sp_count * tok_rows, model_width // sp_count),
            all_out.reshape(sp_count * tok_rows, channels),
            (gate_grad, up_grad, down_grad, value_grad, gate_input_grad),
        )
        return tuple(g[None] for g in ends[:3]) + (proj_grad,) + tuple(ends[3:])
    resid_f = resid.astype(jnp.float32)
    inv_rms = lax.rsqrt(jnp.mean(resid_f * resid_f, axis=-1, keepdims=True) + 1e-06)
    normed = (resid_f * inv_rms * norm_gain).astype(jnp.bfloat16)
    my_sp = lax.axis_index("sp")
    away = (routes - my_sp) % sp_count
    steps_away = jnp.arange(sp_count, dtype=jnp.int32)
    named = away[:, :, None] == steps_away[None, None, :]
    chosen = jnp.any(named, axis=1)
    weight_of = jnp.sum(jnp.where(named, route_weights[:, :, None], 0.0), axis=1)
    token_ids = jnp.arange(tok_rows, dtype=jnp.int32)
    earlier = (token_ids[None, :] < token_ids[:, None]).astype(jnp.bfloat16)
    rank = jnp.dot(earlier, chosen.astype(jnp.bfloat16), preferred_element_type=jnp.float32)
    rank = jnp.where(chosen, rank, -1.0).astype(jnp.int32)
    slots = jnp.arange(capacity, dtype=jnp.int32)
    held = rank.T[:, None, :] == slots[None, :, None]
    slot_weight = jnp.sum(jnp.where(held, weight_of.T[:, None, :], 0.0), axis=2)
    pick = held.astype(jnp.bfloat16).reshape(sp_count * capacity, tok_rows)
    first_col = lax.axis_index("tp") * col_count
    normed_part = lax.dynamic_slice_in_dim(normed, first_col, col_count, 1)
    cots_part = lax.dynamic_slice_in_dim(grad_out, first_col, col_count, 1)
    slot_weight = slot_weight.reshape(-1, 1)
    send_rows = jnp.dot(pick, normed_part, preferred_element_type=jnp.float32).astype(jnp.bfloat16)
    send_cots = jnp.dot(pick, cots_part, preferred_element_type=jnp.float32)
    send_cots = (send_cots * slot_weight).astype(jnp.bfloat16)
    own_pick = pick[:capacity]
    own_rows = jnp.dot(own_pick, normed, preferred_element_type=jnp.float32).astype(jnp.bfloat16)
    own_cots = jnp.dot(own_pick, grad_out, preferred_element_type=jnp.float32)
    own_cots = (own_cots * slot_weight[:capacity]).astype(jnp.bfloat16)
    summed = conv_sum.astype(jnp.float32).reshape(tok_rows, channels // GROUP, GROUP)
    centre = summed - jnp.mean(summed, axis=-1, keepdims=True)
    inv_std = lax.rsqrt(jnp.mean(centre * centre, axis=-1, keepdims=True) + 1e-05)
    grouped = centre * inv_std
    chan_normed = grouped.reshape(tok_rows, channels)
    pre_act = chan_normed * conv_gain
    sigma_conv = jax.nn.sigmoid(pre_act)
    conv_out = (pre_act * sigma_conv).astype(jnp.bfloat16)
    routed_rows, routed_cots = spread(
        (
            send_rows.reshape(sp_count, capacity, col_count),
            send_cots.reshape(sp_count, capacity, col_count),
        ),
        (own_rows, own_cots),
        None,
        True,
        False,
        0,
    )
    routed_rows = routed_rows.reshape(sp_count * capacity, model_width)
    routed_cots = routed_cots.reshape(sp_count * capacity, model_width)
    gate_grad, up_grad, down_grad, partial_value = expert_backward(
        routed_rows, routed_cots, gate_weight[0], up_weight[0], down_weight[0]
    )
    returned = combine(
        partial_value.reshape(sp_count, capacity, model_width).astype(jnp.bfloat16), 1
    ).reshape(sp_count * capacity, col_count)
    normed_part_grad = contract_rows(pick, returned).astype(jnp.bfloat16)
    chunks = 4
    normed_grad, all_out = spread(
        (normed_part_grad.reshape(chunks, tok_rows // chunks, col_count),),
        None,
        conv_out,
        True,
        False,
        2,
    )
    normed_grad = normed_grad.reshape(tok_rows, model_width)
    feature_grad = normed_grad.astype(jnp.float32) * norm_gain
    cubed = inv_rms * inv_rms * inv_rms
    resid_grad = (
        grad_out.astype(jnp.float32)
        + inv_rms * feature_grad
        - resid_f * cubed * jnp.mean(resid_f * feature_grad, axis=-1, keepdims=True)
    ).astype(jnp.bfloat16)
    share = tok_rows // tp_count
    feat_rows = model_width // sp_count
    tokens_part = lax.dynamic_slice_in_dim(resid_grad, lax.axis_index("tp") * share, share, 0)
    by_feature = tokens_part.reshape(share, sp_count, feat_rows).transpose(1, 0, 2)
    own_features = lax.dynamic_slice_in_dim(resid_grad, my_sp * feat_rows, feat_rows, 1)
    (feature_cols,) = spread(
        (by_feature,), (own_features.reshape(tp_count, share, feat_rows),), None, False, True, 3
    )
    proj_grad = contract_rows(
        feature_cols.reshape(sp_count * tok_rows, feat_rows),
        all_out.reshape(sp_count * tok_rows, channels),
    )
    out_grad = jnp.dot(resid_grad, proj_weight, preferred_element_type=jnp.float32)
    normal_grad = (
        out_grad * sigma_conv * (1.0 + pre_act * (1.0 - sigma_conv)) * conv_gain
    ).reshape(tok_rows, channels // GROUP, GROUP)
    sum_grad = inv_std * (
        normal_grad
        - jnp.mean(normal_grad, axis=-1, keepdims=True)
        - grouped * jnp.mean(normal_grad * grouped, axis=-1, keepdims=True)
    )
    sum_grad = sum_grad.reshape(tok_rows, channels)
    following = passed_along(sum_grad[: CONV_K - 1], "sp", -1)
    extended = jnp.concatenate([sum_grad, following], axis=0)
    gated_grad = lax.conv_general_dilated(
        extended[None],
        conv_taps[::-1][:, None, :],
        (1,),
        ((0, 0),),
        dimension_numbers=("NWC", "WIO", "NWC"),
        feature_group_count=channels,
        precision=lax.Precision.HIGHEST,
    )[0]
    sigma_gate = jax.nn.sigmoid(conv_gate.astype(jnp.float32))
    value_grad = (gated_grad * sigma_gate).astype(jnp.bfloat16)
    gate_input_grad = (
        gated_grad * conv_value.astype(jnp.float32) * sigma_gate * (1.0 - sigma_gate)
    ).astype(jnp.bfloat16)
    return (gate_grad[None], up_grad[None], down_grad[None], proj_grad, value_grad, gate_input_grad)


def solution(mesh):
    in_specs = (
        P("sp", None),
        P("sp", None),
        P(),
        P("sp", None),
        P("sp", None),
        P("sp", None, "tp"),
        P("sp", None, "tp"),
        P("sp", "tp", None),
        P(None, "tp"),
        P("sp", "tp"),
        P("tp"),
        P(None, "tp"),
        P("sp", "tp"),
        P("sp", "tp"),
    )
    out_specs = (
        P("sp", None, "tp"),
        P("sp", None, "tp"),
        P("sp", "tp", None),
        P("sp", "tp"),
        P("sp", "tp"),
        P("sp", "tp"),
    )
    return jax.shard_map(local, mesh=mesh, in_specs=in_specs, out_specs=out_specs, check_vma=False)
```

```python
import functools

import jax
import jax.numpy as jnp
from jax import lax
from jax.experimental import pallas as pl
from jax.experimental.pallas import tpu as pltpu
from jax.sharding import PartitionSpec as P

CONV_K = 31
GROUP = 128
MESH = pl.DeviceIdType.MESH


CLAMP_LIMIT = 7.0
SLOPE_ALPHA = 1.702


def passed_along(block, axis, distance):
    devices = range(lax.axis_size(axis))
    route = [(i - distance, i) for i in devices if i - distance in devices]
    return lax.ppermute(block, axis, route)


def tp_places():
    mine = lax.axis_index("tp")
    near = mine + 1 - 2 * (mine % 2)
    far = (mine + 2) % 4
    diag = (near + 2) % 4
    return mine, near, far, diag


def meet(steps, over_sp, near, far):
    s, t = lax.axis_index("sp"), lax.axis_index("tp")
    barrier = pltpu.get_barrier_semaphore()
    pl.semaphore_signal(barrier, inc=1, device_id=(s, near), device_id_type=MESH)
    pl.semaphore_signal(barrier, inc=1, device_id=(s, far), device_id_type=MESH)
    total = 2
    if over_sp:

        def greet(d, carry):
            pl.semaphore_signal(
                barrier, inc=1, device_id=((s + d) % steps, t), device_id_type=MESH
            )
            return carry

        lax.fori_loop(1, steps, greet, 0)
        total += steps - 1
    pl.semaphore_wait(barrier, total)


def crossing_first(steps, k):
    return steps // 2 + ((k + 1) // 2) * (2 * (k % 2) - 1)


def looped(first, last, body):
    def step(k, carry):
        body(k)
        return carry

    lax.fori_loop(first, last, step, 0)


def spread_kernel(count, steps, over_sp, in_lanes, absolute, beside, sp_count, *refs):
    refs = list(refs)
    sends, refs = refs[:count], refs[count:]
    fulls, refs = (refs[:count], refs[count:]) if over_sp else (None, refs)
    side, refs = (refs[0], refs[1:]) if beside else (None, refs)
    outs, refs = refs[:count], refs[count:]
    side_out, refs = (refs[0], refs[1:]) if beside else (None, refs)
    own_sem, a_send, a_recv, b_send, f_send, c_send, near_recv, fwd_recv, far_recv = refs[:9]
    s = lax.axis_index("sp")
    t, near, far, _ = tp_places()
    width = sends[0].shape[-1]

    def place(c, d, q):
        if in_lanes:
            return outs[c].at[d, :, pl.ds(pl.multiple_of(q * width, width), width)]
        return outs[c].at[d, q]

    def source(c, d):
        return sends[c].at[(s + d) % steps if absolute else d]

    def own(c, d):
        if over_sp:
            return pltpu.make_async_copy(fulls[c], outs[c].at[0], own_sem.at[c, 0])
        return pltpu.make_async_copy(source(c, d), place(c, d, t), own_sem.at[c, d])

    def to_sp(c, d):
        return pltpu.make_async_remote_copy(
            src_ref=source(c, d),
            dst_ref=place(c, d, t),
            send_sem=a_send.at[c, d],
            recv_sem=a_recv.at[c, d],
            device_id=((s + d) % steps, t),
            device_id_type=MESH,
        )

    def to_tp(c, d, q, target, send_sem, recv_sem):
        return pltpu.make_async_remote_copy(
            src_ref=place(c, d, q),
            dst_ref=place(c, d, q),
            send_sem=send_sem.at[c, d],
            recv_sem=recv_sem.at[c, d],
            device_id=(s, target),
            device_id_type=MESH,
        )

    def near_copy(c, d):
        return to_tp(c, d, t, near, b_send, near_recv)

    def far_copy(c, d):
        return to_tp(c, d, t, far, f_send, far_recv)

    def fwd_copy(c, d):
        return to_tp(c, d, far, near, c_send, fwd_recv)

    def side_copy(d):
        side_send, side_recv = refs[10:12]
        return pltpu.make_async_remote_copy(
            src_ref=side,
            dst_ref=side_out.at[d],
            send_sem=side_send.at[d],
            recv_sem=side_recv.at[d],
            device_id=((s + d) % sp_count, t),
            device_id_type=MESH,
        )

    def own_side():
        return pltpu.make_async_copy(side, side_out.at[0], refs[9].at[0])

    def share(c, d):
        far_copy(c, d).start()
        near_copy(c, d).start()

    def forward(c, d):
        far_copy(c, d).wait_recv()
        fwd_copy(c, d).start()

    def finish(c, d):
        near_copy(c, d).wait()
        far_copy(c, d).wait_send()
        fwd_copy(c, d).wait()

    def loop(first, last, body):
        def each(k):
            d = k + 1 if over_sp else k
            for c in range(count):
                body(c, d)

        looped(first, last, each)

    meet(sp_count, over_sp or beside, near, far)
    if over_sp:
        loop(0, steps - 1, lambda c, d: to_sp(c, d).start())
        for c in range(count):
            own(c, 0).start()

        def pass_on(k):
            for c in range(count):
                d = k + 1
                to_sp(c, d).wait_recv()
                share(c, d)

        def pass_on_twice(k):
            pass_on(k)
            for c in range(count):
                forward(c, k)

        pass_on(0)
        looped(1, steps - 1, pass_on_twice)
        loop(steps - 2, steps - 1, forward)
        loop(0, steps - 1, finish)
        loop(0, steps - 1, lambda c, d: to_sp(c, d).wait_send())
        for c in range(count):
            own(c, 0).wait()
    else:
        loop(0, steps, lambda c, d: own(c, d).start())
        if beside:
            looped(0, sp_count - 1, lambda k: side_copy(crossing_first(sp_count, k)).start())
            own_side().start()

        def share_own(c, d):
            own(c, d).wait()
            share(c, d)

        loop(0, steps, share_own)
        loop(0, steps, forward)
        loop(0, steps, finish)
        if beside:
            looped(0, sp_count - 1, lambda k: side_copy(crossing_first(sp_count, k)).wait())
            own_side().wait()


def spread(sends, fulls, side, in_lanes, absolute, collective_id):
    count = len(sends)
    steps, rows, width = sends[0].shape
    tp_count, sp_count = lax.axis_size("tp"), lax.axis_size("sp")
    over_sp, beside = fulls is not None, side is not None
    shape = (steps, rows, tp_count * width) if in_lanes else (steps, tp_count, rows, width)
    out_shape = [jax.ShapeDtypeStruct(shape, x.dtype) for x in sends]
    operands = list(sends) + (list(fulls) if over_sp else []) + ([side] if beside else [])
    scratch = [pltpu.SemaphoreType.DMA((count, steps))] * 9
    if beside:
        out_shape.append(jax.ShapeDtypeStruct((sp_count,) + side.shape, side.dtype))
        scratch += [pltpu.SemaphoreType.DMA((1,))] + [pltpu.SemaphoreType.DMA((sp_count,))] * 2
    return pl.pallas_call(
        functools.partial(
            spread_kernel, count, steps, over_sp, in_lanes, absolute, beside, sp_count
        ),
        out_shape=tuple(out_shape),
        in_specs=[pl.BlockSpec(memory_space=pltpu.VMEM)] * len(operands),
        out_specs=tuple(pl.BlockSpec(memory_space=pltpu.VMEM) for _ in out_shape),
        scratch_shapes=scratch,
        compiler_params=pltpu.CompilerParams(
            collective_id=collective_id, has_side_effects=True, vmem_limit_bytes=40 << 20
        ),
    )(*operands)


def combine_kernel(
    steps, part, out, near_in, pair, far_in, total,
    n0_send, n0_recv, n1_send, n1_recv, f_send, f_recv, a_send, a_recv,
):
    s = lax.axis_index("sp")
    t, near, far, diag = tp_places()
    width = out.shape[-1]

    def lanes(q):
        return pl.ds(pl.multiple_of(q * width, width), width)

    def near_copy(d, which, q, send_sem, recv_sem):
        return pltpu.make_async_remote_copy(
            src_ref=part.at[d, :, lanes(q)],
            dst_ref=near_in.at[which, d],
            send_sem=send_sem.at[d],
            recv_sem=recv_sem.at[d],
            device_id=(s, near),
            device_id_type=MESH,
        )

    def for_near(d):
        return near_copy(d, 0, near, n0_send, n0_recv)

    def for_diag(d):
        return near_copy(d, 1, diag, n1_send, n1_recv)

    def far_copy(d):
        return pltpu.make_async_remote_copy(
            src_ref=pair.at[d],
            dst_ref=far_in.at[d],
            send_sem=f_send.at[d],
            recv_sem=f_recv.at[d],
            device_id=(s, far),
            device_id_type=MESH,
        )

    def back(d):
        return pltpu.make_async_remote_copy(
            src_ref=total.at[d],
            dst_ref=out.at[d],
            send_sem=a_send.at[d],
            recv_sem=a_recv.at[d],
            device_id=((s + steps - d) % steps, t),
            device_id_type=MESH,
        )

    meet(steps, True, near, far)

    def open_up(d):
        for_diag(d).start()
        for_near(d).start()

    def add_pair(d):
        for_diag(d).wait_recv()
        mine = part[d, :, lanes(far)].astype(jnp.float32)
        pair[d] = (mine + near_in[1, d].astype(jnp.float32)).astype(pair.dtype)
        far_copy(d).start()

    def whole(d):
        for_near(d).wait_recv()
        far_copy(d).wait_recv()
        mine = part[d, :, lanes(t)].astype(jnp.float32)
        both = mine + near_in[0, d].astype(jnp.float32)
        return (both + far_in[d].astype(jnp.float32)).astype(out.dtype)

    def send_back(d):
        total[d] = whole(d)
        back(d).start()

    def at(k):
        return crossing_first(steps, k)

    lag = min(3, steps - 1)
    looped(0, steps - 1, lambda k: open_up(at(k)))
    open_up(0)
    looped(0, lag, lambda k: add_pair(at(k)))

    def middle(k):
        add_pair(at(k))
        send_back(at(k - lag))

    looped(lag, steps - 1, middle)
    add_pair(0)
    looped(steps - 1 - lag, steps - 1, lambda k: send_back(at(k)))
    out[0] = whole(0)

    def finish(d):
        for_near(d).wait_send()
        for_diag(d).wait_send()
        far_copy(d).wait_send()

    looped(0, steps, finish)
    looped(1, steps, lambda d: back(d).wait())


def combine(part, collective_id):
    steps, rows, all_width = part.shape
    width = all_width // lax.axis_size("tp")
    block = (steps, rows, width)
    return pl.pallas_call(
        functools.partial(combine_kernel, steps),
        out_shape=jax.ShapeDtypeStruct(block, part.dtype),
        in_specs=[pl.BlockSpec(memory_space=pltpu.VMEM)],
        out_specs=pl.BlockSpec(memory_space=pltpu.VMEM),
        scratch_shapes=[
            pltpu.VMEM((2,) + block, part.dtype),
            pltpu.VMEM(block, part.dtype),
            pltpu.VMEM(block, part.dtype),
            pltpu.VMEM(block, part.dtype),
        ]
        + [pltpu.SemaphoreType.DMA((steps,))] * 8,
        compiler_params=pltpu.CompilerParams(
            collective_id=collective_id, has_side_effects=True, vmem_limit_bytes=40 << 20
        ),
    )(part)


def contract_rows(left_side, right_side):
    return lax.dot_general(
        left_side, right_side, (((0,), (0,)), ((), ())), preferred_element_type=jnp.float32
    )


def contract_cols(left_side, right_side):
    return lax.dot_general(
        left_side, right_side, (((1,), (1,)), ((), ())), preferred_element_type=jnp.float32
    )


def expert_backward(routed_rows, routed_cots, w_gate, w_up, w_down):
    gate_pre = jnp.dot(routed_rows, w_gate, preferred_element_type=jnp.float32)
    up_pre = jnp.dot(routed_rows, w_up, preferred_element_type=jnp.float32)
    gate_clamped = jnp.minimum(gate_pre, CLAMP_LIMIT)
    up_clamped = jnp.clip(up_pre, -CLAMP_LIMIT, CLAMP_LIMIT)
    sigma = jax.nn.sigmoid(SLOPE_ALPHA * gate_clamped)
    gated = gate_clamped * sigma
    act = ((up_clamped + 1.0) * gated).astype(jnp.bfloat16)
    down_grad = contract_rows(act, routed_cots).astype(jnp.bfloat16)
    act_grad = contract_cols(routed_cots, w_down)
    inside = (up_pre > -CLAMP_LIMIT) & (up_pre < CLAMP_LIMIT)
    up_pre_grad = jnp.where(inside, act_grad * gated, 0.0).astype(jnp.bfloat16)
    slope = sigma + SLOPE_ALPHA * gate_clamped * sigma * (1.0 - sigma)
    gate_pre_grad = jnp.where(
        gate_pre < CLAMP_LIMIT, act_grad * (up_clamped + 1.0) * slope, 0.0
    ).astype(jnp.bfloat16)
    gate_grad = contract_rows(routed_rows, gate_pre_grad).astype(jnp.bfloat16)
    up_grad = contract_rows(routed_rows, up_pre_grad).astype(jnp.bfloat16)
    partial_value = contract_cols(gate_pre_grad, w_gate) + contract_cols(up_pre_grad, w_up)
    return (gate_grad, up_grad, down_grad, partial_value)


def line_schedule(line):
    codes = []
    for z in range(line):
        slots = [[(z, 0), 0, 0, 0], [(z, 1), 1, 1, 0]]
        groups = [[b for b in (z - k, z + k) if 0 <= b < line] for k in range(1, line)]
        groups = [g for g in groups if g]
        for k, group in enumerate(groups, 1):
            following = k + 1 if k < len(groups) else 0
            added = [[(b, 0), 0, 0, 0] for b in group] + [[(b, 1), 0, 0, 0] for b in group]
            many = len(group)
            added[0][3] = group[0] + 1
            if many > 1:
                added[many][3] = group[1] + 1
            added[1][1] = following
            added[many][2] = following
            slots += added
        row = []
        for (zb, col), first, second, meeting in slots:
            row.append((((meeting * 16 + second) * 16 + first) * 2 + col) * 16 + zb)
        codes.append(row)
    return codes


def relay_kernel(
    steps, routes_in, weights_in, grad_in, resid_in, gain_in, gate_in, up_in, down_in, sum_in,
    conv_gain_in,
    gate_grad, up_grad, down_grad, part_grad, side_out,
    routes, route_weights, grad_out, resid, norm_gain, w_gate, w_up, w_down, conv_sum, conv_gain,
    normed, info, infos, ranks, weights, before, picks,
    tok, over, cross, cross_far, held, act, gate_pg, up_pg, part,
    near_in, pair, far_in, total, ret, side,
    own_sem, info_send, info_recv, line_send, line_recv, end_send, cross_recv,
    across_send, afar_send, arr_recv, b_send, f_send, c_send, near_recv, fwd_recv, far_recv,
    n0_send, n0_recv, n1_send, n1_recv, g_send, g_recv, r_send, r_recv, s_send, s_recv,
):
    s = lax.axis_index("sp")
    t, near, far, diag = tp_places()
    line = steps // 2
    z, y = s // 2, s % 2
    across = s + 1 - 2 * y
    tok_rows, width = part_grad.shape
    count = cross.shape[2]
    hidden = w_gate.shape[1]
    model_width = resid.shape[1]
    both = (0, 1)
    kind = held.dtype
    sources = (grad_out, normed)

    def lanes(q):
        return pl.ds(pl.multiple_of(q * width, width), width)

    def remote(src, dst, send_sem, recv_sem, sp_to, tp_to):
        return pltpu.make_async_remote_copy(
            src_ref=src,
            dst_ref=dst,
            send_sem=send_sem,
            recv_sem=recv_sem,
            device_id=(sp_to, tp_to),
            device_id_type=MESH,
        )

    moves = [
        pltpu.make_async_copy(a, b, own_sem.at[i])
        for i, (a, b) in enumerate(
            (
                (grad_in, grad_out),
                (routes_in, routes),
                (weights_in, route_weights),
                (resid_in, resid),
                (gain_in, norm_gain),
                (sum_in, conv_sum),
                (conv_gain_in, conv_gain),
                (gate_in, w_gate),
                (up_in, w_up),
                (down_in, w_down),
            )
        )
    ]

    def info_copy(dz):
        peer = ((z + dz) % line) * 2 + y
        return remote(info, infos.at[z], info_send.at[dz], info_recv.at[z], peer, t)

    def info_from(zb):
        return remote(info, infos.at[zb], info_send.at[0], info_recv.at[zb], across, t)

    def line_copy(a, zb, src, up):
        to = s + 2 if up else s - 2
        return remote(src, tok.at[a, zb], line_send.at[a, up, zb], line_recv.at[a, zb], to, t)

    def end_copy(a, zb, col, up):
        to = s + 2 if up else s - 2
        j = 2 * zb + y
        if col == 0:
            dst, recv = held.at[a, j, :, lanes(t)], arr_recv.at[a, j]
        else:
            dst, recv = cross.at[a, zb], cross_recv.at[a, zb]
        return remote(over.at[a, zb, col], dst, end_send.at[a, col, zb], recv, to, t)

    def across_copy(a, zb):
        j = 2 * zb + y
        dst = held.at[a, j, :, lanes(t)]
        return remote(cross.at[a, zb], dst, across_send.at[a, zb], arr_recv.at[a, j], across, t)

    def across_far(a):
        dst = held.at[a, s, :, lanes(far)]
        return remote(cross_far.at[a], dst, afar_send.at[a], far_recv.at[a, s], across, t)

    def arrival(a, j):
        place = held.at[a, j, :, lanes(t)]
        return remote(place, place, f_send.at[a, j], arr_recv.at[a, j], s, far)

    def to_tp(a, j, q, target, send_sem, recv_sem):
        place = held.at[a, j, :, lanes(q)]
        return remote(place, place, send_sem.at[a, j], recv_sem.at[a, j], s, target)

    def near_copy(a, j):
        return to_tp(a, j, t, near, b_send, near_recv)

    def far_copy(a, j):
        return to_tp(a, j, t, far, f_send, far_recv)

    def fwd_copy(a, j):
        return to_tp(a, j, far, near, c_send, fwd_recv)

    def part_copy(j, which, q, send_sem, recv_sem):
        src, dst = part.at[j, :, lanes(q)], near_in.at[which, j]
        return remote(src, dst, send_sem.at[j], recv_sem.at[j], s, near)

    def for_near(j):
        return part_copy(j, 0, near, n0_send, n0_recv)

    def for_diag(j):
        return part_copy(j, 1, diag, n1_send, n1_recv)

    def pair_copy(j):
        return remote(pair.at[j], far_in.at[j], g_send.at[j], g_recv.at[j], s, far)

    def back(j):
        return remote(total.at[j], ret.at[s], r_send.at[j], r_recv.at[s], j, t)

    def back_from(e):
        return remote(total.at[e], ret.at[e], r_send.at[e], r_recv.at[e], e, t)

    def side_copy(d):
        to = (s + d) % steps
        return remote(side, side_out.at[d], s_send.at[d], s_recv.at[d], to, t)

    def table(zb):
        first, second = infos[zb, pl.ds(0, 1), :], infos[zb, pl.ds(1, 1), :]
        ids = lax.broadcasted_iota(jnp.int32, (steps, tok_rows), 0).astype(jnp.float32)
        chosen = (first == ids) | (second == ids)
        ones = jnp.where(chosen, 1.0, 0.0).astype(kind)
        rank = jnp.dot(ones, before[...], preferred_element_type=jnp.float32)
        ranks[zb] = jnp.where(chosen, rank, -1.0)
        weights[zb] = jnp.where(
            first == ids, infos[zb, pl.ds(2, 1), :], infos[zb, pl.ds(3, 1), :]
        )

    def pick(zb, e):
        slots = lax.broadcasted_iota(jnp.int32, (count, tok_rows), 0).astype(jnp.float32)
        return slots == ranks[zb, pl.ds(e, 1), :]

    def selected(a, zb, e, value):
        mask = pick(zb, e)
        hot = jnp.where(mask, 1.0, 0.0).astype(kind)
        out = jnp.dot(hot, value, preferred_element_type=jnp.float32)
        if a == 0:
            scale = jnp.where(mask, weights[zb, pl.ds(e, 1), :], 0.0)
            out = out * jnp.sum(scale, axis=1, keepdims=True)
        return out.astype(kind)

    def to_end(a, zb, value, up):
        end = z + 1 if up else z - 1
        for col in both:
            e = 2 * end + (y if col == 0 else 1 - y)
            over[a, zb, col] = selected(a, zb, e, value)
            end_copy(a, zb, col, up).start()

    def valid(m, up):
        return (z >= m) if up else (z + m < line)

    def block_at(m, up):
        return z - m if up else z + m

    def next_is_end(up):
        return (z + 1 == line - 1) if up else (z == 1)

    def next_is_inner(up):
        return (z + 1 < line - 1) if up else (z >= 2)

    def at_end(up):
        return (z == line - 1) if up else (z == 0)

    def share(a, j):
        far_copy(a, j).start()
        near_copy(a, j).start()

    def read_info(m, up):
        zb = block_at(m, up)

        @pl.when(valid(m, up))
        def _():
            info_from(zb).wait_recv()

        @pl.when(valid(m, up) & jnp.logical_not(at_end(up)))
        def _():
            table(zb)

    def handle(a, m, up):
        zb = block_at(m, up)
        j = 2 * zb + y

        @pl.when(valid(m, up) & at_end(up))
        def _():
            arrival(a, j).wait_recv()
            end_copy(a, zb, 1, up).wait_recv()
            across_copy(a, zb).start()
            share(a, j)

        @pl.when(valid(m, up) & jnp.logical_not(at_end(up)))
        def _():
            line_copy(a, zb, tok.at[a, zb], up).wait_recv()

            @pl.when(next_is_end(up))
            def _():
                to_end(a, zb, tok[a, zb], up)

            @pl.when(next_is_inner(up))
            def _():
                line_copy(a, zb, tok.at[a, zb], up).start()

            cross[a, zb] = selected(a, zb, across, tok[a, zb])
            across_copy(a, zb).start()
            held[a, j, :, lanes(t)] = selected(a, zb, s, tok[a, zb])
            share(a, j)

    def unless_own(j, body):
        @pl.when(j != s)
        def _():
            body()

    def experts(j):
        def settle():
            for a in both:
                near_copy(a, j).wait_recv()
                fwd_copy(a, j).wait_recv()

        unless_own(j, settle)
        gate_pre = jnp.dot(held[1, j], w_gate[...], preferred_element_type=jnp.float32)
        up_pre = jnp.dot(held[1, j], w_up[...], preferred_element_type=jnp.float32)
        act_grad = contract_cols(held[0, j], w_down[...])
        gate_clamped = jnp.minimum(gate_pre, CLAMP_LIMIT)
        up_clamped = jnp.clip(up_pre, -CLAMP_LIMIT, CLAMP_LIMIT)
        sigma = jax.nn.sigmoid(SLOPE_ALPHA * gate_clamped)
        gated = gate_clamped * sigma
        act[j] = ((up_clamped + 1.0) * gated).astype(kind)
        inside = (up_pre > -CLAMP_LIMIT) & (up_pre < CLAMP_LIMIT)
        up_g = jnp.where(inside, act_grad * gated, 0.0).astype(kind)
        slope = sigma + SLOPE_ALPHA * gate_clamped * sigma * (1.0 - sigma)
        gate_g = jnp.where(
            gate_pre < CLAMP_LIMIT, act_grad * (up_clamped + 1.0) * slope, 0.0
        ).astype(kind)
        gate_pg[j] = gate_g
        up_pg[j] = up_g
        for q in range(model_width // width):
            mine = pl.ds(q * width, width)
            value = contract_cols(gate_g, w_gate[mine, :]) + contract_cols(up_g, w_up[mine, :])
            part[j, :, mine] = value.astype(kind)
        for_diag(j).start()
        for_near(j).start()

    def add_pair(j):
        for_diag(j).wait_recv()
        mine = part[j, :, lanes(far)].astype(jnp.float32)
        pair[j] = (mine + near_in[1, j].astype(jnp.float32)).astype(kind)
        pair_copy(j).start()

    def whole(j):
        for_near(j).wait_recv()
        pair_copy(j).wait_recv()
        mine = part[j, :, lanes(t)].astype(jnp.float32)
        summed = mine + near_in[0, j].astype(jnp.float32)
        return (summed + far_in[j].astype(jnp.float32)).astype(kind)

    def send_back(j):
        @pl.when(j == s)
        def _():
            ret[s] = whole(j)

        @pl.when(j != s)
        def _():
            total[j] = whole(j)
            back(j).start()

    def forward(j):
        def run():
            for a in both:
                far_copy(a, j).wait_recv()
                fwd_copy(a, j).start()

        unless_own(j, run)

    def flat(value):
        return value.reshape(-1, value.shape[-1])

    def row_grads(k):
        cols = pl.ds(pl.multiple_of(k * 256, 256), 256)
        left = flat(held[1, :, :, cols])
        gate_grad[cols, :] = contract_rows(left, flat(gate_pg[...])).astype(kind)
        up_grad[cols, :] = contract_rows(left, flat(up_pg[...])).astype(kind)

    def act_grads(k):
        cols = pl.ds(pl.multiple_of(k * 512, 512), 512)
        down_grad[:, cols] = contract_rows(flat(act[...]), flat(held[0, :, :, cols])).astype(kind)

    for move in moves:
        move.start()
    meet(steps, True, near, far)
    moves[0].wait()

    def start_own(a):
        src = sources[a]
        for up in both:

            @pl.when(next_is_inner(up))
            def _():
                line_copy(a, z, src.at[:, lanes(t)], up).start()

    def end_own(a):
        for up in both:

            @pl.when(next_is_end(up))
            def _():
                to_end(a, z, sources[a][:, lanes(t)], up)

    start_own(0)
    moves[1].wait()
    moves[2].wait()
    info[pl.ds(0, 2), :] = routes[...].astype(jnp.float32)
    info[pl.ds(2, 2), :] = route_weights[...]
    infos[z] = info[...]
    looped(1, line, lambda dz: info_copy(dz).start())
    row_ids = lax.broadcasted_iota(jnp.int32, (tok_rows, tok_rows), 0)
    col_ids = lax.broadcasted_iota(jnp.int32, (tok_rows, tok_rows), 1)
    before[...] = jnp.where(row_ids < col_ids, 1.0, 0.0).astype(kind)
    table(z)
    end_own(0)
    for move in moves[3:5]:
        move.wait()
    gain = norm_gain[...]

    def normalise(k):
        here = pl.ds(pl.multiple_of(k * 32, 32), 32)
        x = resid[here, :].astype(jnp.float32)
        scale = lax.rsqrt(jnp.mean(x * x, axis=-1, keepdims=True) + 1e-06)
        normed[here, :] = (x * scale * gain).astype(kind)

    looped(0, tok_rows // 32, normalise)
    start_own(1)
    end_own(1)
    for a in both:
        cross[a, z] = selected(a, z, across, sources[a][:, lanes(t)])
        across_copy(a, z).start()
        cross_far[a] = selected(a, z, across, sources[a][:, lanes(far)])
        across_far(a).start()

    def own_chunk(q):
        for a in both:
            held[a, s, :, lanes(q)] = selected(a, z, s, sources[a][:, lanes(q)])

    looped(0, model_width // width, own_chunk)
    for move in moves[5:7]:
        move.wait()
    summed = conv_sum[...].astype(jnp.float32)
    centre = summed - jnp.mean(summed, axis=-1, keepdims=True)
    inv_std = lax.rsqrt(jnp.mean(centre * centre, axis=-1, keepdims=True) + 1e-05)
    pre_act = centre * inv_std * conv_gain[...]
    conv_out = (pre_act * jax.nn.sigmoid(pre_act)).astype(kind)
    side[...] = conv_out
    side_out[0] = conv_out

    def own_picks(e):
        picks[e] = jnp.where(pick(z, e), 1.0, 0.0).astype(kind)

    looped(0, steps, own_picks)
    for move in moves[7:]:
        move.wait()

    codes = line_schedule(line)
    middle = steps // 2

    def slot_code(n):
        code = 0
        for zz in range(line):
            for nn in range(steps):
                code = code + jnp.where((z == zz) & (n == nn), codes[zz][nn], 0)
        return code

    def chunk_at(n):
        code = slot_code(n)
        other = (code // 16) % 2
        return 2 * (code % 16) + y + other * (1 - 2 * y)

    def slot(n):
        code = slot_code(n)
        zb, other = code % 16, (code // 16) % 2
        first, second = (code // 32) % 16, (code // 512) % 16
        meeting = code // 8192
        j = 2 * zb + y + other * (1 - 2 * y)

        @pl.when(meeting > 0)
        def _():
            met = 2 * (meeting - 1) + 1 - y
            for a in both:
                arrival(a, met).wait_recv()
                share(a, met)

        @pl.when(first > 0)
        def _():
            for up in both:
                read_info(first, up)
            for up in both:
                handle(0, first, up)

        @pl.when(second > 0)
        def _():
            for up in both:
                handle(1, second, up)

        @pl.when(n == 1)
        def _():
            for a in both:
                arrival(a, j).wait_recv()
                near_copy(a, j).start()

        @pl.when(n == steps - 2)
        def _():
            looped(1, steps, lambda d: side_copy(d).start())

        forward(j)
        experts(j)

        @pl.when(n == 0)
        def _():
            add_pair(j)

        @pl.when(n > middle)
        def _():
            add_pair(chunk_at(n - 1))

    def pair_at(n):
        add_pair(chunk_at(n))

    def back_at(n):
        send_back(chunk_at(n))

    looped(0, steps, slot)
    half = model_width // 512
    pair_at(steps - 1)
    looped(1, middle, pair_at)
    looped(middle, steps - 2, back_at)
    looped(0, half, row_grads)
    back_at(steps - 2)
    looped(half, 2 * half, row_grads)
    back_at(steps - 1)
    looped(0, half, act_grads)
    looped(1, middle, back_at)
    back_at(0)

    def gather_back(d):
        back_from((s + d) % steps).wait_recv()

    looped(1, steps, gather_back)
    part_grad[...] = contract_rows(flat(picks[...]), flat(ret[...])).astype(kind)

    def finish(j):
        for_near(j).wait_send()
        for_diag(j).wait_send()
        pair_copy(j).wait_send()

        @pl.when(j != s)
        def _():
            back(j).wait_send()
            for a in both:
                near_copy(a, j).wait_send()
                fwd_copy(a, j).wait_send()

        @pl.when(j // 2 != z)
        def _():
            for a in both:
                far_copy(a, j).wait_send()

    looped(0, steps, finish)

    def finish_side(d):
        side_copy(d).wait()

    looped(1, steps, finish_side)
    looped(1, line, lambda dz: info_copy(dz).wait_send())

    def finish_line(m):
        for up in both:
            zb = block_at(m, up)

            @pl.when(valid(m, up) & next_is_inner(up))
            def _():
                for a in both:
                    line_copy(a, zb, tok.at[a, zb], up).wait_send()

            @pl.when(valid(m, up) & next_is_end(up))
            def _():
                for a in both:
                    for col in both:
                        end_copy(a, zb, col, up).wait_send()

    looped(0, line, finish_line)

    def finish_across(zb):
        for a in both:
            across_copy(a, zb).wait_send()

    looped(0, line, finish_across)
    for a in both:
        across_far(a).wait_send()


def relay_experts(operands, collective_id):
    routes, resid, w_gate, conv_sum = operands[0], operands[3], operands[5], operands[8]
    steps, tp_count = lax.axis_size("sp"), lax.axis_size("tp")
    line = steps // 2
    tok_rows, model_width = resid.shape
    count = 3 * tok_rows // steps
    width = model_width // tp_count
    hidden = w_gate.shape[1]
    kind = resid.dtype
    block = (steps, count, width)
    outs = [
        jax.ShapeDtypeStruct((model_width, hidden), kind),
        jax.ShapeDtypeStruct((model_width, hidden), kind),
        jax.ShapeDtypeStruct((hidden, model_width), kind),
        jax.ShapeDtypeStruct((tok_rows, width), kind),
        jax.ShapeDtypeStruct((steps,) + conv_sum.shape, kind),
    ]
    held = pl.BlockSpec(memory_space=pltpu.VMEM)
    outside = pl.BlockSpec(memory_space=pltpu.HBM)

    def sems(*shape):
        return pltpu.SemaphoreType.DMA(shape)

    return pl.pallas_call(
        functools.partial(relay_kernel, steps),
        out_shape=tuple(outs),
        in_specs=[outside] * len(operands),
        out_specs=tuple(held for _ in outs),
        scratch_shapes=[pltpu.VMEM(x.shape, x.dtype) for x in operands]
        + [
            pltpu.VMEM((tok_rows, model_width), kind),
            pltpu.VMEM((2 * routes.shape[0], tok_rows), jnp.float32),
            pltpu.VMEM((line, 2 * routes.shape[0], tok_rows), jnp.float32),
            pltpu.VMEM((line, steps, tok_rows), jnp.float32),
            pltpu.VMEM((line, steps, tok_rows), jnp.float32),
            pltpu.VMEM((tok_rows, tok_rows), kind),
            pltpu.VMEM((steps, count, tok_rows), kind),
            pltpu.VMEM((2, line, tok_rows, width), kind),
            pltpu.VMEM((2, line, 2, count, width), kind),
            pltpu.VMEM((2, line, count, width), kind),
            pltpu.VMEM((2, count, width), kind),
            pltpu.VMEM((2, steps, count, model_width), kind),
        ]
        + [pltpu.VMEM((steps, count, hidden), kind)] * 3
        + [pltpu.VMEM((steps, count, model_width), kind), pltpu.VMEM((2,) + block, kind)]
        + [pltpu.VMEM(block, kind)] * 4
        + [pltpu.VMEM(conv_sum.shape, kind)]
        + [sems(len(operands)), sems(line), sems(line), sems(2, 2, line), sems(2, line), sems(2, 2, line)]
        + [sems(2, line), sems(2, line), sems(2), sems(2, steps)]
        + [sems(2, steps)] * 6
        + [sems(steps)] * 10,
        compiler_params=pltpu.CompilerParams(
            collective_id=collective_id, has_side_effects=True, vmem_limit_bytes=42 << 20
        ),
    )(*(pltpu.with_memory_space_constraint(x, pltpu.HBM) for x in operands))


def settle_kernel(
    steps, part_grad, grad_out, resid, norm_gain, proj_weight,
    conv_sum, conv_gain, conv_taps, conv_value, conv_gate,
    feature_cols, value_grad, gate_input_grad,
    full, grads, extended, far_send, far_recv, near_send, near_recv, fwd_send, fwd_recv,
    own_sem, x_send, x_recv, xf_send, xf_recv, xn_send, xn_recv, xw_send, xw_recv,
    h_send, h_recv,
):
    s = lax.axis_index("sp")
    t, near, far, diag = tp_places()
    tok_rows, width = part_grad.shape
    chunks, share = feature_cols.shape[1], feature_cols.shape[2]
    feat_rows = feature_cols.shape[3]
    overlap = conv_taps.shape[0] - 1

    def rows_of(j):
        return pl.ds(pl.multiple_of(j * share, share), share)

    def lanes(q):
        return pl.ds(pl.multiple_of(q * width, width), width)

    def mine_at(j):
        return full.at[rows_of(j), lanes(t)]

    def own_copy():
        return pltpu.make_async_copy(part_grad, full.at[:, lanes(t)], own_sem.at[0])

    def gather(j, q, src, target, send_sem, recv_sem):
        return pltpu.make_async_remote_copy(
            src_ref=src,
            dst_ref=full.at[rows_of(j), lanes(q)],
            send_sem=send_sem.at[j],
            recv_sem=recv_sem.at[j],
            device_id=(s, target),
            device_id_type=MESH,
        )

    def to_far(j):
        return gather(j, t, part_grad.at[rows_of(j), :], far, far_send, far_recv)

    def to_near(j):
        return gather(j, t, part_grad.at[rows_of(j), :], near, near_send, near_recv)

    def pass_near(j):
        return gather(j, far, full.at[rows_of(j), lanes(far)], near, fwd_send, fwd_recv)

    def spread_out(d):
        feats = pl.ds(pl.multiple_of(((s + d) % steps) * feat_rows, feat_rows), feat_rows)
        return pltpu.make_async_remote_copy(
            src_ref=grads.at[rows_of(t), feats],
            dst_ref=feature_cols.at[d, t],
            send_sem=x_send.at[d],
            recv_sem=x_recv.at[d],
            device_id=((s + d) % steps, t),
            device_id_type=MESH,
        )

    def beside(d, q, target, send_sem, recv_sem):
        return pltpu.make_async_remote_copy(
            src_ref=feature_cols.at[d, q],
            dst_ref=feature_cols.at[d, q],
            send_sem=send_sem.at[d],
            recv_sem=recv_sem.at[d],
            device_id=(s, target),
            device_id_type=MESH,
        )

    def x_far(d):
        return beside(d, t, far, xf_send, xf_recv)

    def x_near(d):
        return beside(d, t, near, xn_send, xn_recv)

    def x_pass(d):
        return beside(d, far, near, xw_send, xw_recv)

    def halo():
        return pltpu.make_async_remote_copy(
            src_ref=extended.at[pl.ds(0, overlap + 2)],
            dst_ref=extended.at[pl.ds(tok_rows, overlap + 2)],
            send_sem=h_send.at[0],
            recv_sem=h_recv.at[0],
            device_id=((s + steps - 1) % steps, t),
            device_id_type=MESH,
        )

    gain = norm_gain[...]

    def settle(j):
        here = rows_of(j)
        feature_grad = full[here, :].astype(jnp.float32) * gain
        x = resid[here, :].astype(jnp.float32)
        scale = lax.rsqrt(jnp.mean(x * x, axis=-1, keepdims=True) + 1e-06)
        cubed = scale * scale * scale
        mean = jnp.mean(x * feature_grad, axis=-1, keepdims=True)
        value = grad_out[here, :].astype(jnp.float32) + scale * feature_grad - x * cubed * mean
        grads[here, :] = value.astype(grads.dtype)

    def crossing(k):
        return crossing_first(steps, k)

    meet(steps, True, near, far)
    for j in (far, diag, t, near):
        to_far(j).start()
    for j in (near, t, diag, far):
        to_near(j).start()
    own_copy().start()
    summed = conv_sum[...].astype(jnp.float32)
    centre = summed - jnp.mean(summed, axis=-1, keepdims=True)
    inv_std = lax.rsqrt(jnp.mean(centre * centre, axis=-1, keepdims=True) + 1e-05)
    grouped = centre * inv_std
    pre_act = grouped * conv_gain[...]
    sigma = jax.nn.sigmoid(pre_act)
    slope = sigma * (1.0 + pre_act * (1.0 - sigma)) * conv_gain[...]
    own_copy().wait()

    def arrive(j):
        to_far(j).wait_recv()
        pass_near(j).start()

    def whole(j):
        to_near(j).wait_recv()
        pass_near(j).wait_recv()

    arrive(t)
    arrive(near)
    whole(t)
    settle(t)
    looped(0, steps - 1, lambda k: spread_out(crossing(k)).start())
    arrive(far)
    arrive(diag)
    for j in (near, far, diag):
        whole(j)
        settle(j)
    feats = pl.ds(pl.multiple_of(s * feat_rows, feat_rows), feat_rows)
    feature_cols[0] = grads[:, feats].reshape(chunks, share, feat_rows)
    out_grad = jnp.dot(grads[...], proj_weight[...], preferred_element_type=jnp.float32)
    normal = out_grad * slope
    sum_grad = inv_std * (
        normal
        - jnp.mean(normal, axis=-1, keepdims=True)
        - grouped * jnp.mean(normal * grouped, axis=-1, keepdims=True)
    )
    extended[pl.ds(0, tok_rows), :] = sum_grad
    halo().start()

    def share_out(d):
        spread_out(d).wait_recv()
        x_far(d).start()
        x_near(d).start()

    def pass_on(d):
        x_far(d).wait_recv()
        x_pass(d).start()

    def both(k):
        share_out(crossing(k))
        pass_on(crossing(k - 1))

    share_out(crossing(0))
    looped(1, steps - 1, both)
    halo().wait()

    @pl.when(s == steps - 1)
    def _():
        extended[pl.ds(tok_rows, overlap + 2), :] = jnp.zeros(
            (overlap + 2, extended.shape[1]), extended.dtype
        )

    gated_grad = extended[pl.ds(overlap, tok_rows), :] * conv_taps[pl.ds(0, 1), :]
    for j in range(1, overlap + 1):
        gated_grad += extended[pl.ds(overlap - j, tok_rows), :] * conv_taps[pl.ds(j, 1), :]
    sigma_gate = jax.nn.sigmoid(conv_gate[...].astype(jnp.float32))
    value_grad[...] = (gated_grad * sigma_gate).astype(value_grad.dtype)
    gate_input_grad[...] = (
        gated_grad * conv_value[...].astype(jnp.float32) * sigma_gate * (1.0 - sigma_gate)
    ).astype(gate_input_grad.dtype)
    pass_on(crossing(steps - 2))

    def finish(k):
        d = crossing(k)
        spread_out(d).wait_send()
        x_near(d).wait()
        x_far(d).wait_send()
        x_pass(d).wait()

    looped(0, steps - 1, finish)

    def finish_gather(j):
        to_far(j).wait_send()
        to_near(j).wait_send()
        pass_near(j).wait_send()

    looped(0, chunks, finish_gather)


def settle_tokens(operands, collective_id):
    part_grad, resid, conv_sum = operands[0], operands[2], operands[5]
    overlap = operands[7].shape[0] - 1
    steps, tp_count = lax.axis_size("sp"), lax.axis_size("tp")
    tok_rows, model_width = resid.shape
    channels = conv_sum.shape[1]
    kind = resid.dtype
    outs = [
        jax.ShapeDtypeStruct((steps, tp_count, tok_rows // tp_count, model_width // steps), kind),
        jax.ShapeDtypeStruct((tok_rows, channels), kind),
        jax.ShapeDtypeStruct((tok_rows, channels), kind),
    ]
    fours = pltpu.SemaphoreType.DMA((tp_count,))
    ones = pltpu.SemaphoreType.DMA((steps,))
    single = pltpu.SemaphoreType.DMA((1,))
    return pl.pallas_call(
        functools.partial(settle_kernel, steps),
        out_shape=tuple(outs),
        in_specs=[pl.BlockSpec(memory_space=pltpu.VMEM)] * len(operands),
        out_specs=tuple(pl.BlockSpec(memory_space=pltpu.VMEM) for _ in outs),
        scratch_shapes=[
            pltpu.VMEM((tok_rows, model_width), kind),
            pltpu.VMEM((tok_rows, model_width), kind),
            pltpu.VMEM((tok_rows + overlap + 2, channels), jnp.float32),
        ]
        + [fours] * 6
        + [single]
        + [ones] * 8
        + [single] * 2,
        compiler_params=pltpu.CompilerParams(
            collective_id=collective_id, has_side_effects=True, vmem_limit_bytes=24 << 20
        ),
    )(*operands)


def last_kernel(count, feature_cols, all_out, *refs):
    ins, proj, outs, sem = refs[:count], refs[count], refs[count + 1 : -1], refs[-1]
    moves = [pltpu.make_async_copy(a, b, sem.at[i]) for i, (a, b) in enumerate(zip(ins, outs))]
    for move in moves:
        move.start()
    proj[...] = contract_rows(feature_cols[...], all_out[...])
    for move in moves:
        move.wait()


def last_stage(feature_cols, all_out, grads):
    held = [pl.BlockSpec(memory_space=pltpu.VMEM)]
    outside = [pl.BlockSpec(memory_space=pl.ANY)]
    shape = (feature_cols.shape[1], all_out.shape[1])
    outs = [jax.ShapeDtypeStruct(shape, jnp.float32)]
    outs += [jax.ShapeDtypeStruct(g.shape, g.dtype) for g in grads]
    return pl.pallas_call(
        functools.partial(last_kernel, len(grads)),
        out_shape=tuple(outs),
        in_specs=held * (2 + len(grads)),
        out_specs=tuple(held + outside * len(grads)),
        scratch_shapes=[pltpu.SemaphoreType.DMA((len(grads),))],
        compiler_params=pltpu.CompilerParams(vmem_limit_bytes=16 << 20),
    )(feature_cols, all_out, *grads)


def local(
    grad_out,
    resid,
    norm_gain,
    routes,
    route_weights,
    gate_weight,
    up_weight,
    down_weight,
    proj_weight,
    conv_sum,
    conv_gain,
    conv_taps,
    conv_value,
    conv_gate,
):
    tok_rows, model_width = resid.shape
    sp_count = lax.axis_size("sp")
    tp_count = lax.axis_size("tp")
    capacity = 3 * tok_rows // sp_count
    col_count = model_width // tp_count
    channels = conv_sum.shape[1]
    aligned = capacity % 16 == 0 and model_width % (128 * sp_count) == 0 and channels == GROUP
    if aligned and sp_count % 4 == 0:
        operands = (
            routes.T,
            route_weights.T,
            grad_out,
            resid,
            norm_gain[None],
            gate_weight[0],
            up_weight[0],
            down_weight[0],
            conv_sum,
            conv_gain[None],
        )
        gate_grad, up_grad, down_grad, part_grad, all_out = relay_experts(operands, 4)
        operands = (
            part_grad,
            grad_out,
            resid,
            norm_gain[None],
            proj_weight,
            conv_sum,
            conv_gain[None],
            conv_taps,
            conv_value,
            conv_gate,
        )
        feature_cols, value_grad, gate_input_grad = settle_tokens(operands, 5)
        proj_grad, *ends = last_stage(
            feature_cols.reshape(sp_count * tok_rows, model_width // sp_count),
            all_out.reshape(sp_count * tok_rows, channels),
            (gate_grad, up_grad, down_grad, value_grad, gate_input_grad),
        )
        return tuple(g[None] for g in ends[:3]) + (proj_grad,) + tuple(ends[3:])
    resid_f = resid.astype(jnp.float32)
    inv_rms = lax.rsqrt(jnp.mean(resid_f * resid_f, axis=-1, keepdims=True) + 1e-06)
    normed = (resid_f * inv_rms * norm_gain).astype(jnp.bfloat16)
    my_sp = lax.axis_index("sp")
    away = (routes - my_sp) % sp_count
    steps_away = jnp.arange(sp_count, dtype=jnp.int32)
    named = away[:, :, None] == steps_away[None, None, :]
    chosen = jnp.any(named, axis=1)
    weight_of = jnp.sum(jnp.where(named, route_weights[:, :, None], 0.0), axis=1)
    token_ids = jnp.arange(tok_rows, dtype=jnp.int32)
    earlier = (token_ids[None, :] < token_ids[:, None]).astype(jnp.bfloat16)
    rank = jnp.dot(earlier, chosen.astype(jnp.bfloat16), preferred_element_type=jnp.float32)
    rank = jnp.where(chosen, rank, -1.0).astype(jnp.int32)
    slots = jnp.arange(capacity, dtype=jnp.int32)
    held = rank.T[:, None, :] == slots[None, :, None]
    slot_weight = jnp.sum(jnp.where(held, weight_of.T[:, None, :], 0.0), axis=2)
    pick = held.astype(jnp.bfloat16).reshape(sp_count * capacity, tok_rows)
    first_col = lax.axis_index("tp") * col_count
    normed_part = lax.dynamic_slice_in_dim(normed, first_col, col_count, 1)
    cots_part = lax.dynamic_slice_in_dim(grad_out, first_col, col_count, 1)
    slot_weight = slot_weight.reshape(-1, 1)
    send_rows = jnp.dot(pick, normed_part, preferred_element_type=jnp.float32).astype(jnp.bfloat16)
    send_cots = jnp.dot(pick, cots_part, preferred_element_type=jnp.float32)
    send_cots = (send_cots * slot_weight).astype(jnp.bfloat16)
    own_pick = pick[:capacity]
    own_rows = jnp.dot(own_pick, normed, preferred_element_type=jnp.float32).astype(jnp.bfloat16)
    own_cots = jnp.dot(own_pick, grad_out, preferred_element_type=jnp.float32)
    own_cots = (own_cots * slot_weight[:capacity]).astype(jnp.bfloat16)
    summed = conv_sum.astype(jnp.float32).reshape(tok_rows, channels // GROUP, GROUP)
    centre = summed - jnp.mean(summed, axis=-1, keepdims=True)
    inv_std = lax.rsqrt(jnp.mean(centre * centre, axis=-1, keepdims=True) + 1e-05)
    grouped = centre * inv_std
    chan_normed = grouped.reshape(tok_rows, channels)
    pre_act = chan_normed * conv_gain
    sigma_conv = jax.nn.sigmoid(pre_act)
    conv_out = (pre_act * sigma_conv).astype(jnp.bfloat16)
    routed_rows, routed_cots = spread(
        (
            send_rows.reshape(sp_count, capacity, col_count),
            send_cots.reshape(sp_count, capacity, col_count),
        ),
        (own_rows, own_cots),
        None,
        True,
        False,
        0,
    )
    routed_rows = routed_rows.reshape(sp_count * capacity, model_width)
    routed_cots = routed_cots.reshape(sp_count * capacity, model_width)
    gate_grad, up_grad, down_grad, partial_value = expert_backward(
        routed_rows, routed_cots, gate_weight[0], up_weight[0], down_weight[0]
    )
    returned = combine(
        partial_value.reshape(sp_count, capacity, model_width).astype(jnp.bfloat16), 1
    ).reshape(sp_count * capacity, col_count)
    normed_part_grad = contract_rows(pick, returned).astype(jnp.bfloat16)
    chunks = 4
    normed_grad, all_out = spread(
        (normed_part_grad.reshape(chunks, tok_rows // chunks, col_count),),
        None,
        conv_out,
        True,
        False,
        2,
    )
    normed_grad = normed_grad.reshape(tok_rows, model_width)
    feature_grad = normed_grad.astype(jnp.float32) * norm_gain
    cubed = inv_rms * inv_rms * inv_rms
    resid_grad = (
        grad_out.astype(jnp.float32)
        + inv_rms * feature_grad
        - resid_f * cubed * jnp.mean(resid_f * feature_grad, axis=-1, keepdims=True)
    ).astype(jnp.bfloat16)
    share = tok_rows // tp_count
    feat_rows = model_width // sp_count
    tokens_part = lax.dynamic_slice_in_dim(resid_grad, lax.axis_index("tp") * share, share, 0)
    by_feature = tokens_part.reshape(share, sp_count, feat_rows).transpose(1, 0, 2)
    own_features = lax.dynamic_slice_in_dim(resid_grad, my_sp * feat_rows, feat_rows, 1)
    (feature_cols,) = spread(
        (by_feature,), (own_features.reshape(tp_count, share, feat_rows),), None, False, True, 3
    )
    proj_grad = contract_rows(
        feature_cols.reshape(sp_count * tok_rows, feat_rows),
        all_out.reshape(sp_count * tok_rows, channels),
    )
    out_grad = jnp.dot(resid_grad, proj_weight, preferred_element_type=jnp.float32)
    normal_grad = (
        out_grad * sigma_conv * (1.0 + pre_act * (1.0 - sigma_conv)) * conv_gain
    ).reshape(tok_rows, channels // GROUP, GROUP)
    sum_grad = inv_std * (
        normal_grad
        - jnp.mean(normal_grad, axis=-1, keepdims=True)
        - grouped * jnp.mean(normal_grad * grouped, axis=-1, keepdims=True)
    )
    sum_grad = sum_grad.reshape(tok_rows, channels)
    following = passed_along(sum_grad[: CONV_K - 1], "sp", -1)
    extended = jnp.concatenate([sum_grad, following], axis=0)
    gated_grad = lax.conv_general_dilated(
        extended[None],
        conv_taps[::-1][:, None, :],
        (1,),
        ((0, 0),),
        dimension_numbers=("NWC", "WIO", "NWC"),
        feature_group_count=channels,
        precision=lax.Precision.HIGHEST,
    )[0]
    sigma_gate = jax.nn.sigmoid(conv_gate.astype(jnp.float32))
    value_grad = (gated_grad * sigma_gate).astype(jnp.bfloat16)
    gate_input_grad = (
        gated_grad * conv_value.astype(jnp.float32) * sigma_gate * (1.0 - sigma_gate)
    ).astype(jnp.bfloat16)
    return (gate_grad[None], up_grad[None], down_grad[None], proj_grad, value_grad, gate_input_grad)


def solution(mesh):
    in_specs = (
        P("sp", None),
        P("sp", None),
        P(),
        P("sp", None),
        P("sp", None),
        P("sp", None, "tp"),
        P("sp", None, "tp"),
        P("sp", "tp", None),
        P(None, "tp"),
        P("sp", "tp"),
        P("tp"),
        P(None, "tp"),
        P("sp", "tp"),
        P("sp", "tp"),
    )
    out_specs = (
        P("sp", None, "tp"),
        P("sp", None, "tp"),
        P("sp", "tp", None),
        P("sp", "tp"),
        P("sp", "tp"),
        P("sp", "tp"),
    )
    return jax.shard_map(local, mesh=mesh, in_specs=in_specs, out_specs=out_specs, check_vma=False)
```

```python
import functools

import jax
import jax.numpy as jnp
from jax import lax
from jax.experimental import pallas as pl
from jax.experimental.pallas import tpu as pltpu
from jax.sharding import PartitionSpec as P

CONV_K = 31
GROUP = 128
MESH = pl.DeviceIdType.MESH


CLAMP_LIMIT = 7.0
SLOPE_ALPHA = 1.702


def passed_along(block, axis, distance):
    devices = range(lax.axis_size(axis))
    route = [(i - distance, i) for i in devices if i - distance in devices]
    return lax.ppermute(block, axis, route)


def tp_places():
    mine = lax.axis_index("tp")
    near = mine + 1 - 2 * (mine % 2)
    far = (mine + 2) % 4
    diag = (near + 2) % 4
    return mine, near, far, diag


def meet(steps, over_sp, near, far):
    s, t = lax.axis_index("sp"), lax.axis_index("tp")
    barrier = pltpu.get_barrier_semaphore()
    pl.semaphore_signal(barrier, inc=1, device_id=(s, near), device_id_type=MESH)
    pl.semaphore_signal(barrier, inc=1, device_id=(s, far), device_id_type=MESH)
    total = 2
    if over_sp:

        def greet(d, carry):
            pl.semaphore_signal(
                barrier, inc=1, device_id=((s + d) % steps, t), device_id_type=MESH
            )
            return carry

        lax.fori_loop(1, steps, greet, 0)
        total += steps - 1
    pl.semaphore_wait(barrier, total)


def crossing_first(steps, k):
    return steps // 2 + ((k + 1) // 2) * (2 * (k % 2) - 1)


def looped(first, last, body):
    def step(k, carry):
        body(k)
        return carry

    lax.fori_loop(first, last, step, 0)


def spread_kernel(count, steps, over_sp, in_lanes, absolute, beside, sp_count, *refs):
    refs = list(refs)
    sends, refs = refs[:count], refs[count:]
    fulls, refs = (refs[:count], refs[count:]) if over_sp else (None, refs)
    side, refs = (refs[0], refs[1:]) if beside else (None, refs)
    outs, refs = refs[:count], refs[count:]
    side_out, refs = (refs[0], refs[1:]) if beside else (None, refs)
    own_sem, a_send, a_recv, b_send, f_send, c_send, near_recv, fwd_recv, far_recv = refs[:9]
    s = lax.axis_index("sp")
    t, near, far, _ = tp_places()
    width = sends[0].shape[-1]

    def place(c, d, q):
        if in_lanes:
            return outs[c].at[d, :, pl.ds(pl.multiple_of(q * width, width), width)]
        return outs[c].at[d, q]

    def source(c, d):
        return sends[c].at[(s + d) % steps if absolute else d]

    def own(c, d):
        if over_sp:
            return pltpu.make_async_copy(fulls[c], outs[c].at[0], own_sem.at[c, 0])
        return pltpu.make_async_copy(source(c, d), place(c, d, t), own_sem.at[c, d])

    def to_sp(c, d):
        return pltpu.make_async_remote_copy(
            src_ref=source(c, d),
            dst_ref=place(c, d, t),
            send_sem=a_send.at[c, d],
            recv_sem=a_recv.at[c, d],
            device_id=((s + d) % steps, t),
            device_id_type=MESH,
        )

    def to_tp(c, d, q, target, send_sem, recv_sem):
        return pltpu.make_async_remote_copy(
            src_ref=place(c, d, q),
            dst_ref=place(c, d, q),
            send_sem=send_sem.at[c, d],
            recv_sem=recv_sem.at[c, d],
            device_id=(s, target),
            device_id_type=MESH,
        )

    def near_copy(c, d):
        return to_tp(c, d, t, near, b_send, near_recv)

    def far_copy(c, d):
        return to_tp(c, d, t, far, f_send, far_recv)

    def fwd_copy(c, d):
        return to_tp(c, d, far, near, c_send, fwd_recv)

    def side_copy(d):
        side_send, side_recv = refs[10:12]
        return pltpu.make_async_remote_copy(
            src_ref=side,
            dst_ref=side_out.at[d],
            send_sem=side_send.at[d],
            recv_sem=side_recv.at[d],
            device_id=((s + d) % sp_count, t),
            device_id_type=MESH,
        )

    def own_side():
        return pltpu.make_async_copy(side, side_out.at[0], refs[9].at[0])

    def share(c, d):
        far_copy(c, d).start()
        near_copy(c, d).start()

    def forward(c, d):
        far_copy(c, d).wait_recv()
        fwd_copy(c, d).start()

    def finish(c, d):
        near_copy(c, d).wait()
        far_copy(c, d).wait_send()
        fwd_copy(c, d).wait()

    def loop(first, last, body):
        def each(k):
            d = k + 1 if over_sp else k
            for c in range(count):
                body(c, d)

        looped(first, last, each)

    meet(sp_count, over_sp or beside, near, far)
    if over_sp:
        loop(0, steps - 1, lambda c, d: to_sp(c, d).start())
        for c in range(count):
            own(c, 0).start()

        def pass_on(k):
            for c in range(count):
                d = k + 1
                to_sp(c, d).wait_recv()
                share(c, d)

        def pass_on_twice(k):
            pass_on(k)
            for c in range(count):
                forward(c, k)

        pass_on(0)
        looped(1, steps - 1, pass_on_twice)
        loop(steps - 2, steps - 1, forward)
        loop(0, steps - 1, finish)
        loop(0, steps - 1, lambda c, d: to_sp(c, d).wait_send())
        for c in range(count):
            own(c, 0).wait()
    else:
        loop(0, steps, lambda c, d: own(c, d).start())
        if beside:
            looped(0, sp_count - 1, lambda k: side_copy(crossing_first(sp_count, k)).start())
            own_side().start()

        def share_own(c, d):
            own(c, d).wait()
            share(c, d)

        loop(0, steps, share_own)
        loop(0, steps, forward)
        loop(0, steps, finish)
        if beside:
            looped(0, sp_count - 1, lambda k: side_copy(crossing_first(sp_count, k)).wait())
            own_side().wait()


def spread(sends, fulls, side, in_lanes, absolute, collective_id):
    count = len(sends)
    steps, rows, width = sends[0].shape
    tp_count, sp_count = lax.axis_size("tp"), lax.axis_size("sp")
    over_sp, beside = fulls is not None, side is not None
    shape = (steps, rows, tp_count * width) if in_lanes else (steps, tp_count, rows, width)
    out_shape = [jax.ShapeDtypeStruct(shape, x.dtype) for x in sends]
    operands = list(sends) + (list(fulls) if over_sp else []) + ([side] if beside else [])
    scratch = [pltpu.SemaphoreType.DMA((count, steps))] * 9
    if beside:
        out_shape.append(jax.ShapeDtypeStruct((sp_count,) + side.shape, side.dtype))
        scratch += [pltpu.SemaphoreType.DMA((1,))] + [pltpu.SemaphoreType.DMA((sp_count,))] * 2
    return pl.pallas_call(
        functools.partial(
            spread_kernel, count, steps, over_sp, in_lanes, absolute, beside, sp_count
        ),
        out_shape=tuple(out_shape),
        in_specs=[pl.BlockSpec(memory_space=pltpu.VMEM)] * len(operands),
        out_specs=tuple(pl.BlockSpec(memory_space=pltpu.VMEM) for _ in out_shape),
        scratch_shapes=scratch,
        compiler_params=pltpu.CompilerParams(
            collective_id=collective_id, has_side_effects=True, vmem_limit_bytes=40 << 20
        ),
    )(*operands)


def combine_kernel(
    steps, part, out, near_in, pair, far_in, total,
    n0_send, n0_recv, n1_send, n1_recv, f_send, f_recv, a_send, a_recv,
):
    s = lax.axis_index("sp")
    t, near, far, diag = tp_places()
    width = out.shape[-1]

    def lanes(q):
        return pl.ds(pl.multiple_of(q * width, width), width)

    def near_copy(d, which, q, send_sem, recv_sem):
        return pltpu.make_async_remote_copy(
            src_ref=part.at[d, :, lanes(q)],
            dst_ref=near_in.at[which, d],
            send_sem=send_sem.at[d],
            recv_sem=recv_sem.at[d],
            device_id=(s, near),
            device_id_type=MESH,
        )

    def for_near(d):
        return near_copy(d, 0, near, n0_send, n0_recv)

    def for_diag(d):
        return near_copy(d, 1, diag, n1_send, n1_recv)

    def far_copy(d):
        return pltpu.make_async_remote_copy(
            src_ref=pair.at[d],
            dst_ref=far_in.at[d],
            send_sem=f_send.at[d],
            recv_sem=f_recv.at[d],
            device_id=(s, far),
            device_id_type=MESH,
        )

    def back(d):
        return pltpu.make_async_remote_copy(
            src_ref=total.at[d],
            dst_ref=out.at[d],
            send_sem=a_send.at[d],
            recv_sem=a_recv.at[d],
            device_id=((s + steps - d) % steps, t),
            device_id_type=MESH,
        )

    meet(steps, True, near, far)

    def open_up(d):
        for_diag(d).start()
        for_near(d).start()

    def add_pair(d):
        for_diag(d).wait_recv()
        mine = part[d, :, lanes(far)].astype(jnp.float32)
        pair[d] = (mine + near_in[1, d].astype(jnp.float32)).astype(pair.dtype)
        far_copy(d).start()

    def whole(d):
        for_near(d).wait_recv()
        far_copy(d).wait_recv()
        mine = part[d, :, lanes(t)].astype(jnp.float32)
        both = mine + near_in[0, d].astype(jnp.float32)
        return (both + far_in[d].astype(jnp.float32)).astype(out.dtype)

    def send_back(d):
        total[d] = whole(d)
        back(d).start()

    def at(k):
        return crossing_first(steps, k)

    lag = min(3, steps - 1)
    looped(0, steps - 1, lambda k: open_up(at(k)))
    open_up(0)
    looped(0, lag, lambda k: add_pair(at(k)))

    def middle(k):
        add_pair(at(k))
        send_back(at(k - lag))

    looped(lag, steps - 1, middle)
    add_pair(0)
    looped(steps - 1 - lag, steps - 1, lambda k: send_back(at(k)))
    out[0] = whole(0)

    def finish(d):
        for_near(d).wait_send()
        for_diag(d).wait_send()
        far_copy(d).wait_send()

    looped(0, steps, finish)
    looped(1, steps, lambda d: back(d).wait())


def combine(part, collective_id):
    steps, rows, all_width = part.shape
    width = all_width // lax.axis_size("tp")
    block = (steps, rows, width)
    return pl.pallas_call(
        functools.partial(combine_kernel, steps),
        out_shape=jax.ShapeDtypeStruct(block, part.dtype),
        in_specs=[pl.BlockSpec(memory_space=pltpu.VMEM)],
        out_specs=pl.BlockSpec(memory_space=pltpu.VMEM),
        scratch_shapes=[
            pltpu.VMEM((2,) + block, part.dtype),
            pltpu.VMEM(block, part.dtype),
            pltpu.VMEM(block, part.dtype),
            pltpu.VMEM(block, part.dtype),
        ]
        + [pltpu.SemaphoreType.DMA((steps,))] * 8,
        compiler_params=pltpu.CompilerParams(
            collective_id=collective_id, has_side_effects=True, vmem_limit_bytes=40 << 20
        ),
    )(part)


def contract_rows(left_side, right_side):
    return lax.dot_general(
        left_side, right_side, (((0,), (0,)), ((), ())), preferred_element_type=jnp.float32
    )


def contract_cols(left_side, right_side):
    return lax.dot_general(
        left_side, right_side, (((1,), (1,)), ((), ())), preferred_element_type=jnp.float32
    )


def expert_backward(routed_rows, routed_cots, w_gate, w_up, w_down):
    gate_pre = jnp.dot(routed_rows, w_gate, preferred_element_type=jnp.float32)
    up_pre = jnp.dot(routed_rows, w_up, preferred_element_type=jnp.float32)
    gate_clamped = jnp.minimum(gate_pre, CLAMP_LIMIT)
    up_clamped = jnp.clip(up_pre, -CLAMP_LIMIT, CLAMP_LIMIT)
    sigma = jax.nn.sigmoid(SLOPE_ALPHA * gate_clamped)
    gated = gate_clamped * sigma
    act = ((up_clamped + 1.0) * gated).astype(jnp.bfloat16)
    down_grad = contract_rows(act, routed_cots).astype(jnp.bfloat16)
    act_grad = contract_cols(routed_cots, w_down)
    inside = (up_pre > -CLAMP_LIMIT) & (up_pre < CLAMP_LIMIT)
    up_pre_grad = jnp.where(inside, act_grad * gated, 0.0).astype(jnp.bfloat16)
    slope = sigma + SLOPE_ALPHA * gate_clamped * sigma * (1.0 - sigma)
    gate_pre_grad = jnp.where(
        gate_pre < CLAMP_LIMIT, act_grad * (up_clamped + 1.0) * slope, 0.0
    ).astype(jnp.bfloat16)
    gate_grad = contract_rows(routed_rows, gate_pre_grad).astype(jnp.bfloat16)
    up_grad = contract_rows(routed_rows, up_pre_grad).astype(jnp.bfloat16)
    partial_value = contract_cols(gate_pre_grad, w_gate) + contract_cols(up_pre_grad, w_up)
    return (gate_grad, up_grad, down_grad, partial_value)


def line_schedule(line):
    codes = []
    for z in range(line):
        slots = [[(z, 0), 0, 0, 0], [(z, 1), 1, 1, 0]]
        groups = [[b for b in (z - k, z + k) if 0 <= b < line] for k in range(1, line)]
        groups = [g for g in groups if g]
        for k, group in enumerate(groups, 1):
            following = k + 1 if k < len(groups) else 0
            added = [[(b, 0), 0, 0, 0] for b in group] + [[(b, 1), 0, 0, 0] for b in group]
            many = len(group)
            added[0][3] = group[0] + 1
            if many > 1:
                added[many][3] = group[1] + 1
            added[1][1] = following
            added[many][2] = following
            slots += added
        row = []
        for (zb, col), first, second, meeting in slots:
            row.append((((meeting * 16 + second) * 16 + first) * 2 + col) * 16 + zb)
        codes.append(row)
    return codes


def settle_body(
    steps, meanwhile, part_grad, grad_out, resid, norm_gain, proj_weight,
    conv_sum, conv_gain, conv_taps, conv_value, conv_gate,
    side_out, feature_cols, proj, value_grad, gate_input_grad,
    full, grads, extended, far_send, far_recv, near_send, near_recv, fwd_send, fwd_recv,
    own_sem, x_send, x_recv, xf_send, xf_recv, xn_send, xn_recv, xw_send, xw_recv,
    h_send, h_recv,
):
    s = lax.axis_index("sp")
    t, near, far, diag = tp_places()
    tok_rows, width = part_grad.shape
    chunks, share = feature_cols.shape[1], feature_cols.shape[2]
    feat_rows = feature_cols.shape[3]
    overlap = conv_taps.shape[0] - 1

    def rows_of(j):
        return pl.ds(pl.multiple_of(j * share, share), share)

    def lanes(q):
        return pl.ds(pl.multiple_of(q * width, width), width)

    def mine_at(j):
        return full.at[rows_of(j), lanes(t)]

    def own_copy():
        return pltpu.make_async_copy(part_grad, full.at[:, lanes(t)], own_sem.at[0])

    def gather(j, q, src, target, send_sem, recv_sem):
        return pltpu.make_async_remote_copy(
            src_ref=src,
            dst_ref=full.at[rows_of(j), lanes(q)],
            send_sem=send_sem.at[j],
            recv_sem=recv_sem.at[j],
            device_id=(s, target),
            device_id_type=MESH,
        )

    def to_far(j):
        return gather(j, t, part_grad.at[rows_of(j), :], far, far_send, far_recv)

    def to_near(j):
        return gather(j, t, part_grad.at[rows_of(j), :], near, near_send, near_recv)

    def pass_near(j):
        return gather(j, far, full.at[rows_of(j), lanes(far)], near, fwd_send, fwd_recv)

    def spread_out(d):
        feats = pl.ds(pl.multiple_of(((s + d) % steps) * feat_rows, feat_rows), feat_rows)
        return pltpu.make_async_remote_copy(
            src_ref=grads.at[rows_of(t), feats],
            dst_ref=feature_cols.at[d, t],
            send_sem=x_send.at[d],
            recv_sem=x_recv.at[d],
            device_id=((s + d) % steps, t),
            device_id_type=MESH,
        )

    def beside(d, q, target, send_sem, recv_sem):
        return pltpu.make_async_remote_copy(
            src_ref=feature_cols.at[d, q],
            dst_ref=feature_cols.at[d, q],
            send_sem=send_sem.at[d],
            recv_sem=recv_sem.at[d],
            device_id=(s, target),
            device_id_type=MESH,
        )

    def x_far(d):
        return beside(d, t, far, xf_send, xf_recv)

    def x_near(d):
        return beside(d, t, near, xn_send, xn_recv)

    def x_pass(d):
        return beside(d, far, near, xw_send, xw_recv)

    def halo():
        return pltpu.make_async_remote_copy(
            src_ref=extended.at[pl.ds(0, overlap + 2)],
            dst_ref=extended.at[pl.ds(tok_rows, overlap + 2)],
            send_sem=h_send.at[0],
            recv_sem=h_recv.at[0],
            device_id=((s + steps - 1) % steps, t),
            device_id_type=MESH,
        )

    gain = norm_gain[...]

    def settle(j):
        here = rows_of(j)
        feature_grad = full[here, :].astype(jnp.float32) * gain
        x = resid[here, :].astype(jnp.float32)
        scale = lax.rsqrt(jnp.mean(x * x, axis=-1, keepdims=True) + 1e-06)
        cubed = scale * scale * scale
        mean = jnp.mean(x * feature_grad, axis=-1, keepdims=True)
        value = grad_out[here, :].astype(jnp.float32) + scale * feature_grad - x * cubed * mean
        grads[here, :] = value.astype(grads.dtype)

    def crossing(k):
        return crossing_first(steps, k)

    for j in (far, diag, t, near):
        to_far(j).start()
    for j in (near, t, diag, far):
        to_near(j).start()
    own_copy().start()
    summed = conv_sum[...].astype(jnp.float32)
    centre = summed - jnp.mean(summed, axis=-1, keepdims=True)
    inv_std = lax.rsqrt(jnp.mean(centre * centre, axis=-1, keepdims=True) + 1e-05)
    grouped = centre * inv_std
    pre_act = grouped * conv_gain[...]
    sigma = jax.nn.sigmoid(pre_act)
    slope = sigma * (1.0 + pre_act * (1.0 - sigma)) * conv_gain[...]
    own_copy().wait()

    def arrive(j):
        to_far(j).wait_recv()
        pass_near(j).start()

    def whole(j):
        to_near(j).wait_recv()
        pass_near(j).wait_recv()

    arrive(t)
    arrive(near)
    whole(t)
    settle(t)
    looped(0, steps - 1, lambda k: spread_out(crossing(k)).start())
    meanwhile()
    arrive(far)
    arrive(diag)
    for j in (near, far, diag):
        whole(j)
        settle(j)
    feats = pl.ds(pl.multiple_of(s * feat_rows, feat_rows), feat_rows)
    feature_cols[0] = grads[:, feats].reshape(chunks, share, feat_rows)
    out_grad = jnp.dot(grads[...], proj_weight[...], preferred_element_type=jnp.float32)
    normal = out_grad * slope
    sum_grad = inv_std * (
        normal
        - jnp.mean(normal, axis=-1, keepdims=True)
        - grouped * jnp.mean(normal * grouped, axis=-1, keepdims=True)
    )
    extended[pl.ds(0, tok_rows), :] = sum_grad
    halo().start()

    def share_out(d):
        spread_out(d).wait_recv()
        x_far(d).start()
        x_near(d).start()

    def pass_on(d):
        x_far(d).wait_recv()
        x_pass(d).start()

    def term(d):
        left = feature_cols[d].reshape(tok_rows, feat_rows)
        return contract_rows(left, side_out[d])

    def gather_term(d):
        x_near(d).wait_recv()
        x_pass(d).wait_recv()
        proj[...] += term(d)

    def both(k):
        share_out(crossing(k))
        pass_on(crossing(k - 1))

        @pl.when(k >= 2)
        def _():
            gather_term(crossing(k - 2))

    proj[...] = term(0)
    share_out(crossing(0))
    looped(1, steps - 1, both)
    halo().wait()

    @pl.when(s == steps - 1)
    def _():
        extended[pl.ds(tok_rows, overlap + 2), :] = jnp.zeros(
            (overlap + 2, extended.shape[1]), extended.dtype
        )

    gated_grad = extended[pl.ds(overlap, tok_rows), :] * conv_taps[pl.ds(0, 1), :]
    for j in range(1, overlap + 1):
        gated_grad += extended[pl.ds(overlap - j, tok_rows), :] * conv_taps[pl.ds(j, 1), :]
    sigma_gate = jax.nn.sigmoid(conv_gate[...].astype(jnp.float32))
    value_grad[...] = (gated_grad * sigma_gate).astype(value_grad.dtype)
    gate_input_grad[...] = (
        gated_grad * conv_value[...].astype(jnp.float32) * sigma_gate * (1.0 - sigma_gate)
    ).astype(gate_input_grad.dtype)
    pass_on(crossing(steps - 2))
    gather_term(crossing(steps - 3))
    gather_term(crossing(steps - 2))

    def finish(k):
        d = crossing(k)
        spread_out(d).wait_send()
        x_near(d).wait_send()
        x_far(d).wait_send()
        x_pass(d).wait_send()

    looped(0, steps - 1, finish)

    def finish_gather(j):
        to_far(j).wait_send()
        to_near(j).wait_send()
        pass_near(j).wait_send()

    looped(0, chunks, finish_gather)


def relay_kernel(
    steps, routes_in, weights_in, grad_in, resid_in, gain_in, gate_in, up_in, down_in, sum_in,
    conv_gain_in, proj_in, taps_in, value_in, convgate_in,
    gate_grad, up_grad, down_grad, proj, value_grad, gate_input_grad,
    routes, route_weights, grad_out, resid, norm_gain, w_gate, w_up, w_down, conv_sum, conv_gain,
    proj_weight, conv_taps, conv_value, conv_gate, part_grad, side_out, feature_cols, full, grads,
    extended, normed, info, infos, ranks, weights, before, picks,
    tok, over, cross, cross_far, held, act, gate_pg, up_pg, part,
    near_in, pair, far_in, total, ret, side,
    own_sem, info_send, info_recv, line_send, line_recv, end_send, cross_recv,
    across_send, afar_send, arr_recv, b_send, f_send, c_send, near_recv, fwd_recv, far_recv,
    n0_send, n0_recv, n1_send, n1_recv, g_send, g_recv, r_send, r_recv, s_send, s_recv,
    *settle_sems,
):
    s = lax.axis_index("sp")
    t, near, far, diag = tp_places()
    line = steps // 2
    z, y = s // 2, s % 2
    across = s + 1 - 2 * y
    tok_rows, width = part_grad.shape
    count = cross.shape[2]
    hidden = w_gate.shape[1]
    model_width = resid.shape[1]
    both = (0, 1)
    kind = held.dtype
    sources = (grad_out, normed)

    def lanes(q):
        return pl.ds(pl.multiple_of(q * width, width), width)

    def remote(src, dst, send_sem, recv_sem, sp_to, tp_to):
        return pltpu.make_async_remote_copy(
            src_ref=src,
            dst_ref=dst,
            send_sem=send_sem,
            recv_sem=recv_sem,
            device_id=(sp_to, tp_to),
            device_id_type=MESH,
        )

    moves = [
        pltpu.make_async_copy(a, b, own_sem.at[i])
        for i, (a, b) in enumerate(
            (
                (grad_in, grad_out),
                (routes_in, routes),
                (weights_in, route_weights),
                (resid_in, resid),
                (gain_in, norm_gain),
                (sum_in, conv_sum),
                (conv_gain_in, conv_gain),
                (gate_in, w_gate),
                (up_in, w_up),
                (down_in, w_down),
                (proj_in, proj_weight),
                (taps_in, conv_taps),
                (value_in, conv_value),
                (convgate_in, conv_gate),
            )
        )
    ]

    def info_copy(dz):
        peer = ((z + dz) % line) * 2 + y
        return remote(info, infos.at[z], info_send.at[dz], info_recv.at[z], peer, t)

    def info_from(zb):
        return remote(info, infos.at[zb], info_send.at[0], info_recv.at[zb], across, t)

    def line_copy(a, zb, src, up):
        to = s + 2 if up else s - 2
        return remote(src, tok.at[a, zb], line_send.at[a, up, zb], line_recv.at[a, zb], to, t)

    def end_copy(a, zb, col, up):
        to = s + 2 if up else s - 2
        j = 2 * zb + y
        if col == 0:
            dst, recv = held.at[a, j, :, lanes(t)], arr_recv.at[a, j]
        else:
            dst, recv = cross.at[a, zb], cross_recv.at[a, zb]
        return remote(over.at[a, zb, col], dst, end_send.at[a, col, zb], recv, to, t)

    def across_copy(a, zb):
        j = 2 * zb + y
        dst = held.at[a, j, :, lanes(t)]
        return remote(cross.at[a, zb], dst, across_send.at[a, zb], arr_recv.at[a, j], across, t)

    def across_far(a):
        dst = held.at[a, s, :, lanes(far)]
        return remote(cross_far.at[a], dst, afar_send.at[a], far_recv.at[a, s], across, t)

    def arrival(a, j):
        place = held.at[a, j, :, lanes(t)]
        return remote(place, place, f_send.at[a, j], arr_recv.at[a, j], s, far)

    def to_tp(a, j, q, target, send_sem, recv_sem):
        place = held.at[a, j, :, lanes(q)]
        return remote(place, place, send_sem.at[a, j], recv_sem.at[a, j], s, target)

    def near_copy(a, j):
        return to_tp(a, j, t, near, b_send, near_recv)

    def far_copy(a, j):
        return to_tp(a, j, t, far, f_send, far_recv)

    def fwd_copy(a, j):
        return to_tp(a, j, far, near, c_send, fwd_recv)

    def part_copy(j, which, q, send_sem, recv_sem):
        src, dst = part.at[j, :, lanes(q)], near_in.at[which, j]
        return remote(src, dst, send_sem.at[j], recv_sem.at[j], s, near)

    def for_near(j):
        return part_copy(j, 0, near, n0_send, n0_recv)

    def for_diag(j):
        return part_copy(j, 1, diag, n1_send, n1_recv)

    def pair_copy(j):
        return remote(pair.at[j], far_in.at[j], g_send.at[j], g_recv.at[j], s, far)

    def back(j):
        return remote(total.at[j], ret.at[s], r_send.at[j], r_recv.at[s], j, t)

    def back_from(e):
        return remote(total.at[e], ret.at[e], r_send.at[e], r_recv.at[e], e, t)

    def side_copy(d):
        to = (s + d) % steps
        return remote(side, side_out.at[d], s_send.at[d], s_recv.at[d], to, t)

    def table(zb):
        first, second = infos[zb, pl.ds(0, 1), :], infos[zb, pl.ds(1, 1), :]
        ids = lax.broadcasted_iota(jnp.int32, (steps, tok_rows), 0).astype(jnp.float32)
        chosen = (first == ids) | (second == ids)
        ones = jnp.where(chosen, 1.0, 0.0).astype(kind)
        rank = jnp.dot(ones, before[...], preferred_element_type=jnp.float32)
        ranks[zb] = jnp.where(chosen, rank, -1.0)
        weights[zb] = jnp.where(
            first == ids, infos[zb, pl.ds(2, 1), :], infos[zb, pl.ds(3, 1), :]
        )

    def pick(zb, e):
        slots = lax.broadcasted_iota(jnp.int32, (count, tok_rows), 0).astype(jnp.float32)
        return slots == ranks[zb, pl.ds(e, 1), :]

    def selected(a, zb, e, value):
        mask = pick(zb, e)
        hot = jnp.where(mask, 1.0, 0.0).astype(kind)
        out = jnp.dot(hot, value, preferred_element_type=jnp.float32)
        if a == 0:
            scale = jnp.where(mask, weights[zb, pl.ds(e, 1), :], 0.0)
            out = out * jnp.sum(scale, axis=1, keepdims=True)
        return out.astype(kind)

    def to_end(a, zb, value, up):
        end = z + 1 if up else z - 1
        for col in both:
            e = 2 * end + (y if col == 0 else 1 - y)
            over[a, zb, col] = selected(a, zb, e, value)
            end_copy(a, zb, col, up).start()

    def valid(m, up):
        return (z >= m) if up else (z + m < line)

    def block_at(m, up):
        return z - m if up else z + m

    def next_is_end(up):
        return (z + 1 == line - 1) if up else (z == 1)

    def next_is_inner(up):
        return (z + 1 < line - 1) if up else (z >= 2)

    def at_end(up):
        return (z == line - 1) if up else (z == 0)

    def share(a, j):
        far_copy(a, j).start()
        near_copy(a, j).start()

    def read_info(m, up):
        zb = block_at(m, up)

        @pl.when(valid(m, up))
        def _():
            info_from(zb).wait_recv()

        @pl.when(valid(m, up) & jnp.logical_not(at_end(up)))
        def _():
            table(zb)

    def handle(a, m, up):
        zb = block_at(m, up)
        j = 2 * zb + y

        @pl.when(valid(m, up) & at_end(up))
        def _():
            arrival(a, j).wait_recv()
            end_copy(a, zb, 1, up).wait_recv()
            across_copy(a, zb).start()
            share(a, j)

        @pl.when(valid(m, up) & jnp.logical_not(at_end(up)))
        def _():
            line_copy(a, zb, tok.at[a, zb], up).wait_recv()

            @pl.when(next_is_end(up))
            def _():
                to_end(a, zb, tok[a, zb], up)

            @pl.when(next_is_inner(up))
            def _():
                line_copy(a, zb, tok.at[a, zb], up).start()

            cross[a, zb] = selected(a, zb, across, tok[a, zb])
            across_copy(a, zb).start()
            held[a, j, :, lanes(t)] = selected(a, zb, s, tok[a, zb])
            share(a, j)

    def unless_own(j, body):
        @pl.when(j != s)
        def _():
            body()

    def experts(j):
        def settle():
            for a in both:
                near_copy(a, j).wait_recv()
                fwd_copy(a, j).wait_recv()

        unless_own(j, settle)
        gate_pre = jnp.dot(held[1, j], w_gate[...], preferred_element_type=jnp.float32)
        up_pre = jnp.dot(held[1, j], w_up[...], preferred_element_type=jnp.float32)
        act_grad = contract_cols(held[0, j], w_down[...])
        gate_clamped = jnp.minimum(gate_pre, CLAMP_LIMIT)
        up_clamped = jnp.clip(up_pre, -CLAMP_LIMIT, CLAMP_LIMIT)
        sigma = jax.nn.sigmoid(SLOPE_ALPHA * gate_clamped)
        gated = gate_clamped * sigma
        act[j] = ((up_clamped + 1.0) * gated).astype(kind)
        inside = (up_pre > -CLAMP_LIMIT) & (up_pre < CLAMP_LIMIT)
        up_g = jnp.where(inside, act_grad * gated, 0.0).astype(kind)
        slope = sigma + SLOPE_ALPHA * gate_clamped * sigma * (1.0 - sigma)
        gate_g = jnp.where(
            gate_pre < CLAMP_LIMIT, act_grad * (up_clamped + 1.0) * slope, 0.0
        ).astype(kind)
        gate_pg[j] = gate_g
        up_pg[j] = up_g
        for q in range(model_width // width):
            mine = pl.ds(q * width, width)
            value = contract_cols(gate_g, w_gate[mine, :]) + contract_cols(up_g, w_up[mine, :])
            part[j, :, mine] = value.astype(kind)
        for_diag(j).start()
        for_near(j).start()

    def add_pair(j):
        for_diag(j).wait_recv()
        mine = part[j, :, lanes(far)].astype(jnp.float32)
        pair[j] = (mine + near_in[1, j].astype(jnp.float32)).astype(kind)
        pair_copy(j).start()

    def whole(j):
        for_near(j).wait_recv()
        pair_copy(j).wait_recv()
        mine = part[j, :, lanes(t)].astype(jnp.float32)
        summed = mine + near_in[0, j].astype(jnp.float32)
        return (summed + far_in[j].astype(jnp.float32)).astype(kind)

    def send_back(j):
        @pl.when(j == s)
        def _():
            ret[s] = whole(j)

        @pl.when(j != s)
        def _():
            total[j] = whole(j)
            back(j).start()

    def forward(j):
        def run():
            for a in both:
                far_copy(a, j).wait_recv()
                fwd_copy(a, j).start()

        unless_own(j, run)

    def flat(value):
        return value.reshape(-1, value.shape[-1])

    def row_grads(k):
        cols = pl.ds(pl.multiple_of(k * 256, 256), 256)
        left = flat(held[1, :, :, cols])
        gate_grad[cols, :] = contract_rows(left, flat(gate_pg[...])).astype(kind)
        up_grad[cols, :] = contract_rows(left, flat(up_pg[...])).astype(kind)

    def act_grads(k):
        cols = pl.ds(pl.multiple_of(k * 512, 512), 512)
        down_grad[:, cols] = contract_rows(flat(act[...]), flat(held[0, :, :, cols])).astype(kind)

    for move in moves:
        move.start()
    meet(steps, True, near, far)
    moves[0].wait()

    def start_own(a):
        src = sources[a]
        for up in both:

            @pl.when(next_is_inner(up))
            def _():
                line_copy(a, z, src.at[:, lanes(t)], up).start()

    def end_own(a):
        for up in both:

            @pl.when(next_is_end(up))
            def _():
                to_end(a, z, sources[a][:, lanes(t)], up)

    start_own(0)
    moves[1].wait()
    moves[2].wait()
    info[pl.ds(0, 2), :] = routes[...].astype(jnp.float32)
    info[pl.ds(2, 2), :] = route_weights[...]
    infos[z] = info[...]
    looped(1, line, lambda dz: info_copy(dz).start())
    row_ids = lax.broadcasted_iota(jnp.int32, (tok_rows, tok_rows), 0)
    col_ids = lax.broadcasted_iota(jnp.int32, (tok_rows, tok_rows), 1)
    before[...] = jnp.where(row_ids < col_ids, 1.0, 0.0).astype(kind)
    table(z)
    end_own(0)
    for move in moves[3:5]:
        move.wait()
    gain = norm_gain[...]

    def normalise(k):
        here = pl.ds(pl.multiple_of(k * 32, 32), 32)
        x = resid[here, :].astype(jnp.float32)
        scale = lax.rsqrt(jnp.mean(x * x, axis=-1, keepdims=True) + 1e-06)
        normed[here, :] = (x * scale * gain).astype(kind)

    looped(0, tok_rows // 32, normalise)
    start_own(1)
    end_own(1)
    for a in both:
        cross[a, z] = selected(a, z, across, sources[a][:, lanes(t)])
        across_copy(a, z).start()
        cross_far[a] = selected(a, z, across, sources[a][:, lanes(far)])
        across_far(a).start()

    def own_chunk(q):
        for a in both:
            held[a, s, :, lanes(q)] = selected(a, z, s, sources[a][:, lanes(q)])

    looped(0, model_width // width, own_chunk)
    for move in moves[5:7]:
        move.wait()
    summed = conv_sum[...].astype(jnp.float32)
    centre = summed - jnp.mean(summed, axis=-1, keepdims=True)
    inv_std = lax.rsqrt(jnp.mean(centre * centre, axis=-1, keepdims=True) + 1e-05)
    pre_act = centre * inv_std * conv_gain[...]
    conv_out = (pre_act * jax.nn.sigmoid(pre_act)).astype(kind)
    side[...] = conv_out
    side_out[0] = conv_out

    def own_picks(e):
        picks[e] = jnp.where(pick(z, e), 1.0, 0.0).astype(kind)

    looped(0, steps, own_picks)
    for move in moves[7:]:
        move.wait()

    codes = line_schedule(line)
    middle = steps // 2

    def slot_code(n):
        code = 0
        for zz in range(line):
            for nn in range(steps):
                code = code + jnp.where((z == zz) & (n == nn), codes[zz][nn], 0)
        return code

    def chunk_at(n):
        code = slot_code(n)
        other = (code // 16) % 2
        return 2 * (code % 16) + y + other * (1 - 2 * y)

    def slot(n):
        code = slot_code(n)
        zb, other = code % 16, (code // 16) % 2
        first, second = (code // 32) % 16, (code // 512) % 16
        meeting = code // 8192
        j = 2 * zb + y + other * (1 - 2 * y)

        @pl.when(meeting > 0)
        def _():
            met = 2 * (meeting - 1) + 1 - y
            for a in both:
                arrival(a, met).wait_recv()
                share(a, met)

        @pl.when(first > 0)
        def _():
            for up in both:
                read_info(first, up)
            for up in both:
                handle(0, first, up)

        @pl.when(second > 0)
        def _():
            for up in both:
                handle(1, second, up)

        @pl.when(n == 1)
        def _():
            for a in both:
                arrival(a, j).wait_recv()
                near_copy(a, j).start()

        @pl.when(n == steps - 2)
        def _():
            looped(1, steps, lambda d: side_copy(d).start())

        forward(j)
        experts(j)

        @pl.when(n == 0)
        def _():
            add_pair(j)

        @pl.when(n > middle)
        def _():
            add_pair(chunk_at(n - 1))

    def pair_at(n):
        add_pair(chunk_at(n))

    def back_at(n):
        send_back(chunk_at(n))

    looped(0, steps, slot)
    half = model_width // 512
    pair_at(steps - 1)
    looped(1, middle, pair_at)
    looped(middle, steps - 2, back_at)
    looped(0, half, row_grads)
    back_at(steps - 2)
    looped(half, 2 * half, row_grads)
    back_at(steps - 1)
    looped(0, half, act_grads)
    looped(1, middle, back_at)
    back_at(0)

    def gather_back(d):
        back_from((s + d) % steps).wait_recv()

    looped(1, steps, gather_back)
    part_grad[...] = contract_rows(flat(picks[...]), flat(ret[...])).astype(kind)

    def finish(j):
        for_near(j).wait_send()
        for_diag(j).wait_send()
        pair_copy(j).wait_send()

        @pl.when(j != s)
        def _():
            back(j).wait_send()
            for a in both:
                near_copy(a, j).wait_send()
                fwd_copy(a, j).wait_send()

        @pl.when(j // 2 != z)
        def _():
            for a in both:
                far_copy(a, j).wait_send()

    def finish_side(d):
        side_copy(d).wait_send()

    def finish_line(m):
        for up in both:
            zb = block_at(m, up)

            @pl.when(valid(m, up) & next_is_inner(up))
            def _():
                for a in both:
                    line_copy(a, zb, tok.at[a, zb], up).wait_send()

            @pl.when(valid(m, up) & next_is_end(up))
            def _():
                for a in both:
                    for col in both:
                        end_copy(a, zb, col, up).wait_send()

    def finish_across(zb):
        for a in both:
            across_copy(a, zb).wait_send()

    def meanwhile():
        looped(1, steps, lambda d: side_copy(d).wait_recv())
        looped(0, steps, finish)
        looped(1, steps, finish_side)
        looped(1, line, lambda dz: info_copy(dz).wait_send())
        looped(0, line, finish_line)
        looped(0, line, finish_across)
        for a in both:
            across_far(a).wait_send()

    settle_body(
        steps, meanwhile, part_grad, grad_out, resid, norm_gain, proj_weight,
        conv_sum, conv_gain, conv_taps, conv_value, conv_gate,
        side_out, feature_cols, proj, value_grad, gate_input_grad,
        full, grads, extended, *settle_sems,
    )


def relay_experts(operands, collective_id):
    routes, resid, w_gate, conv_sum = operands[0], operands[3], operands[5], operands[8]
    steps, tp_count = lax.axis_size("sp"), lax.axis_size("tp")
    line = steps // 2
    tok_rows, model_width = resid.shape
    count = 3 * tok_rows // steps
    width = model_width // tp_count
    hidden = w_gate.shape[1]
    kind = resid.dtype
    block = (steps, count, width)
    channels = conv_sum.shape[1]
    tail_rows = conv_sum.shape[0] + operands[11].shape[0] + 1
    outs = [
        jax.ShapeDtypeStruct((model_width, hidden), kind),
        jax.ShapeDtypeStruct((model_width, hidden), kind),
        jax.ShapeDtypeStruct((hidden, model_width), kind),
        jax.ShapeDtypeStruct((model_width // steps, channels), jnp.float32),
        jax.ShapeDtypeStruct((tok_rows, channels), kind),
        jax.ShapeDtypeStruct((tok_rows, channels), kind),
    ]
    held = pl.BlockSpec(memory_space=pltpu.VMEM)
    outside = pl.BlockSpec(memory_space=pltpu.HBM)

    def sems(*shape):
        return pltpu.SemaphoreType.DMA(shape)

    return pl.pallas_call(
        functools.partial(relay_kernel, steps),
        out_shape=tuple(outs),
        in_specs=[outside] * len(operands),
        out_specs=tuple(held for _ in outs),
        scratch_shapes=[pltpu.VMEM(x.shape, x.dtype) for x in operands]
        + [
            pltpu.VMEM((tok_rows, width), kind),
            pltpu.VMEM((steps,) + conv_sum.shape, kind),
            pltpu.VMEM((steps, tp_count, tok_rows // tp_count, model_width // steps), kind),
            pltpu.VMEM((tok_rows, model_width), kind),
            pltpu.VMEM((tok_rows, model_width), kind),
            pltpu.VMEM((tail_rows, channels), jnp.float32),
            pltpu.VMEM((tok_rows, model_width), kind),
            pltpu.VMEM((2 * routes.shape[0], tok_rows), jnp.float32),
            pltpu.VMEM((line, 2 * routes.shape[0], tok_rows), jnp.float32),
            pltpu.VMEM((line, steps, tok_rows), jnp.float32),
            pltpu.VMEM((line, steps, tok_rows), jnp.float32),
            pltpu.VMEM((tok_rows, tok_rows), kind),
            pltpu.VMEM((steps, count, tok_rows), kind),
            pltpu.VMEM((2, line, tok_rows, width), kind),
            pltpu.VMEM((2, line, 2, count, width), kind),
            pltpu.VMEM((2, line, count, width), kind),
            pltpu.VMEM((2, count, width), kind),
            pltpu.VMEM((2, steps, count, model_width), kind),
        ]
        + [pltpu.VMEM((steps, count, hidden), kind)] * 3
        + [pltpu.VMEM((steps, count, model_width), kind), pltpu.VMEM((2,) + block, kind)]
        + [pltpu.VMEM(block, kind)] * 4
        + [pltpu.VMEM(conv_sum.shape, kind)]
        + [sems(len(operands)), sems(line), sems(line), sems(2, 2, line), sems(2, line), sems(2, 2, line)]
        + [sems(2, line), sems(2, line), sems(2), sems(2, steps)]
        + [sems(2, steps)] * 6
        + [sems(steps)] * 10
        + [sems(tp_count)] * 6
        + [sems(1)]
        + [sems(steps)] * 8
        + [sems(1)] * 2,
        compiler_params=pltpu.CompilerParams(
            collective_id=collective_id, has_side_effects=True, vmem_limit_bytes=42 << 20
        ),
    )(*(pltpu.with_memory_space_constraint(x, pltpu.HBM) for x in operands))


def last_kernel(count, *refs):
    ins, outs, sem = refs[:count], refs[count:-1], refs[-1]
    moves = [pltpu.make_async_copy(a, b, sem.at[i]) for i, (a, b) in enumerate(zip(ins, outs))]
    for move in moves:
        move.start()
    for move in moves:
        move.wait()


def last_stage(results):
    return pl.pallas_call(
        functools.partial(last_kernel, len(results)),
        out_shape=tuple(jax.ShapeDtypeStruct(x.shape, x.dtype) for x in results),
        in_specs=[pl.BlockSpec(memory_space=pltpu.VMEM)] * len(results),
        out_specs=tuple(pl.BlockSpec(memory_space=pl.ANY) for _ in results),
        scratch_shapes=[pltpu.SemaphoreType.DMA((len(results),))],
        compiler_params=pltpu.CompilerParams(vmem_limit_bytes=16 << 20),
    )(*results)


def local(
    grad_out,
    resid,
    norm_gain,
    routes,
    route_weights,
    gate_weight,
    up_weight,
    down_weight,
    proj_weight,
    conv_sum,
    conv_gain,
    conv_taps,
    conv_value,
    conv_gate,
):
    tok_rows, model_width = resid.shape
    sp_count = lax.axis_size("sp")
    tp_count = lax.axis_size("tp")
    capacity = 3 * tok_rows // sp_count
    col_count = model_width // tp_count
    channels = conv_sum.shape[1]
    aligned = capacity % 16 == 0 and model_width % (128 * sp_count) == 0 and channels == GROUP
    if aligned and sp_count % 4 == 0:
        operands = (
            routes.T,
            route_weights.T,
            grad_out,
            resid,
            norm_gain[None],
            gate_weight[0],
            up_weight[0],
            down_weight[0],
            conv_sum,
            conv_gain[None],
            proj_weight,
            conv_taps,
            conv_value,
            conv_gate,
        )
        gate_grad, up_grad, down_grad, *rest = last_stage(relay_experts(operands, 4))
        return (gate_grad[None], up_grad[None], down_grad[None], *rest)
    resid_f = resid.astype(jnp.float32)
    inv_rms = lax.rsqrt(jnp.mean(resid_f * resid_f, axis=-1, keepdims=True) + 1e-06)
    normed = (resid_f * inv_rms * norm_gain).astype(jnp.bfloat16)
    my_sp = lax.axis_index("sp")
    away = (routes - my_sp) % sp_count
    steps_away = jnp.arange(sp_count, dtype=jnp.int32)
    named = away[:, :, None] == steps_away[None, None, :]
    chosen = jnp.any(named, axis=1)
    weight_of = jnp.sum(jnp.where(named, route_weights[:, :, None], 0.0), axis=1)
    token_ids = jnp.arange(tok_rows, dtype=jnp.int32)
    earlier = (token_ids[None, :] < token_ids[:, None]).astype(jnp.bfloat16)
    rank = jnp.dot(earlier, chosen.astype(jnp.bfloat16), preferred_element_type=jnp.float32)
    rank = jnp.where(chosen, rank, -1.0).astype(jnp.int32)
    slots = jnp.arange(capacity, dtype=jnp.int32)
    held = rank.T[:, None, :] == slots[None, :, None]
    slot_weight = jnp.sum(jnp.where(held, weight_of.T[:, None, :], 0.0), axis=2)
    pick = held.astype(jnp.bfloat16).reshape(sp_count * capacity, tok_rows)
    first_col = lax.axis_index("tp") * col_count
    normed_part = lax.dynamic_slice_in_dim(normed, first_col, col_count, 1)
    cots_part = lax.dynamic_slice_in_dim(grad_out, first_col, col_count, 1)
    slot_weight = slot_weight.reshape(-1, 1)
    send_rows = jnp.dot(pick, normed_part, preferred_element_type=jnp.float32).astype(jnp.bfloat16)
    send_cots = jnp.dot(pick, cots_part, preferred_element_type=jnp.float32)
    send_cots = (send_cots * slot_weight).astype(jnp.bfloat16)
    own_pick = pick[:capacity]
    own_rows = jnp.dot(own_pick, normed, preferred_element_type=jnp.float32).astype(jnp.bfloat16)
    own_cots = jnp.dot(own_pick, grad_out, preferred_element_type=jnp.float32)
    own_cots = (own_cots * slot_weight[:capacity]).astype(jnp.bfloat16)
    summed = conv_sum.astype(jnp.float32).reshape(tok_rows, channels // GROUP, GROUP)
    centre = summed - jnp.mean(summed, axis=-1, keepdims=True)
    inv_std = lax.rsqrt(jnp.mean(centre * centre, axis=-1, keepdims=True) + 1e-05)
    grouped = centre * inv_std
    chan_normed = grouped.reshape(tok_rows, channels)
    pre_act = chan_normed * conv_gain
    sigma_conv = jax.nn.sigmoid(pre_act)
    conv_out = (pre_act * sigma_conv).astype(jnp.bfloat16)
    routed_rows, routed_cots = spread(
        (
            send_rows.reshape(sp_count, capacity, col_count),
            send_cots.reshape(sp_count, capacity, col_count),
        ),
        (own_rows, own_cots),
        None,
        True,
        False,
        0,
    )
    routed_rows = routed_rows.reshape(sp_count * capacity, model_width)
    routed_cots = routed_cots.reshape(sp_count * capacity, model_width)
    gate_grad, up_grad, down_grad, partial_value = expert_backward(
        routed_rows, routed_cots, gate_weight[0], up_weight[0], down_weight[0]
    )
    returned = combine(
        partial_value.reshape(sp_count, capacity, model_width).astype(jnp.bfloat16), 1
    ).reshape(sp_count * capacity, col_count)
    normed_part_grad = contract_rows(pick, returned).astype(jnp.bfloat16)
    chunks = 4
    normed_grad, all_out = spread(
        (normed_part_grad.reshape(chunks, tok_rows // chunks, col_count),),
        None,
        conv_out,
        True,
        False,
        2,
    )
    normed_grad = normed_grad.reshape(tok_rows, model_width)
    feature_grad = normed_grad.astype(jnp.float32) * norm_gain
    cubed = inv_rms * inv_rms * inv_rms
    resid_grad = (
        grad_out.astype(jnp.float32)
        + inv_rms * feature_grad
        - resid_f * cubed * jnp.mean(resid_f * feature_grad, axis=-1, keepdims=True)
    ).astype(jnp.bfloat16)
    share = tok_rows // tp_count
    feat_rows = model_width // sp_count
    tokens_part = lax.dynamic_slice_in_dim(resid_grad, lax.axis_index("tp") * share, share, 0)
    by_feature = tokens_part.reshape(share, sp_count, feat_rows).transpose(1, 0, 2)
    own_features = lax.dynamic_slice_in_dim(resid_grad, my_sp * feat_rows, feat_rows, 1)
    (feature_cols,) = spread(
        (by_feature,), (own_features.reshape(tp_count, share, feat_rows),), None, False, True, 3
    )
    proj_grad = contract_rows(
        feature_cols.reshape(sp_count * tok_rows, feat_rows),
        all_out.reshape(sp_count * tok_rows, channels),
    )
    out_grad = jnp.dot(resid_grad, proj_weight, preferred_element_type=jnp.float32)
    normal_grad = (
        out_grad * sigma_conv * (1.0 + pre_act * (1.0 - sigma_conv)) * conv_gain
    ).reshape(tok_rows, channels // GROUP, GROUP)
    sum_grad = inv_std * (
        normal_grad
        - jnp.mean(normal_grad, axis=-1, keepdims=True)
        - grouped * jnp.mean(normal_grad * grouped, axis=-1, keepdims=True)
    )
    sum_grad = sum_grad.reshape(tok_rows, channels)
    following = passed_along(sum_grad[: CONV_K - 1], "sp", -1)
    extended = jnp.concatenate([sum_grad, following], axis=0)
    gated_grad = lax.conv_general_dilated(
        extended[None],
        conv_taps[::-1][:, None, :],
        (1,),
        ((0, 0),),
        dimension_numbers=("NWC", "WIO", "NWC"),
        feature_group_count=channels,
        precision=lax.Precision.HIGHEST,
    )[0]
    sigma_gate = jax.nn.sigmoid(conv_gate.astype(jnp.float32))
    value_grad = (gated_grad * sigma_gate).astype(jnp.bfloat16)
    gate_input_grad = (
        gated_grad * conv_value.astype(jnp.float32) * sigma_gate * (1.0 - sigma_gate)
    ).astype(jnp.bfloat16)
    return (gate_grad[None], up_grad[None], down_grad[None], proj_grad, value_grad, gate_input_grad)


def solution(mesh):
    in_specs = (
        P("sp", None),
        P("sp", None),
        P(),
        P("sp", None),
        P("sp", None),
        P("sp", None, "tp"),
        P("sp", None, "tp"),
        P("sp", "tp", None),
        P(None, "tp"),
        P("sp", "tp"),
        P("tp"),
        P(None, "tp"),
        P("sp", "tp"),
        P("sp", "tp"),
    )
    out_specs = (
        P("sp", None, "tp"),
        P("sp", None, "tp"),
        P("sp", "tp", None),
        P("sp", "tp"),
        P("sp", "tp"),
        P("sp", "tp"),
    )
    return jax.shard_map(local, mesh=mesh, in_specs=in_specs, out_specs=out_specs, check_vma=False)
```

```python
import functools

import jax
import jax.numpy as jnp
from jax import lax
from jax.experimental import pallas as pl
from jax.experimental.pallas import tpu as pltpu
from jax.sharding import PartitionSpec as P

CONV_K = 31
GROUP = 128
MESH = pl.DeviceIdType.MESH


CLAMP_LIMIT = 7.0
SLOPE_ALPHA = 1.702


def passed_along(block, axis, distance):
    devices = range(lax.axis_size(axis))
    route = [(i - distance, i) for i in devices if i - distance in devices]
    return lax.ppermute(block, axis, route)


def tp_places():
    mine = lax.axis_index("tp")
    near = mine + 1 - 2 * (mine % 2)
    far = (mine + 2) % 4
    diag = (near + 2) % 4
    return mine, near, far, diag


def meet(steps, over_sp, near, far):
    s, t = lax.axis_index("sp"), lax.axis_index("tp")
    barrier = pltpu.get_barrier_semaphore()
    pl.semaphore_signal(barrier, inc=1, device_id=(s, near), device_id_type=MESH)
    pl.semaphore_signal(barrier, inc=1, device_id=(s, far), device_id_type=MESH)
    total = 2
    if over_sp:

        def greet(d, carry):
            pl.semaphore_signal(
                barrier, inc=1, device_id=((s + d) % steps, t), device_id_type=MESH
            )
            return carry

        lax.fori_loop(1, steps, greet, 0)
        total += steps - 1
    pl.semaphore_wait(barrier, total)


def crossing_first(steps, k):
    return steps // 2 + ((k + 1) // 2) * (2 * (k % 2) - 1)


def looped(first, last, body):
    def step(k, carry):
        body(k)
        return carry

    lax.fori_loop(first, last, step, 0)


def spread_kernel(count, steps, over_sp, in_lanes, absolute, beside, sp_count, *refs):
    refs = list(refs)
    sends, refs = refs[:count], refs[count:]
    fulls, refs = (refs[:count], refs[count:]) if over_sp else (None, refs)
    side, refs = (refs[0], refs[1:]) if beside else (None, refs)
    outs, refs = refs[:count], refs[count:]
    side_out, refs = (refs[0], refs[1:]) if beside else (None, refs)
    own_sem, a_send, a_recv, b_send, f_send, c_send, near_recv, fwd_recv, far_recv = refs[:9]
    s = lax.axis_index("sp")
    t, near, far, _ = tp_places()
    width = sends[0].shape[-1]

    def place(c, d, q):
        if in_lanes:
            return outs[c].at[d, :, pl.ds(pl.multiple_of(q * width, width), width)]
        return outs[c].at[d, q]

    def source(c, d):
        return sends[c].at[(s + d) % steps if absolute else d]

    def own(c, d):
        if over_sp:
            return pltpu.make_async_copy(fulls[c], outs[c].at[0], own_sem.at[c, 0])
        return pltpu.make_async_copy(source(c, d), place(c, d, t), own_sem.at[c, d])

    def to_sp(c, d):
        return pltpu.make_async_remote_copy(
            src_ref=source(c, d),
            dst_ref=place(c, d, t),
            send_sem=a_send.at[c, d],
            recv_sem=a_recv.at[c, d],
            device_id=((s + d) % steps, t),
            device_id_type=MESH,
        )

    def to_tp(c, d, q, target, send_sem, recv_sem):
        return pltpu.make_async_remote_copy(
            src_ref=place(c, d, q),
            dst_ref=place(c, d, q),
            send_sem=send_sem.at[c, d],
            recv_sem=recv_sem.at[c, d],
            device_id=(s, target),
            device_id_type=MESH,
        )

    def near_copy(c, d):
        return to_tp(c, d, t, near, b_send, near_recv)

    def far_copy(c, d):
        return to_tp(c, d, t, far, f_send, far_recv)

    def fwd_copy(c, d):
        return to_tp(c, d, far, near, c_send, fwd_recv)

    def side_copy(d):
        side_send, side_recv = refs[10:12]
        return pltpu.make_async_remote_copy(
            src_ref=side,
            dst_ref=side_out.at[d],
            send_sem=side_send.at[d],
            recv_sem=side_recv.at[d],
            device_id=((s + d) % sp_count, t),
            device_id_type=MESH,
        )

    def own_side():
        return pltpu.make_async_copy(side, side_out.at[0], refs[9].at[0])

    def share(c, d):
        far_copy(c, d).start()
        near_copy(c, d).start()

    def forward(c, d):
        far_copy(c, d).wait_recv()
        fwd_copy(c, d).start()

    def finish(c, d):
        near_copy(c, d).wait()
        far_copy(c, d).wait_send()
        fwd_copy(c, d).wait()

    def loop(first, last, body):
        def each(k):
            d = k + 1 if over_sp else k
            for c in range(count):
                body(c, d)

        looped(first, last, each)

    meet(sp_count, over_sp or beside, near, far)
    if over_sp:
        loop(0, steps - 1, lambda c, d: to_sp(c, d).start())
        for c in range(count):
            own(c, 0).start()

        def pass_on(k):
            for c in range(count):
                d = k + 1
                to_sp(c, d).wait_recv()
                share(c, d)

        def pass_on_twice(k):
            pass_on(k)
            for c in range(count):
                forward(c, k)

        pass_on(0)
        looped(1, steps - 1, pass_on_twice)
        loop(steps - 2, steps - 1, forward)
        loop(0, steps - 1, finish)
        loop(0, steps - 1, lambda c, d: to_sp(c, d).wait_send())
        for c in range(count):
            own(c, 0).wait()
    else:
        loop(0, steps, lambda c, d: own(c, d).start())
        if beside:
            looped(0, sp_count - 1, lambda k: side_copy(crossing_first(sp_count, k)).start())
            own_side().start()

        def share_own(c, d):
            own(c, d).wait()
            share(c, d)

        loop(0, steps, share_own)
        loop(0, steps, forward)
        loop(0, steps, finish)
        if beside:
            looped(0, sp_count - 1, lambda k: side_copy(crossing_first(sp_count, k)).wait())
            own_side().wait()


def spread(sends, fulls, side, in_lanes, absolute, collective_id):
    count = len(sends)
    steps, rows, width = sends[0].shape
    tp_count, sp_count = lax.axis_size("tp"), lax.axis_size("sp")
    over_sp, beside = fulls is not None, side is not None
    shape = (steps, rows, tp_count * width) if in_lanes else (steps, tp_count, rows, width)
    out_shape = [jax.ShapeDtypeStruct(shape, x.dtype) for x in sends]
    operands = list(sends) + (list(fulls) if over_sp else []) + ([side] if beside else [])
    scratch = [pltpu.SemaphoreType.DMA((count, steps))] * 9
    if beside:
        out_shape.append(jax.ShapeDtypeStruct((sp_count,) + side.shape, side.dtype))
        scratch += [pltpu.SemaphoreType.DMA((1,))] + [pltpu.SemaphoreType.DMA((sp_count,))] * 2
    return pl.pallas_call(
        functools.partial(
            spread_kernel, count, steps, over_sp, in_lanes, absolute, beside, sp_count
        ),
        out_shape=tuple(out_shape),
        in_specs=[pl.BlockSpec(memory_space=pltpu.VMEM)] * len(operands),
        out_specs=tuple(pl.BlockSpec(memory_space=pltpu.VMEM) for _ in out_shape),
        scratch_shapes=scratch,
        compiler_params=pltpu.CompilerParams(
            collective_id=collective_id, has_side_effects=True, vmem_limit_bytes=40 << 20
        ),
    )(*operands)


def combine_kernel(
    steps, part, out, near_in, pair, far_in, total,
    n0_send, n0_recv, n1_send, n1_recv, f_send, f_recv, a_send, a_recv,
):
    s = lax.axis_index("sp")
    t, near, far, diag = tp_places()
    width = out.shape[-1]

    def lanes(q):
        return pl.ds(pl.multiple_of(q * width, width), width)

    def near_copy(d, which, q, send_sem, recv_sem):
        return pltpu.make_async_remote_copy(
            src_ref=part.at[d, :, lanes(q)],
            dst_ref=near_in.at[which, d],
            send_sem=send_sem.at[d],
            recv_sem=recv_sem.at[d],
            device_id=(s, near),
            device_id_type=MESH,
        )

    def for_near(d):
        return near_copy(d, 0, near, n0_send, n0_recv)

    def for_diag(d):
        return near_copy(d, 1, diag, n1_send, n1_recv)

    def far_copy(d):
        return pltpu.make_async_remote_copy(
            src_ref=pair.at[d],
            dst_ref=far_in.at[d],
            send_sem=f_send.at[d],
            recv_sem=f_recv.at[d],
            device_id=(s, far),
            device_id_type=MESH,
        )

    def back(d):
        return pltpu.make_async_remote_copy(
            src_ref=total.at[d],
            dst_ref=out.at[d],
            send_sem=a_send.at[d],
            recv_sem=a_recv.at[d],
            device_id=((s + steps - d) % steps, t),
            device_id_type=MESH,
        )

    meet(steps, True, near, far)

    def open_up(d):
        for_diag(d).start()
        for_near(d).start()

    def add_pair(d):
        for_diag(d).wait_recv()
        mine = part[d, :, lanes(far)].astype(jnp.float32)
        pair[d] = (mine + near_in[1, d].astype(jnp.float32)).astype(pair.dtype)
        far_copy(d).start()

    def whole(d):
        for_near(d).wait_recv()
        far_copy(d).wait_recv()
        mine = part[d, :, lanes(t)].astype(jnp.float32)
        both = mine + near_in[0, d].astype(jnp.float32)
        return (both + far_in[d].astype(jnp.float32)).astype(out.dtype)

    def send_back(d):
        total[d] = whole(d)
        back(d).start()

    def at(k):
        return crossing_first(steps, k)

    lag = min(3, steps - 1)
    looped(0, steps - 1, lambda k: open_up(at(k)))
    open_up(0)
    looped(0, lag, lambda k: add_pair(at(k)))

    def middle(k):
        add_pair(at(k))
        send_back(at(k - lag))

    looped(lag, steps - 1, middle)
    add_pair(0)
    looped(steps - 1 - lag, steps - 1, lambda k: send_back(at(k)))
    out[0] = whole(0)

    def finish(d):
        for_near(d).wait_send()
        for_diag(d).wait_send()
        far_copy(d).wait_send()

    looped(0, steps, finish)
    looped(1, steps, lambda d: back(d).wait())


def combine(part, collective_id):
    steps, rows, all_width = part.shape
    width = all_width // lax.axis_size("tp")
    block = (steps, rows, width)
    return pl.pallas_call(
        functools.partial(combine_kernel, steps),
        out_shape=jax.ShapeDtypeStruct(block, part.dtype),
        in_specs=[pl.BlockSpec(memory_space=pltpu.VMEM)],
        out_specs=pl.BlockSpec(memory_space=pltpu.VMEM),
        scratch_shapes=[
            pltpu.VMEM((2,) + block, part.dtype),
            pltpu.VMEM(block, part.dtype),
            pltpu.VMEM(block, part.dtype),
            pltpu.VMEM(block, part.dtype),
        ]
        + [pltpu.SemaphoreType.DMA((steps,))] * 8,
        compiler_params=pltpu.CompilerParams(
            collective_id=collective_id, has_side_effects=True, vmem_limit_bytes=40 << 20
        ),
    )(part)


def contract_rows(left_side, right_side):
    return lax.dot_general(
        left_side, right_side, (((0,), (0,)), ((), ())), preferred_element_type=jnp.float32
    )


def contract_cols(left_side, right_side):
    return lax.dot_general(
        left_side, right_side, (((1,), (1,)), ((), ())), preferred_element_type=jnp.float32
    )


def expert_backward(routed_rows, routed_cots, w_gate, w_up, w_down):
    gate_pre = jnp.dot(routed_rows, w_gate, preferred_element_type=jnp.float32)
    up_pre = jnp.dot(routed_rows, w_up, preferred_element_type=jnp.float32)
    gate_clamped = jnp.minimum(gate_pre, CLAMP_LIMIT)
    up_clamped = jnp.clip(up_pre, -CLAMP_LIMIT, CLAMP_LIMIT)
    sigma = jax.nn.sigmoid(SLOPE_ALPHA * gate_clamped)
    gated = gate_clamped * sigma
    act = ((up_clamped + 1.0) * gated).astype(jnp.bfloat16)
    down_grad = contract_rows(act, routed_cots).astype(jnp.bfloat16)
    act_grad = contract_cols(routed_cots, w_down)
    inside = (up_pre > -CLAMP_LIMIT) & (up_pre < CLAMP_LIMIT)
    up_pre_grad = jnp.where(inside, act_grad * gated, 0.0).astype(jnp.bfloat16)
    slope = sigma + SLOPE_ALPHA * gate_clamped * sigma * (1.0 - sigma)
    gate_pre_grad = jnp.where(
        gate_pre < CLAMP_LIMIT, act_grad * (up_clamped + 1.0) * slope, 0.0
    ).astype(jnp.bfloat16)
    gate_grad = contract_rows(routed_rows, gate_pre_grad).astype(jnp.bfloat16)
    up_grad = contract_rows(routed_rows, up_pre_grad).astype(jnp.bfloat16)
    partial_value = contract_cols(gate_pre_grad, w_gate) + contract_cols(up_pre_grad, w_up)
    return (gate_grad, up_grad, down_grad, partial_value)


def line_schedule(line):
    codes = []
    for z in range(line):
        slots = [[(z, 0), 0, 0, 0], [(z, 1), 1, 1, 0]]
        groups = [[b for b in (z - k, z + k) if 0 <= b < line] for k in range(1, line)]
        groups = [g for g in groups if g]
        for k, group in enumerate(groups, 1):
            following = k + 1 if k < len(groups) else 0
            added = [[(b, 0), 0, 0, 0] for b in group] + [[(b, 1), 0, 0, 0] for b in group]
            many = len(group)
            added[0][3] = group[0] + 1
            if many > 1:
                added[many][3] = group[1] + 1
            added[1][1] = following
            added[many][2] = following
            slots += added
        row = []
        for (zb, col), first, second, meeting in slots:
            row.append((((meeting * 16 + second) * 16 + first) * 2 + col) * 16 + zb)
        codes.append(row)
    return codes


def settle_body(
    steps, meanwhile, part_grad, grad_out, resid, norm_gain, proj_weight,
    conv_sum, conv_gain, conv_taps, conv_value, conv_gate,
    side_out, feature_cols, proj, value_grad, gate_input_grad,
    full, grads, extended, far_send, far_recv, near_send, near_recv, fwd_send, fwd_recv,
    own_sem, x_send, x_recv, xf_send, xf_recv, xn_send, xn_recv, xw_send, xw_recv,
    h_send, h_recv,
):
    s = lax.axis_index("sp")
    t, near, far, diag = tp_places()
    tok_rows, width = part_grad.shape
    chunks, share = feature_cols.shape[1], feature_cols.shape[2]
    feat_rows = feature_cols.shape[3]
    overlap = conv_taps.shape[0] - 1

    def rows_of(j):
        return pl.ds(pl.multiple_of(j * share, share), share)

    def lanes(q):
        return pl.ds(pl.multiple_of(q * width, width), width)

    def mine_at(j):
        return full.at[rows_of(j), lanes(t)]

    def own_copy():
        return pltpu.make_async_copy(part_grad, full.at[:, lanes(t)], own_sem.at[0])

    def gather(j, q, src, target, send_sem, recv_sem):
        return pltpu.make_async_remote_copy(
            src_ref=src,
            dst_ref=full.at[rows_of(j), lanes(q)],
            send_sem=send_sem.at[j],
            recv_sem=recv_sem.at[j],
            device_id=(s, target),
            device_id_type=MESH,
        )

    def to_far(j):
        return gather(j, t, part_grad.at[rows_of(j), :], far, far_send, far_recv)

    def to_near(j):
        return gather(j, t, part_grad.at[rows_of(j), :], near, near_send, near_recv)

    def pass_near(j):
        return gather(j, far, full.at[rows_of(j), lanes(far)], near, fwd_send, fwd_recv)

    def spread_out(d):
        feats = pl.ds(pl.multiple_of(((s + d) % steps) * feat_rows, feat_rows), feat_rows)
        return pltpu.make_async_remote_copy(
            src_ref=grads.at[rows_of(t), feats],
            dst_ref=feature_cols.at[d, t],
            send_sem=x_send.at[d],
            recv_sem=x_recv.at[d],
            device_id=((s + d) % steps, t),
            device_id_type=MESH,
        )

    def beside(d, q, target, send_sem, recv_sem):
        return pltpu.make_async_remote_copy(
            src_ref=feature_cols.at[d, q],
            dst_ref=feature_cols.at[d, q],
            send_sem=send_sem.at[d],
            recv_sem=recv_sem.at[d],
            device_id=(s, target),
            device_id_type=MESH,
        )

    def x_far(d):
        return beside(d, t, far, xf_send, xf_recv)

    def x_near(d):
        return beside(d, t, near, xn_send, xn_recv)

    def x_pass(d):
        return beside(d, far, near, xw_send, xw_recv)

    def halo():
        return pltpu.make_async_remote_copy(
            src_ref=extended.at[pl.ds(0, overlap + 2)],
            dst_ref=extended.at[pl.ds(tok_rows, overlap + 2)],
            send_sem=h_send.at[0],
            recv_sem=h_recv.at[0],
            device_id=((s + steps - 1) % steps, t),
            device_id_type=MESH,
        )

    gain = norm_gain[...]

    def settle(j):
        here = rows_of(j)
        feature_grad = full[here, :].astype(jnp.float32) * gain
        x = resid[here, :].astype(jnp.float32)
        scale = lax.rsqrt(jnp.mean(x * x, axis=-1, keepdims=True) + 1e-06)
        cubed = scale * scale * scale
        mean = jnp.mean(x * feature_grad, axis=-1, keepdims=True)
        value = grad_out[here, :].astype(jnp.float32) + scale * feature_grad - x * cubed * mean
        grads[here, :] = value.astype(grads.dtype)

    def crossing(k):
        return crossing_first(steps, k)

    for j in (far, diag, t, near):
        to_far(j).start()
    for j in (near, t, diag, far):
        to_near(j).start()
    own_copy().start()
    summed = conv_sum[...].astype(jnp.float32)
    centre = summed - jnp.mean(summed, axis=-1, keepdims=True)
    inv_std = lax.rsqrt(jnp.mean(centre * centre, axis=-1, keepdims=True) + 1e-05)
    grouped = centre * inv_std
    pre_act = grouped * conv_gain[...]
    sigma = jax.nn.sigmoid(pre_act)
    slope = sigma * (1.0 + pre_act * (1.0 - sigma)) * conv_gain[...]
    own_copy().wait()

    def arrive(j):
        to_far(j).wait_recv()
        pass_near(j).start()

    def whole(j):
        to_near(j).wait_recv()
        pass_near(j).wait_recv()

    arrive(t)
    arrive(near)
    whole(t)
    settle(t)
    looped(0, steps - 1, lambda k: spread_out(crossing(k)).start())
    meanwhile()
    arrive(far)
    arrive(diag)
    for j in (near, far, diag):
        whole(j)
        settle(j)
    feats = pl.ds(pl.multiple_of(s * feat_rows, feat_rows), feat_rows)
    feature_cols[0] = grads[:, feats].reshape(chunks, share, feat_rows)
    out_grad = jnp.dot(grads[...], proj_weight[...], preferred_element_type=jnp.float32)
    normal = out_grad * slope
    sum_grad = inv_std * (
        normal
        - jnp.mean(normal, axis=-1, keepdims=True)
        - grouped * jnp.mean(normal * grouped, axis=-1, keepdims=True)
    )
    extended[pl.ds(0, tok_rows), :] = sum_grad
    halo().start()

    def share_out(d):
        spread_out(d).wait_recv()
        x_far(d).start()
        x_near(d).start()

    def pass_on(d):
        x_far(d).wait_recv()
        x_pass(d).start()

    def term(d):
        left = feature_cols[d].reshape(tok_rows, feat_rows)
        return contract_rows(left, side_out[d])

    def gather_term(d):
        x_near(d).wait_recv()
        x_pass(d).wait_recv()
        proj[...] += term(d)

    proj[...] = term(0)
    looped(0, steps - 1, lambda k: share_out(crossing(k)))
    looped(0, steps - 1, lambda k: pass_on(crossing(k)))
    halo().wait()

    @pl.when(s == steps - 1)
    def _():
        extended[pl.ds(tok_rows, overlap + 2), :] = jnp.zeros(
            (overlap + 2, extended.shape[1]), extended.dtype
        )

    gated_grad = extended[pl.ds(overlap, tok_rows), :] * conv_taps[pl.ds(0, 1), :]
    for j in range(1, overlap + 1):
        gated_grad += extended[pl.ds(overlap - j, tok_rows), :] * conv_taps[pl.ds(j, 1), :]
    sigma_gate = jax.nn.sigmoid(conv_gate[...].astype(jnp.float32))
    value_grad[...] = (gated_grad * sigma_gate).astype(value_grad.dtype)
    gate_input_grad[...] = (
        gated_grad * conv_value[...].astype(jnp.float32) * sigma_gate * (1.0 - sigma_gate)
    ).astype(gate_input_grad.dtype)
    looped(0, steps - 1, lambda k: gather_term(crossing(k)))

    def finish(k):
        d = crossing(k)
        spread_out(d).wait_send()
        x_near(d).wait_send()
        x_far(d).wait_send()
        x_pass(d).wait_send()

    looped(0, steps - 1, finish)

    def finish_gather(j):
        to_far(j).wait_send()
        to_near(j).wait_send()
        pass_near(j).wait_send()

    looped(0, chunks, finish_gather)


def relay_kernel(
    steps, routes_in, weights_in, grad_in, resid_in, gain_in, gate_in, up_in, down_in, sum_in,
    conv_gain_in, proj_in, taps_in, value_in, convgate_in,
    gate_grad, up_grad, down_grad, proj, value_grad, gate_input_grad,
    routes, route_weights, grad_out, resid, norm_gain, w_gate, w_up, w_down, conv_sum, conv_gain,
    proj_weight, conv_taps, conv_value, conv_gate, part_grad, side_out, feature_cols, full, grads,
    extended, normed, info, infos, ranks, weights, before, picks,
    tok, over, cross, cross_far, held, act, gate_pg, up_pg, part,
    near_in, pair, far_in, total, ret, side,
    own_sem, info_send, info_recv, line_send, line_recv, end_send, cross_recv,
    across_send, afar_send, arr_recv, b_send, f_send, c_send, near_recv, fwd_recv, far_recv,
    n0_send, n0_recv, n1_send, n1_recv, g_send, g_recv, r_send, r_recv, s_send, s_recv,
    *settle_sems,
):
    s = lax.axis_index("sp")
    t, near, far, diag = tp_places()
    line = steps // 2
    z, y = s // 2, s % 2
    across = s + 1 - 2 * y
    tok_rows, width = part_grad.shape
    count = cross.shape[2]
    hidden = w_gate.shape[1]
    model_width = resid.shape[1]
    both = (0, 1)
    kind = held.dtype
    sources = (grad_out, normed)

    def lanes(q):
        return pl.ds(pl.multiple_of(q * width, width), width)

    def remote(src, dst, send_sem, recv_sem, sp_to, tp_to):
        return pltpu.make_async_remote_copy(
            src_ref=src,
            dst_ref=dst,
            send_sem=send_sem,
            recv_sem=recv_sem,
            device_id=(sp_to, tp_to),
            device_id_type=MESH,
        )

    moves = [
        pltpu.make_async_copy(a, b, own_sem.at[i])
        for i, (a, b) in enumerate(
            (
                (grad_in, grad_out),
                (routes_in, routes),
                (weights_in, route_weights),
                (resid_in, resid),
                (gain_in, norm_gain),
                (sum_in, conv_sum),
                (conv_gain_in, conv_gain),
                (gate_in, w_gate),
                (up_in, w_up),
                (down_in, w_down),
                (proj_in, proj_weight),
                (taps_in, conv_taps),
                (value_in, conv_value),
                (convgate_in, conv_gate),
            )
        )
    ]

    def info_copy(dz):
        peer = ((z + dz) % line) * 2 + y
        return remote(info, infos.at[z], info_send.at[dz], info_recv.at[z], peer, t)

    def info_from(zb):
        return remote(info, infos.at[zb], info_send.at[0], info_recv.at[zb], across, t)

    def line_copy(a, zb, src, up):
        to = s + 2 if up else s - 2
        return remote(src, tok.at[a, zb], line_send.at[a, up, zb], line_recv.at[a, zb], to, t)

    def end_copy(a, zb, col, up):
        to = s + 2 if up else s - 2
        j = 2 * zb + y
        if col == 0:
            dst, recv = held.at[a, j, :, lanes(t)], arr_recv.at[a, j]
        else:
            dst, recv = cross.at[a, zb], cross_recv.at[a, zb]
        return remote(over.at[a, zb, col], dst, end_send.at[a, col, zb], recv, to, t)

    def across_copy(a, zb):
        j = 2 * zb + y
        dst = held.at[a, j, :, lanes(t)]
        return remote(cross.at[a, zb], dst, across_send.at[a, zb], arr_recv.at[a, j], across, t)

    def across_far(a):
        dst = held.at[a, s, :, lanes(far)]
        return remote(cross_far.at[a], dst, afar_send.at[a], far_recv.at[a, s], across, t)

    def arrival(a, j):
        place = held.at[a, j, :, lanes(t)]
        return remote(place, place, f_send.at[a, j], arr_recv.at[a, j], s, far)

    def to_tp(a, j, q, target, send_sem, recv_sem):
        place = held.at[a, j, :, lanes(q)]
        return remote(place, place, send_sem.at[a, j], recv_sem.at[a, j], s, target)

    def near_copy(a, j):
        return to_tp(a, j, t, near, b_send, near_recv)

    def far_copy(a, j):
        return to_tp(a, j, t, far, f_send, far_recv)

    def fwd_copy(a, j):
        return to_tp(a, j, far, near, c_send, fwd_recv)

    def part_copy(j, which, q, send_sem, recv_sem):
        src, dst = part.at[j, :, lanes(q)], near_in.at[which, j]
        return remote(src, dst, send_sem.at[j], recv_sem.at[j], s, near)

    def for_near(j):
        return part_copy(j, 0, near, n0_send, n0_recv)

    def for_diag(j):
        return part_copy(j, 1, diag, n1_send, n1_recv)

    def pair_copy(j):
        return remote(pair.at[j], far_in.at[j], g_send.at[j], g_recv.at[j], s, far)

    def back(j):
        return remote(total.at[j], ret.at[s], r_send.at[j], r_recv.at[s], j, t)

    def back_from(e):
        return remote(total.at[e], ret.at[e], r_send.at[e], r_recv.at[e], e, t)

    def side_copy(d):
        to = (s + d) % steps
        return remote(side, side_out.at[d], s_send.at[d], s_recv.at[d], to, t)

    def table(zb):
        first, second = infos[zb, pl.ds(0, 1), :], infos[zb, pl.ds(1, 1), :]
        ids = lax.broadcasted_iota(jnp.int32, (steps, tok_rows), 0).astype(jnp.float32)
        chosen = (first == ids) | (second == ids)
        ones = jnp.where(chosen, 1.0, 0.0).astype(kind)
        rank = jnp.dot(ones, before[...], preferred_element_type=jnp.float32)
        ranks[zb] = jnp.where(chosen, rank, -1.0)
        weights[zb] = jnp.where(
            first == ids, infos[zb, pl.ds(2, 1), :], infos[zb, pl.ds(3, 1), :]
        )

    def pick(zb, e):
        slots = lax.broadcasted_iota(jnp.int32, (count, tok_rows), 0).astype(jnp.float32)
        return slots == ranks[zb, pl.ds(e, 1), :]

    def selected(a, zb, e, value):
        mask = pick(zb, e)
        hot = jnp.where(mask, 1.0, 0.0).astype(kind)
        out = jnp.dot(hot, value, preferred_element_type=jnp.float32)
        if a == 0:
            scale = jnp.where(mask, weights[zb, pl.ds(e, 1), :], 0.0)
            out = out * jnp.sum(scale, axis=1, keepdims=True)
        return out.astype(kind)

    def to_end(a, zb, value, up):
        end = z + 1 if up else z - 1
        for col in both:
            e = 2 * end + (y if col == 0 else 1 - y)
            over[a, zb, col] = selected(a, zb, e, value)
            end_copy(a, zb, col, up).start()

    def valid(m, up):
        return (z >= m) if up else (z + m < line)

    def block_at(m, up):
        return z - m if up else z + m

    def next_is_end(up):
        return (z + 1 == line - 1) if up else (z == 1)

    def next_is_inner(up):
        return (z + 1 < line - 1) if up else (z >= 2)

    def at_end(up):
        return (z == line - 1) if up else (z == 0)

    def share(a, j):
        far_copy(a, j).start()
        near_copy(a, j).start()

    def read_info(m, up):
        zb = block_at(m, up)

        @pl.when(valid(m, up))
        def _():
            info_from(zb).wait_recv()

        @pl.when(valid(m, up) & jnp.logical_not(at_end(up)))
        def _():
            table(zb)

    def handle(a, m, up):
        zb = block_at(m, up)
        j = 2 * zb + y

        @pl.when(valid(m, up) & at_end(up))
        def _():
            arrival(a, j).wait_recv()
            end_copy(a, zb, 1, up).wait_recv()
            across_copy(a, zb).start()
            share(a, j)

        @pl.when(valid(m, up) & jnp.logical_not(at_end(up)))
        def _():
            line_copy(a, zb, tok.at[a, zb], up).wait_recv()

            @pl.when(next_is_end(up))
            def _():
                to_end(a, zb, tok[a, zb], up)

            @pl.when(next_is_inner(up))
            def _():
                line_copy(a, zb, tok.at[a, zb], up).start()

            cross[a, zb] = selected(a, zb, across, tok[a, zb])
            across_copy(a, zb).start()
            held[a, j, :, lanes(t)] = selected(a, zb, s, tok[a, zb])
            share(a, j)

    def unless_own(j, body):
        @pl.when(j != s)
        def _():
            body()

    def experts(j):
        def settle():
            for a in both:
                near_copy(a, j).wait_recv()
                fwd_copy(a, j).wait_recv()

        unless_own(j, settle)
        gate_pre = jnp.dot(held[1, j], w_gate[...], preferred_element_type=jnp.float32)
        up_pre = jnp.dot(held[1, j], w_up[...], preferred_element_type=jnp.float32)
        act_grad = contract_cols(held[0, j], w_down[...])
        gate_clamped = jnp.minimum(gate_pre, CLAMP_LIMIT)
        up_clamped = jnp.clip(up_pre, -CLAMP_LIMIT, CLAMP_LIMIT)
        sigma = jax.nn.sigmoid(SLOPE_ALPHA * gate_clamped)
        gated = gate_clamped * sigma
        act[j] = ((up_clamped + 1.0) * gated).astype(kind)
        inside = (up_pre > -CLAMP_LIMIT) & (up_pre < CLAMP_LIMIT)
        up_g = jnp.where(inside, act_grad * gated, 0.0).astype(kind)
        slope = sigma + SLOPE_ALPHA * gate_clamped * sigma * (1.0 - sigma)
        gate_g = jnp.where(
            gate_pre < CLAMP_LIMIT, act_grad * (up_clamped + 1.0) * slope, 0.0
        ).astype(kind)
        gate_pg[j] = gate_g
        up_pg[j] = up_g
        for q in range(model_width // width):
            mine = pl.ds(q * width, width)
            value = contract_cols(gate_g, w_gate[mine, :]) + contract_cols(up_g, w_up[mine, :])
            part[j, :, mine] = value.astype(kind)
        for_diag(j).start()
        for_near(j).start()

    def add_pair(j):
        for_diag(j).wait_recv()
        mine = part[j, :, lanes(far)].astype(jnp.float32)
        pair[j] = (mine + near_in[1, j].astype(jnp.float32)).astype(kind)
        pair_copy(j).start()

    def whole(j):
        for_near(j).wait_recv()
        pair_copy(j).wait_recv()
        mine = part[j, :, lanes(t)].astype(jnp.float32)
        summed = mine + near_in[0, j].astype(jnp.float32)
        return (summed + far_in[j].astype(jnp.float32)).astype(kind)

    def send_back(j):
        @pl.when(j == s)
        def _():
            ret[s] = whole(j)

        @pl.when(j != s)
        def _():
            total[j] = whole(j)
            back(j).start()

    def forward(j):
        def run():
            for a in both:
                far_copy(a, j).wait_recv()
                fwd_copy(a, j).start()

        unless_own(j, run)

    def flat(value):
        return value.reshape(-1, value.shape[-1])

    def row_grads(k):
        cols = pl.ds(pl.multiple_of(k * 256, 256), 256)
        left = flat(held[1, :, :, cols])
        gate_grad[cols, :] = contract_rows(left, flat(gate_pg[...])).astype(kind)
        up_grad[cols, :] = contract_rows(left, flat(up_pg[...])).astype(kind)

    def act_grads(k):
        cols = pl.ds(pl.multiple_of(k * 512, 512), 512)
        down_grad[:, cols] = contract_rows(flat(act[...]), flat(held[0, :, :, cols])).astype(kind)

    for move in moves:
        move.start()
    meet(steps, True, near, far)
    moves[0].wait()

    def start_own(a):
        src = sources[a]
        for up in both:

            @pl.when(next_is_inner(up))
            def _():
                line_copy(a, z, src.at[:, lanes(t)], up).start()

    def end_own(a):
        for up in both:

            @pl.when(next_is_end(up))
            def _():
                to_end(a, z, sources[a][:, lanes(t)], up)

    start_own(0)
    moves[1].wait()
    moves[2].wait()
    info[pl.ds(0, 2), :] = routes[...].astype(jnp.float32)
    info[pl.ds(2, 2), :] = route_weights[...]
    infos[z] = info[...]
    looped(1, line, lambda dz: info_copy(dz).start())
    row_ids = lax.broadcasted_iota(jnp.int32, (tok_rows, tok_rows), 0)
    col_ids = lax.broadcasted_iota(jnp.int32, (tok_rows, tok_rows), 1)
    before[...] = jnp.where(row_ids < col_ids, 1.0, 0.0).astype(kind)
    table(z)
    end_own(0)
    for move in moves[3:5]:
        move.wait()
    gain = norm_gain[...]

    def normalise(k):
        here = pl.ds(pl.multiple_of(k * 32, 32), 32)
        x = resid[here, :].astype(jnp.float32)
        scale = lax.rsqrt(jnp.mean(x * x, axis=-1, keepdims=True) + 1e-06)
        normed[here, :] = (x * scale * gain).astype(kind)

    looped(0, tok_rows // 32, normalise)
    start_own(1)
    end_own(1)
    for a in both:
        cross[a, z] = selected(a, z, across, sources[a][:, lanes(t)])
        across_copy(a, z).start()
        cross_far[a] = selected(a, z, across, sources[a][:, lanes(far)])
        across_far(a).start()

    def own_chunk(q):
        for a in both:
            held[a, s, :, lanes(q)] = selected(a, z, s, sources[a][:, lanes(q)])

    looped(0, model_width // width, own_chunk)
    for move in moves[5:7]:
        move.wait()
    summed = conv_sum[...].astype(jnp.float32)
    centre = summed - jnp.mean(summed, axis=-1, keepdims=True)
    inv_std = lax.rsqrt(jnp.mean(centre * centre, axis=-1, keepdims=True) + 1e-05)
    pre_act = centre * inv_std * conv_gain[...]
    conv_out = (pre_act * jax.nn.sigmoid(pre_act)).astype(kind)
    side[...] = conv_out
    side_out[0] = conv_out

    def own_picks(e):
        picks[e] = jnp.where(pick(z, e), 1.0, 0.0).astype(kind)

    looped(0, steps, own_picks)
    for move in moves[7:]:
        move.wait()

    codes = line_schedule(line)
    middle = steps // 2

    def slot_code(n):
        code = 0
        for zz in range(line):
            for nn in range(steps):
                code = code + jnp.where((z == zz) & (n == nn), codes[zz][nn], 0)
        return code

    def chunk_at(n):
        code = slot_code(n)
        other = (code // 16) % 2
        return 2 * (code % 16) + y + other * (1 - 2 * y)

    def slot(n):
        code = slot_code(n)
        zb, other = code % 16, (code // 16) % 2
        first, second = (code // 32) % 16, (code // 512) % 16
        meeting = code // 8192
        j = 2 * zb + y + other * (1 - 2 * y)

        @pl.when(meeting > 0)
        def _():
            met = 2 * (meeting - 1) + 1 - y
            for a in both:
                arrival(a, met).wait_recv()
                share(a, met)

        @pl.when(first > 0)
        def _():
            for up in both:
                read_info(first, up)
            for up in both:
                handle(0, first, up)

        @pl.when(second > 0)
        def _():
            for up in both:
                handle(1, second, up)

        @pl.when(n == 1)
        def _():
            for a in both:
                arrival(a, j).wait_recv()
                near_copy(a, j).start()

        @pl.when(n == steps - 2)
        def _():
            looped(1, steps, lambda d: side_copy(d).start())

        forward(j)

        @pl.when(n >= 1)
        def _():
            experts(chunk_at(n - 1))

        @pl.when(n == 1)
        def _():
            add_pair(chunk_at(0))

        @pl.when(n > middle + 1)
        def _():
            add_pair(chunk_at(n - 2))

    def pair_at(n):
        add_pair(chunk_at(n))

    def back_at(n):
        send_back(chunk_at(n))

    looped(0, steps, slot)
    half = model_width // 512
    experts(chunk_at(steps - 1))
    add_pair(chunk_at(steps - 2))
    pair_at(steps - 1)
    looped(1, middle, pair_at)
    looped(middle, steps - 2, back_at)
    looped(0, half // 2, row_grads)
    back_at(steps - 2)
    looped(half // 2, half, row_grads)
    back_at(steps - 1)
    looped(half, half + half // 2, row_grads)
    looped(1, middle, back_at)
    looped(half + half // 2, 2 * half, row_grads)
    looped(0, half, act_grads)
    back_at(0)

    def gather_back(d):
        back_from((s + d) % steps).wait_recv()

    looped(1, steps, gather_back)
    part_grad[...] = contract_rows(flat(picks[...]), flat(ret[...])).astype(kind)

    def finish(j):
        for_near(j).wait_send()
        for_diag(j).wait_send()
        pair_copy(j).wait_send()

        @pl.when(j != s)
        def _():
            back(j).wait_send()
            for a in both:
                near_copy(a, j).wait_send()
                fwd_copy(a, j).wait_send()

        @pl.when(j // 2 != z)
        def _():
            for a in both:
                far_copy(a, j).wait_send()

    def finish_side(d):
        side_copy(d).wait_send()

    def finish_line(m):
        for up in both:
            zb = block_at(m, up)

            @pl.when(valid(m, up) & next_is_inner(up))
            def _():
                for a in both:
                    line_copy(a, zb, tok.at[a, zb], up).wait_send()

            @pl.when(valid(m, up) & next_is_end(up))
            def _():
                for a in both:
                    for col in both:
                        end_copy(a, zb, col, up).wait_send()

    def finish_across(zb):
        for a in both:
            across_copy(a, zb).wait_send()

    def meanwhile():
        looped(1, steps, lambda d: side_copy(d).wait_recv())
        looped(0, steps, finish)
        looped(1, steps, finish_side)
        looped(1, line, lambda dz: info_copy(dz).wait_send())
        looped(0, line, finish_line)
        looped(0, line, finish_across)
        for a in both:
            across_far(a).wait_send()

    settle_body(
        steps, meanwhile, part_grad, grad_out, resid, norm_gain, proj_weight,
        conv_sum, conv_gain, conv_taps, conv_value, conv_gate,
        side_out, feature_cols, proj, value_grad, gate_input_grad,
        full, grads, extended, *settle_sems,
    )


def relay_experts(operands, collective_id):
    routes, resid, w_gate, conv_sum = operands[0], operands[3], operands[5], operands[8]
    steps, tp_count = lax.axis_size("sp"), lax.axis_size("tp")
    line = steps // 2
    tok_rows, model_width = resid.shape
    count = 3 * tok_rows // steps
    width = model_width // tp_count
    hidden = w_gate.shape[1]
    kind = resid.dtype
    block = (steps, count, width)
    channels = conv_sum.shape[1]
    tail_rows = conv_sum.shape[0] + operands[11].shape[0] + 1
    outs = [
        jax.ShapeDtypeStruct((model_width, hidden), kind),
        jax.ShapeDtypeStruct((model_width, hidden), kind),
        jax.ShapeDtypeStruct((hidden, model_width), kind),
        jax.ShapeDtypeStruct((model_width // steps, channels), jnp.float32),
        jax.ShapeDtypeStruct((tok_rows, channels), kind),
        jax.ShapeDtypeStruct((tok_rows, channels), kind),
    ]
    held = pl.BlockSpec(memory_space=pltpu.VMEM)
    outside = pl.BlockSpec(memory_space=pltpu.HBM)

    def sems(*shape):
        return pltpu.SemaphoreType.DMA(shape)

    return pl.pallas_call(
        functools.partial(relay_kernel, steps),
        out_shape=tuple(outs),
        in_specs=[outside] * len(operands),
        out_specs=tuple(held for _ in outs),
        scratch_shapes=[pltpu.VMEM(x.shape, x.dtype) for x in operands]
        + [
            pltpu.VMEM((tok_rows, width), kind),
            pltpu.VMEM((steps,) + conv_sum.shape, kind),
            pltpu.VMEM((steps, tp_count, tok_rows // tp_count, model_width // steps), kind),
            pltpu.VMEM((tok_rows, model_width), kind),
            pltpu.VMEM((tok_rows, model_width), kind),
            pltpu.VMEM((tail_rows, channels), jnp.float32),
            pltpu.VMEM((tok_rows, model_width), kind),
            pltpu.VMEM((2 * routes.shape[0], tok_rows), jnp.float32),
            pltpu.VMEM((line, 2 * routes.shape[0], tok_rows), jnp.float32),
            pltpu.VMEM((line, steps, tok_rows), jnp.float32),
            pltpu.VMEM((line, steps, tok_rows), jnp.float32),
            pltpu.VMEM((tok_rows, tok_rows), kind),
            pltpu.VMEM((steps, count, tok_rows), kind),
            pltpu.VMEM((2, line, tok_rows, width), kind),
            pltpu.VMEM((2, line, 2, count, width), kind),
            pltpu.VMEM((2, line, count, width), kind),
            pltpu.VMEM((2, count, width), kind),
            pltpu.VMEM((2, steps, count, model_width), kind),
        ]
        + [pltpu.VMEM((steps, count, hidden), kind)] * 3
        + [pltpu.VMEM((steps, count, model_width), kind), pltpu.VMEM((2,) + block, kind)]
        + [pltpu.VMEM(block, kind)] * 4
        + [pltpu.VMEM(conv_sum.shape, kind)]
        + [sems(len(operands)), sems(line), sems(line), sems(2, 2, line), sems(2, line), sems(2, 2, line)]
        + [sems(2, line), sems(2, line), sems(2), sems(2, steps)]
        + [sems(2, steps)] * 6
        + [sems(steps)] * 10
        + [sems(tp_count)] * 6
        + [sems(1)]
        + [sems(steps)] * 8
        + [sems(1)] * 2,
        compiler_params=pltpu.CompilerParams(
            collective_id=collective_id, has_side_effects=True, vmem_limit_bytes=42 << 20
        ),
    )(*(pltpu.with_memory_space_constraint(x, pltpu.HBM) for x in operands))


def last_kernel(count, *refs):
    ins, outs, sem = refs[:count], refs[count:-1], refs[-1]
    moves = [pltpu.make_async_copy(a, b, sem.at[i]) for i, (a, b) in enumerate(zip(ins, outs))]
    for move in moves:
        move.start()
    for move in moves:
        move.wait()


def last_stage(results):
    return pl.pallas_call(
        functools.partial(last_kernel, len(results)),
        out_shape=tuple(jax.ShapeDtypeStruct(x.shape, x.dtype) for x in results),
        in_specs=[pl.BlockSpec(memory_space=pltpu.VMEM)] * len(results),
        out_specs=tuple(pl.BlockSpec(memory_space=pl.ANY) for _ in results),
        scratch_shapes=[pltpu.SemaphoreType.DMA((len(results),))],
        compiler_params=pltpu.CompilerParams(vmem_limit_bytes=16 << 20),
    )(*results)


def local(
    grad_out,
    resid,
    norm_gain,
    routes,
    route_weights,
    gate_weight,
    up_weight,
    down_weight,
    proj_weight,
    conv_sum,
    conv_gain,
    conv_taps,
    conv_value,
    conv_gate,
):
    tok_rows, model_width = resid.shape
    sp_count = lax.axis_size("sp")
    tp_count = lax.axis_size("tp")
    capacity = 3 * tok_rows // sp_count
    col_count = model_width // tp_count
    channels = conv_sum.shape[1]
    aligned = capacity % 16 == 0 and model_width % (128 * sp_count) == 0 and channels == GROUP
    if aligned and sp_count % 4 == 0:
        operands = (
            routes.T,
            route_weights.T,
            grad_out,
            resid,
            norm_gain[None],
            gate_weight[0],
            up_weight[0],
            down_weight[0],
            conv_sum,
            conv_gain[None],
            proj_weight,
            conv_taps,
            conv_value,
            conv_gate,
        )
        gate_grad, up_grad, down_grad, *rest = last_stage(relay_experts(operands, 4))
        return (gate_grad[None], up_grad[None], down_grad[None], *rest)
    resid_f = resid.astype(jnp.float32)
    inv_rms = lax.rsqrt(jnp.mean(resid_f * resid_f, axis=-1, keepdims=True) + 1e-06)
    normed = (resid_f * inv_rms * norm_gain).astype(jnp.bfloat16)
    my_sp = lax.axis_index("sp")
    away = (routes - my_sp) % sp_count
    steps_away = jnp.arange(sp_count, dtype=jnp.int32)
    named = away[:, :, None] == steps_away[None, None, :]
    chosen = jnp.any(named, axis=1)
    weight_of = jnp.sum(jnp.where(named, route_weights[:, :, None], 0.0), axis=1)
    token_ids = jnp.arange(tok_rows, dtype=jnp.int32)
    earlier = (token_ids[None, :] < token_ids[:, None]).astype(jnp.bfloat16)
    rank = jnp.dot(earlier, chosen.astype(jnp.bfloat16), preferred_element_type=jnp.float32)
    rank = jnp.where(chosen, rank, -1.0).astype(jnp.int32)
    slots = jnp.arange(capacity, dtype=jnp.int32)
    held = rank.T[:, None, :] == slots[None, :, None]
    slot_weight = jnp.sum(jnp.where(held, weight_of.T[:, None, :], 0.0), axis=2)
    pick = held.astype(jnp.bfloat16).reshape(sp_count * capacity, tok_rows)
    first_col = lax.axis_index("tp") * col_count
    normed_part = lax.dynamic_slice_in_dim(normed, first_col, col_count, 1)
    cots_part = lax.dynamic_slice_in_dim(grad_out, first_col, col_count, 1)
    slot_weight = slot_weight.reshape(-1, 1)
    send_rows = jnp.dot(pick, normed_part, preferred_element_type=jnp.float32).astype(jnp.bfloat16)
    send_cots = jnp.dot(pick, cots_part, preferred_element_type=jnp.float32)
    send_cots = (send_cots * slot_weight).astype(jnp.bfloat16)
    own_pick = pick[:capacity]
    own_rows = jnp.dot(own_pick, normed, preferred_element_type=jnp.float32).astype(jnp.bfloat16)
    own_cots = jnp.dot(own_pick, grad_out, preferred_element_type=jnp.float32)
    own_cots = (own_cots * slot_weight[:capacity]).astype(jnp.bfloat16)
    summed = conv_sum.astype(jnp.float32).reshape(tok_rows, channels // GROUP, GROUP)
    centre = summed - jnp.mean(summed, axis=-1, keepdims=True)
    inv_std = lax.rsqrt(jnp.mean(centre * centre, axis=-1, keepdims=True) + 1e-05)
    grouped = centre * inv_std
    chan_normed = grouped.reshape(tok_rows, channels)
    pre_act = chan_normed * conv_gain
    sigma_conv = jax.nn.sigmoid(pre_act)
    conv_out = (pre_act * sigma_conv).astype(jnp.bfloat16)
    routed_rows, routed_cots = spread(
        (
            send_rows.reshape(sp_count, capacity, col_count),
            send_cots.reshape(sp_count, capacity, col_count),
        ),
        (own_rows, own_cots),
        None,
        True,
        False,
        0,
    )
    routed_rows = routed_rows.reshape(sp_count * capacity, model_width)
    routed_cots = routed_cots.reshape(sp_count * capacity, model_width)
    gate_grad, up_grad, down_grad, partial_value = expert_backward(
        routed_rows, routed_cots, gate_weight[0], up_weight[0], down_weight[0]
    )
    returned = combine(
        partial_value.reshape(sp_count, capacity, model_width).astype(jnp.bfloat16), 1
    ).reshape(sp_count * capacity, col_count)
    normed_part_grad = contract_rows(pick, returned).astype(jnp.bfloat16)
    chunks = 4
    normed_grad, all_out = spread(
        (normed_part_grad.reshape(chunks, tok_rows // chunks, col_count),),
        None,
        conv_out,
        True,
        False,
        2,
    )
    normed_grad = normed_grad.reshape(tok_rows, model_width)
    feature_grad = normed_grad.astype(jnp.float32) * norm_gain
    cubed = inv_rms * inv_rms * inv_rms
    resid_grad = (
        grad_out.astype(jnp.float32)
        + inv_rms * feature_grad
        - resid_f * cubed * jnp.mean(resid_f * feature_grad, axis=-1, keepdims=True)
    ).astype(jnp.bfloat16)
    share = tok_rows // tp_count
    feat_rows = model_width // sp_count
    tokens_part = lax.dynamic_slice_in_dim(resid_grad, lax.axis_index("tp") * share, share, 0)
    by_feature = tokens_part.reshape(share, sp_count, feat_rows).transpose(1, 0, 2)
    own_features = lax.dynamic_slice_in_dim(resid_grad, my_sp * feat_rows, feat_rows, 1)
    (feature_cols,) = spread(
        (by_feature,), (own_features.reshape(tp_count, share, feat_rows),), None, False, True, 3
    )
    proj_grad = contract_rows(
        feature_cols.reshape(sp_count * tok_rows, feat_rows),
        all_out.reshape(sp_count * tok_rows, channels),
    )
    out_grad = jnp.dot(resid_grad, proj_weight, preferred_element_type=jnp.float32)
    normal_grad = (
        out_grad * sigma_conv * (1.0 + pre_act * (1.0 - sigma_conv)) * conv_gain
    ).reshape(tok_rows, channels // GROUP, GROUP)
    sum_grad = inv_std * (
        normal_grad
        - jnp.mean(normal_grad, axis=-1, keepdims=True)
        - grouped * jnp.mean(normal_grad * grouped, axis=-1, keepdims=True)
    )
    sum_grad = sum_grad.reshape(tok_rows, channels)
    following = passed_along(sum_grad[: CONV_K - 1], "sp", -1)
    extended = jnp.concatenate([sum_grad, following], axis=0)
    gated_grad = lax.conv_general_dilated(
        extended[None],
        conv_taps[::-1][:, None, :],
        (1,),
        ((0, 0),),
        dimension_numbers=("NWC", "WIO", "NWC"),
        feature_group_count=channels,
        precision=lax.Precision.HIGHEST,
    )[0]
    sigma_gate = jax.nn.sigmoid(conv_gate.astype(jnp.float32))
    value_grad = (gated_grad * sigma_gate).astype(jnp.bfloat16)
    gate_input_grad = (
        gated_grad * conv_value.astype(jnp.float32) * sigma_gate * (1.0 - sigma_gate)
    ).astype(jnp.bfloat16)
    return (gate_grad[None], up_grad[None], down_grad[None], proj_grad, value_grad, gate_input_grad)


def solution(mesh):
    in_specs = (
        P("sp", None),
        P("sp", None),
        P(),
        P("sp", None),
        P("sp", None),
        P("sp", None, "tp"),
        P("sp", None, "tp"),
        P("sp", "tp", None),
        P(None, "tp"),
        P("sp", "tp"),
        P("tp"),
        P(None, "tp"),
        P("sp", "tp"),
        P("sp", "tp"),
    )
    out_specs = (
        P("sp", None, "tp"),
        P("sp", None, "tp"),
        P("sp", "tp", None),
        P("sp", "tp"),
        P("sp", "tp"),
        P("sp", "tp"),
    )
    return jax.shard_map(local, mesh=mesh, in_specs=in_specs, out_specs=out_specs, check_vma=False)
```

```python
import functools

import jax
import jax.numpy as jnp
from jax import lax
from jax.experimental import pallas as pl
from jax.experimental.pallas import tpu as pltpu
from jax.sharding import PartitionSpec as P

CONV_K = 31
GROUP = 128
MESH = pl.DeviceIdType.MESH


CLAMP_LIMIT = 7.0
SLOPE_ALPHA = 1.702


def passed_along(block, axis, distance):
    devices = range(lax.axis_size(axis))
    route = [(i - distance, i) for i in devices if i - distance in devices]
    return lax.ppermute(block, axis, route)


def tp_places():
    mine = lax.axis_index("tp")
    near = mine + 1 - 2 * (mine % 2)
    far = (mine + 2) % 4
    diag = (near + 2) % 4
    return mine, near, far, diag


def meet(steps, over_sp, near, far):
    s, t = lax.axis_index("sp"), lax.axis_index("tp")
    barrier = pltpu.get_barrier_semaphore()
    pl.semaphore_signal(barrier, inc=1, device_id=(s, near), device_id_type=MESH)
    pl.semaphore_signal(barrier, inc=1, device_id=(s, far), device_id_type=MESH)
    total = 2
    if over_sp:

        def greet(d, carry):
            pl.semaphore_signal(
                barrier, inc=1, device_id=((s + d) % steps, t), device_id_type=MESH
            )
            return carry

        lax.fori_loop(1, steps, greet, 0)
        total += steps - 1
    pl.semaphore_wait(barrier, total)


def crossing_first(steps, k):
    return steps // 2 + ((k + 1) // 2) * (2 * (k % 2) - 1)


def looped(first, last, body):
    def step(k, carry):
        body(k)
        return carry

    lax.fori_loop(first, last, step, 0)


def spread_kernel(count, steps, over_sp, in_lanes, absolute, beside, sp_count, *refs):
    refs = list(refs)
    sends, refs = refs[:count], refs[count:]
    fulls, refs = (refs[:count], refs[count:]) if over_sp else (None, refs)
    side, refs = (refs[0], refs[1:]) if beside else (None, refs)
    outs, refs = refs[:count], refs[count:]
    side_out, refs = (refs[0], refs[1:]) if beside else (None, refs)
    own_sem, a_send, a_recv, b_send, f_send, c_send, near_recv, fwd_recv, far_recv = refs[:9]
    s = lax.axis_index("sp")
    t, near, far, _ = tp_places()
    width = sends[0].shape[-1]

    def place(c, d, q):
        if in_lanes:
            return outs[c].at[d, :, pl.ds(pl.multiple_of(q * width, width), width)]
        return outs[c].at[d, q]

    def source(c, d):
        return sends[c].at[(s + d) % steps if absolute else d]

    def own(c, d):
        if over_sp:
            return pltpu.make_async_copy(fulls[c], outs[c].at[0], own_sem.at[c, 0])
        return pltpu.make_async_copy(source(c, d), place(c, d, t), own_sem.at[c, d])

    def to_sp(c, d):
        return pltpu.make_async_remote_copy(
            src_ref=source(c, d),
            dst_ref=place(c, d, t),
            send_sem=a_send.at[c, d],
            recv_sem=a_recv.at[c, d],
            device_id=((s + d) % steps, t),
            device_id_type=MESH,
        )

    def to_tp(c, d, q, target, send_sem, recv_sem):
        return pltpu.make_async_remote_copy(
            src_ref=place(c, d, q),
            dst_ref=place(c, d, q),
            send_sem=send_sem.at[c, d],
            recv_sem=recv_sem.at[c, d],
            device_id=(s, target),
            device_id_type=MESH,
        )

    def near_copy(c, d):
        return to_tp(c, d, t, near, b_send, near_recv)

    def far_copy(c, d):
        return to_tp(c, d, t, far, f_send, far_recv)

    def fwd_copy(c, d):
        return to_tp(c, d, far, near, c_send, fwd_recv)

    def side_copy(d):
        side_send, side_recv = refs[10:12]
        return pltpu.make_async_remote_copy(
            src_ref=side,
            dst_ref=side_out.at[d],
            send_sem=side_send.at[d],
            recv_sem=side_recv.at[d],
            device_id=((s + d) % sp_count, t),
            device_id_type=MESH,
        )

    def own_side():
        return pltpu.make_async_copy(side, side_out.at[0], refs[9].at[0])

    def share(c, d):
        far_copy(c, d).start()
        near_copy(c, d).start()

    def forward(c, d):
        far_copy(c, d).wait_recv()
        fwd_copy(c, d).start()

    def finish(c, d):
        near_copy(c, d).wait()
        far_copy(c, d).wait_send()
        fwd_copy(c, d).wait()

    def loop(first, last, body):
        def each(k):
            d = k + 1 if over_sp else k
            for c in range(count):
                body(c, d)

        looped(first, last, each)

    meet(sp_count, over_sp or beside, near, far)
    if over_sp:
        loop(0, steps - 1, lambda c, d: to_sp(c, d).start())
        for c in range(count):
            own(c, 0).start()

        def pass_on(k):
            for c in range(count):
                d = k + 1
                to_sp(c, d).wait_recv()
                share(c, d)

        def pass_on_twice(k):
            pass_on(k)
            for c in range(count):
                forward(c, k)

        pass_on(0)
        looped(1, steps - 1, pass_on_twice)
        loop(steps - 2, steps - 1, forward)
        loop(0, steps - 1, finish)
        loop(0, steps - 1, lambda c, d: to_sp(c, d).wait_send())
        for c in range(count):
            own(c, 0).wait()
    else:
        loop(0, steps, lambda c, d: own(c, d).start())
        if beside:
            looped(0, sp_count - 1, lambda k: side_copy(crossing_first(sp_count, k)).start())
            own_side().start()

        def share_own(c, d):
            own(c, d).wait()
            share(c, d)

        loop(0, steps, share_own)
        loop(0, steps, forward)
        loop(0, steps, finish)
        if beside:
            looped(0, sp_count - 1, lambda k: side_copy(crossing_first(sp_count, k)).wait())
            own_side().wait()


def spread(sends, fulls, side, in_lanes, absolute, collective_id):
    count = len(sends)
    steps, rows, width = sends[0].shape
    tp_count, sp_count = lax.axis_size("tp"), lax.axis_size("sp")
    over_sp, beside = fulls is not None, side is not None
    shape = (steps, rows, tp_count * width) if in_lanes else (steps, tp_count, rows, width)
    out_shape = [jax.ShapeDtypeStruct(shape, x.dtype) for x in sends]
    operands = list(sends) + (list(fulls) if over_sp else []) + ([side] if beside else [])
    scratch = [pltpu.SemaphoreType.DMA((count, steps))] * 9
    if beside:
        out_shape.append(jax.ShapeDtypeStruct((sp_count,) + side.shape, side.dtype))
        scratch += [pltpu.SemaphoreType.DMA((1,))] + [pltpu.SemaphoreType.DMA((sp_count,))] * 2
    return pl.pallas_call(
        functools.partial(
            spread_kernel, count, steps, over_sp, in_lanes, absolute, beside, sp_count
        ),
        out_shape=tuple(out_shape),
        in_specs=[pl.BlockSpec(memory_space=pltpu.VMEM)] * len(operands),
        out_specs=tuple(pl.BlockSpec(memory_space=pltpu.VMEM) for _ in out_shape),
        scratch_shapes=scratch,
        compiler_params=pltpu.CompilerParams(
            collective_id=collective_id, has_side_effects=True, vmem_limit_bytes=40 << 20
        ),
    )(*operands)


def combine_kernel(
    steps, part, out, near_in, pair, far_in, total,
    n0_send, n0_recv, n1_send, n1_recv, f_send, f_recv, a_send, a_recv,
):
    s = lax.axis_index("sp")
    t, near, far, diag = tp_places()
    width = out.shape[-1]

    def lanes(q):
        return pl.ds(pl.multiple_of(q * width, width), width)

    def near_copy(d, which, q, send_sem, recv_sem):
        return pltpu.make_async_remote_copy(
            src_ref=part.at[d, :, lanes(q)],
            dst_ref=near_in.at[which, d],
            send_sem=send_sem.at[d],
            recv_sem=recv_sem.at[d],
            device_id=(s, near),
            device_id_type=MESH,
        )

    def for_near(d):
        return near_copy(d, 0, near, n0_send, n0_recv)

    def for_diag(d):
        return near_copy(d, 1, diag, n1_send, n1_recv)

    def far_copy(d):
        return pltpu.make_async_remote_copy(
            src_ref=pair.at[d],
            dst_ref=far_in.at[d],
            send_sem=f_send.at[d],
            recv_sem=f_recv.at[d],
            device_id=(s, far),
            device_id_type=MESH,
        )

    def back(d):
        return pltpu.make_async_remote_copy(
            src_ref=total.at[d],
            dst_ref=out.at[d],
            send_sem=a_send.at[d],
            recv_sem=a_recv.at[d],
            device_id=((s + steps - d) % steps, t),
            device_id_type=MESH,
        )

    meet(steps, True, near, far)

    def open_up(d):
        for_diag(d).start()
        for_near(d).start()

    def add_pair(d):
        for_diag(d).wait_recv()
        mine = part[d, :, lanes(far)].astype(jnp.float32)
        pair[d] = (mine + near_in[1, d].astype(jnp.float32)).astype(pair.dtype)
        far_copy(d).start()

    def whole(d):
        for_near(d).wait_recv()
        far_copy(d).wait_recv()
        mine = part[d, :, lanes(t)].astype(jnp.float32)
        both = mine + near_in[0, d].astype(jnp.float32)
        return (both + far_in[d].astype(jnp.float32)).astype(out.dtype)

    def send_back(d):
        total[d] = whole(d)
        back(d).start()

    def at(k):
        return crossing_first(steps, k)

    lag = min(3, steps - 1)
    looped(0, steps - 1, lambda k: open_up(at(k)))
    open_up(0)
    looped(0, lag, lambda k: add_pair(at(k)))

    def middle(k):
        add_pair(at(k))
        send_back(at(k - lag))

    looped(lag, steps - 1, middle)
    add_pair(0)
    looped(steps - 1 - lag, steps - 1, lambda k: send_back(at(k)))
    out[0] = whole(0)

    def finish(d):
        for_near(d).wait_send()
        for_diag(d).wait_send()
        far_copy(d).wait_send()

    looped(0, steps, finish)
    looped(1, steps, lambda d: back(d).wait())


def combine(part, collective_id):
    steps, rows, all_width = part.shape
    width = all_width // lax.axis_size("tp")
    block = (steps, rows, width)
    return pl.pallas_call(
        functools.partial(combine_kernel, steps),
        out_shape=jax.ShapeDtypeStruct(block, part.dtype),
        in_specs=[pl.BlockSpec(memory_space=pltpu.VMEM)],
        out_specs=pl.BlockSpec(memory_space=pltpu.VMEM),
        scratch_shapes=[
            pltpu.VMEM((2,) + block, part.dtype),
            pltpu.VMEM(block, part.dtype),
            pltpu.VMEM(block, part.dtype),
            pltpu.VMEM(block, part.dtype),
        ]
        + [pltpu.SemaphoreType.DMA((steps,))] * 8,
        compiler_params=pltpu.CompilerParams(
            collective_id=collective_id, has_side_effects=True, vmem_limit_bytes=40 << 20
        ),
    )(part)


def contract_rows(left_side, right_side):
    return lax.dot_general(
        left_side, right_side, (((0,), (0,)), ((), ())), preferred_element_type=jnp.float32
    )


def contract_cols(left_side, right_side):
    return lax.dot_general(
        left_side, right_side, (((1,), (1,)), ((), ())), preferred_element_type=jnp.float32
    )


def expert_backward(routed_rows, routed_cots, w_gate, w_up, w_down):
    gate_pre = jnp.dot(routed_rows, w_gate, preferred_element_type=jnp.float32)
    up_pre = jnp.dot(routed_rows, w_up, preferred_element_type=jnp.float32)
    gate_clamped = jnp.minimum(gate_pre, CLAMP_LIMIT)
    up_clamped = jnp.clip(up_pre, -CLAMP_LIMIT, CLAMP_LIMIT)
    sigma = jax.nn.sigmoid(SLOPE_ALPHA * gate_clamped)
    gated = gate_clamped * sigma
    act = ((up_clamped + 1.0) * gated).astype(jnp.bfloat16)
    down_grad = contract_rows(act, routed_cots).astype(jnp.bfloat16)
    act_grad = contract_cols(routed_cots, w_down)
    inside = (up_pre > -CLAMP_LIMIT) & (up_pre < CLAMP_LIMIT)
    up_pre_grad = jnp.where(inside, act_grad * gated, 0.0).astype(jnp.bfloat16)
    slope = sigma + SLOPE_ALPHA * gate_clamped * sigma * (1.0 - sigma)
    gate_pre_grad = jnp.where(
        gate_pre < CLAMP_LIMIT, act_grad * (up_clamped + 1.0) * slope, 0.0
    ).astype(jnp.bfloat16)
    gate_grad = contract_rows(routed_rows, gate_pre_grad).astype(jnp.bfloat16)
    up_grad = contract_rows(routed_rows, up_pre_grad).astype(jnp.bfloat16)
    partial_value = contract_cols(gate_pre_grad, w_gate) + contract_cols(up_pre_grad, w_up)
    return (gate_grad, up_grad, down_grad, partial_value)


def line_schedule(line):
    codes = []
    for z in range(line):
        slots = [[(z, 0), 0, 0, 0], [(z, 1), 1, 1, 0]]
        groups = [[b for b in (z - k, z + k) if 0 <= b < line] for k in range(1, line)]
        groups = [g for g in groups if g]
        for k, group in enumerate(groups, 1):
            following = k + 1 if k < len(groups) else 0
            added = [[(b, 0), 0, 0, 0] for b in group] + [[(b, 1), 0, 0, 0] for b in group]
            many = len(group)
            added[0][3] = group[0] + 1
            if many > 1:
                added[many][3] = group[1] + 1
            added[1][1] = following
            added[many][2] = following
            slots += added
        row = []
        for (zb, col), first, second, meeting in slots:
            row.append((((meeting * 16 + second) * 16 + first) * 2 + col) * 16 + zb)
        codes.append(row)
    return codes


def settle_body(
    steps, meanwhile, part_grad, grad_out, resid, norm_gain, proj_weight,
    conv_sum, conv_gain, conv_taps, conv_value, conv_gate,
    side_out, feature_cols, proj, value_grad, gate_input_grad,
    full, grads, extended, far_send, far_recv, near_send, near_recv, fwd_send, fwd_recv,
    own_sem, x_send, x_recv, xf_send, xf_recv, xn_send, xn_recv, xw_send, xw_recv,
    h_send, h_recv,
):
    s = lax.axis_index("sp")
    t, near, far, diag = tp_places()
    tok_rows, width = part_grad.shape
    chunks, share = feature_cols.shape[1], feature_cols.shape[2]
    feat_rows = feature_cols.shape[3]
    overlap = conv_taps.shape[0] - 1

    def rows_of(j):
        return pl.ds(pl.multiple_of(j * share, share), share)

    def lanes(q):
        return pl.ds(pl.multiple_of(q * width, width), width)

    def mine_at(j):
        return full.at[rows_of(j), lanes(t)]

    def own_copy():
        return pltpu.make_async_copy(part_grad, full.at[:, lanes(t)], own_sem.at[0])

    def gather(j, q, src, target, send_sem, recv_sem):
        return pltpu.make_async_remote_copy(
            src_ref=src,
            dst_ref=full.at[rows_of(j), lanes(q)],
            send_sem=send_sem.at[j],
            recv_sem=recv_sem.at[j],
            device_id=(s, target),
            device_id_type=MESH,
        )

    def to_far(j):
        return gather(j, t, part_grad.at[rows_of(j), :], far, far_send, far_recv)

    def to_near(j):
        return gather(j, t, part_grad.at[rows_of(j), :], near, near_send, near_recv)

    def pass_near(j):
        return gather(j, far, full.at[rows_of(j), lanes(far)], near, fwd_send, fwd_recv)

    def spread_out(d):
        feats = pl.ds(pl.multiple_of(((s + d) % steps) * feat_rows, feat_rows), feat_rows)
        return pltpu.make_async_remote_copy(
            src_ref=grads.at[rows_of(t), feats],
            dst_ref=feature_cols.at[d, t],
            send_sem=x_send.at[d],
            recv_sem=x_recv.at[d],
            device_id=((s + d) % steps, t),
            device_id_type=MESH,
        )

    def beside(d, q, target, send_sem, recv_sem):
        return pltpu.make_async_remote_copy(
            src_ref=feature_cols.at[d, q],
            dst_ref=feature_cols.at[d, q],
            send_sem=send_sem.at[d],
            recv_sem=recv_sem.at[d],
            device_id=(s, target),
            device_id_type=MESH,
        )

    def x_far(d):
        return beside(d, t, far, xf_send, xf_recv)

    def x_near(d):
        return beside(d, t, near, xn_send, xn_recv)

    def x_pass(d):
        return beside(d, far, near, xw_send, xw_recv)

    def halo():
        return pltpu.make_async_remote_copy(
            src_ref=extended.at[pl.ds(0, overlap + 2)],
            dst_ref=extended.at[pl.ds(tok_rows, overlap + 2)],
            send_sem=h_send.at[0],
            recv_sem=h_recv.at[0],
            device_id=((s + steps - 1) % steps, t),
            device_id_type=MESH,
        )

    gain = norm_gain[...]

    def settle(j):
        here = rows_of(j)
        feature_grad = full[here, :].astype(jnp.float32) * gain
        x = resid[here, :].astype(jnp.float32)
        scale = lax.rsqrt(jnp.mean(x * x, axis=-1, keepdims=True) + 1e-06)
        cubed = scale * scale * scale
        mean = jnp.mean(x * feature_grad, axis=-1, keepdims=True)
        value = grad_out[here, :].astype(jnp.float32) + scale * feature_grad - x * cubed * mean
        grads[here, :] = value.astype(grads.dtype)

    def crossing(k):
        return crossing_first(steps, k)

    for j in (diag, far, t, near):
        to_far(j).start()
    for j in (near, t, diag, far):
        to_near(j).start()
    own_copy().start()
    summed = conv_sum[...].astype(jnp.float32)
    centre = summed - jnp.mean(summed, axis=-1, keepdims=True)
    inv_std = lax.rsqrt(jnp.mean(centre * centre, axis=-1, keepdims=True) + 1e-05)
    grouped = centre * inv_std
    pre_act = grouped * conv_gain[...]
    sigma = jax.nn.sigmoid(pre_act)
    slope = sigma * (1.0 + pre_act * (1.0 - sigma)) * conv_gain[...]
    own_copy().wait()

    def arrive(j):
        to_far(j).wait_recv()
        pass_near(j).start()

    def whole(j):
        to_near(j).wait_recv()
        pass_near(j).wait_recv()

    arrive(near)
    arrive(t)
    whole(t)
    settle(t)
    looped(0, steps - 1, lambda k: spread_out(crossing(k)).start())
    meanwhile()
    arrive(far)
    arrive(diag)
    for j in (near, far, diag):
        whole(j)
        settle(j)
    feats = pl.ds(pl.multiple_of(s * feat_rows, feat_rows), feat_rows)
    feature_cols[0] = grads[:, feats].reshape(chunks, share, feat_rows)
    out_grad = jnp.dot(grads[...], proj_weight[...], preferred_element_type=jnp.float32)
    normal = out_grad * slope
    sum_grad = inv_std * (
        normal
        - jnp.mean(normal, axis=-1, keepdims=True)
        - grouped * jnp.mean(normal * grouped, axis=-1, keepdims=True)
    )
    extended[pl.ds(0, tok_rows), :] = sum_grad
    halo().start()

    def share_out(d):
        spread_out(d).wait_recv()
        x_far(d).start()
        x_near(d).start()

    def pass_on(d):
        x_far(d).wait_recv()
        x_pass(d).start()

    def term(d):
        left = feature_cols[d].reshape(tok_rows, feat_rows)
        return contract_rows(left, side_out[d])

    def gather_term(d):
        x_near(d).wait_recv()
        x_pass(d).wait_recv()
        proj[...] += term(d)

    proj[...] = term(0)
    looped(0, steps - 1, lambda k: share_out(crossing(k)))
    looped(0, steps - 1, lambda k: pass_on(crossing(k)))
    halo().wait()

    @pl.when(s == steps - 1)
    def _():
        extended[pl.ds(tok_rows, overlap + 2), :] = jnp.zeros(
            (overlap + 2, extended.shape[1]), extended.dtype
        )

    gated_grad = extended[pl.ds(overlap, tok_rows), :] * conv_taps[pl.ds(0, 1), :]
    for j in range(1, overlap + 1):
        gated_grad += extended[pl.ds(overlap - j, tok_rows), :] * conv_taps[pl.ds(j, 1), :]
    sigma_gate = jax.nn.sigmoid(conv_gate[...].astype(jnp.float32))
    value_grad[...] = (gated_grad * sigma_gate).astype(value_grad.dtype)
    gate_input_grad[...] = (
        gated_grad * conv_value[...].astype(jnp.float32) * sigma_gate * (1.0 - sigma_gate)
    ).astype(gate_input_grad.dtype)
    looped(0, steps - 1, lambda k: gather_term(crossing(k)))

    def finish(k):
        d = crossing(k)
        spread_out(d).wait_send()
        x_near(d).wait_send()
        x_far(d).wait_send()
        x_pass(d).wait_send()

    looped(0, steps - 1, finish)

    def finish_gather(j):
        to_far(j).wait_send()
        to_near(j).wait_send()
        pass_near(j).wait_send()

    looped(0, chunks, finish_gather)


def relay_kernel(
    steps, routes_in, weights_in, grad_in, resid_in, gain_in, gate_in, up_in, down_in, sum_in,
    conv_gain_in, proj_in, taps_in, value_in, convgate_in,
    gate_grad, up_grad, down_grad, proj, value_grad, gate_input_grad,
    routes, route_weights, grad_out, resid, norm_gain, w_gate, w_up, w_down, conv_sum, conv_gain,
    proj_weight, conv_taps, conv_value, conv_gate, part_grad, side_out, feature_cols, full, grads,
    extended, normed, info, infos, ranks, weights, before, picks,
    tok, over, cross, cross_far, held, act, gate_pg, up_pg, part,
    near_in, pair, far_in, total, ret, side,
    own_sem, info_send, info_recv, line_send, line_recv, end_send, cross_recv,
    across_send, afar_send, arr_recv, b_send, f_send, c_send, near_recv, fwd_recv, far_recv,
    n0_send, n0_recv, n1_send, n1_recv, g_send, g_recv, r_send, r_recv, s_send, s_recv,
    *settle_sems,
):
    s = lax.axis_index("sp")
    t, near, far, diag = tp_places()
    line = steps // 2
    z, y = s // 2, s % 2
    across = s + 1 - 2 * y
    tok_rows, width = part_grad.shape
    count = cross.shape[2]
    hidden = w_gate.shape[1]
    model_width = resid.shape[1]
    both = (0, 1)
    kind = held.dtype
    sources = (grad_out, normed)

    def lanes(q):
        return pl.ds(pl.multiple_of(q * width, width), width)

    def remote(src, dst, send_sem, recv_sem, sp_to, tp_to):
        return pltpu.make_async_remote_copy(
            src_ref=src,
            dst_ref=dst,
            send_sem=send_sem,
            recv_sem=recv_sem,
            device_id=(sp_to, tp_to),
            device_id_type=MESH,
        )

    moves = [
        pltpu.make_async_copy(a, b, own_sem.at[i])
        for i, (a, b) in enumerate(
            (
                (grad_in, grad_out),
                (routes_in, routes),
                (weights_in, route_weights),
                (resid_in, resid),
                (gain_in, norm_gain),
                (sum_in, conv_sum),
                (conv_gain_in, conv_gain),
                (gate_in, w_gate),
                (up_in, w_up),
                (down_in, w_down),
                (proj_in, proj_weight),
                (taps_in, conv_taps),
                (value_in, conv_value),
                (convgate_in, conv_gate),
            )
        )
    ]

    def info_copy(dz):
        peer = ((z + dz) % line) * 2 + y
        return remote(info, infos.at[z], info_send.at[dz], info_recv.at[z], peer, t)

    def info_from(zb):
        return remote(info, infos.at[zb], info_send.at[0], info_recv.at[zb], across, t)

    def line_copy(a, zb, src, up):
        to = s + 2 if up else s - 2
        return remote(src, tok.at[a, zb], line_send.at[a, up, zb], line_recv.at[a, zb], to, t)

    def end_copy(a, zb, col, up):
        to = s + 2 if up else s - 2
        j = 2 * zb + y
        if col == 0:
            dst, recv = held.at[a, j, :, lanes(t)], arr_recv.at[a, j]
        else:
            dst, recv = cross.at[a, zb], cross_recv.at[a, zb]
        return remote(over.at[a, zb, col], dst, end_send.at[a, col, zb], recv, to, t)

    def across_copy(a, zb):
        j = 2 * zb + y
        dst = held.at[a, j, :, lanes(t)]
        return remote(cross.at[a, zb], dst, across_send.at[a, zb], arr_recv.at[a, j], across, t)

    def across_far(a):
        dst = held.at[a, s, :, lanes(far)]
        return remote(cross_far.at[a], dst, afar_send.at[a], far_recv.at[a, s], across, t)

    def arrival(a, j):
        place = held.at[a, j, :, lanes(t)]
        return remote(place, place, f_send.at[a, j], arr_recv.at[a, j], s, far)

    def to_tp(a, j, q, target, send_sem, recv_sem):
        place = held.at[a, j, :, lanes(q)]
        return remote(place, place, send_sem.at[a, j], recv_sem.at[a, j], s, target)

    def near_copy(a, j):
        return to_tp(a, j, t, near, b_send, near_recv)

    def far_copy(a, j):
        return to_tp(a, j, t, far, f_send, far_recv)

    def fwd_copy(a, j):
        return to_tp(a, j, far, near, c_send, fwd_recv)

    def part_copy(j, which, q, send_sem, recv_sem):
        src, dst = part.at[j, :, lanes(q)], near_in.at[which, j]
        return remote(src, dst, send_sem.at[j], recv_sem.at[j], s, near)

    def for_near(j):
        return part_copy(j, 0, near, n0_send, n0_recv)

    def for_diag(j):
        return part_copy(j, 1, diag, n1_send, n1_recv)

    def pair_copy(j):
        return remote(pair.at[j], far_in.at[j], g_send.at[j], g_recv.at[j], s, far)

    def back(j):
        return remote(total.at[j], ret.at[s], r_send.at[j], r_recv.at[s], j, t)

    def back_from(e):
        return remote(total.at[e], ret.at[e], r_send.at[e], r_recv.at[e], e, t)

    def side_copy(d):
        to = (s + d) % steps
        return remote(side, side_out.at[d], s_send.at[d], s_recv.at[d], to, t)

    def table(zb):
        first, second = infos[zb, pl.ds(0, 1), :], infos[zb, pl.ds(1, 1), :]
        ids = lax.broadcasted_iota(jnp.int32, (steps, tok_rows), 0).astype(jnp.float32)
        chosen = (first == ids) | (second == ids)
        ones = jnp.where(chosen, 1.0, 0.0).astype(kind)
        rank = jnp.dot(ones, before[...], preferred_element_type=jnp.float32)
        ranks[zb] = jnp.where(chosen, rank, -1.0)
        weights[zb] = jnp.where(
            first == ids, infos[zb, pl.ds(2, 1), :], infos[zb, pl.ds(3, 1), :]
        )

    def pick(zb, e):
        slots = lax.broadcasted_iota(jnp.int32, (count, tok_rows), 0).astype(jnp.float32)
        return slots == ranks[zb, pl.ds(e, 1), :]

    def selected(a, zb, e, value):
        mask = pick(zb, e)
        hot = jnp.where(mask, 1.0, 0.0).astype(kind)
        out = jnp.dot(hot, value, preferred_element_type=jnp.float32)
        if a == 0:
            scale = jnp.where(mask, weights[zb, pl.ds(e, 1), :], 0.0)
            out = out * jnp.sum(scale, axis=1, keepdims=True)
        return out.astype(kind)

    def to_end(a, zb, value, up):
        end = z + 1 if up else z - 1
        for col in both:
            e = 2 * end + (y if col == 0 else 1 - y)
            over[a, zb, col] = selected(a, zb, e, value)
            end_copy(a, zb, col, up).start()

    def valid(m, up):
        return (z >= m) if up else (z + m < line)

    def block_at(m, up):
        return z - m if up else z + m

    def next_is_end(up):
        return (z + 1 == line - 1) if up else (z == 1)

    def next_is_inner(up):
        return (z + 1 < line - 1) if up else (z >= 2)

    def at_end(up):
        return (z == line - 1) if up else (z == 0)

    def share(a, j):
        far_copy(a, j).start()
        near_copy(a, j).start()

    def read_info(m, up):
        zb = block_at(m, up)

        @pl.when(valid(m, up))
        def _():
            info_from(zb).wait_recv()

        @pl.when(valid(m, up) & jnp.logical_not(at_end(up)))
        def _():
            table(zb)

    def handle(a, m, up):
        zb = block_at(m, up)
        j = 2 * zb + y

        @pl.when(valid(m, up) & at_end(up))
        def _():
            arrival(a, j).wait_recv()
            end_copy(a, zb, 1, up).wait_recv()
            share(a, j)
            across_copy(a, zb).start()

        @pl.when(valid(m, up) & jnp.logical_not(at_end(up)))
        def _():
            line_copy(a, zb, tok.at[a, zb], up).wait_recv()

            @pl.when(next_is_end(up))
            def _():
                to_end(a, zb, tok[a, zb], up)

            @pl.when(next_is_inner(up))
            def _():
                line_copy(a, zb, tok.at[a, zb], up).start()

            held[a, j, :, lanes(t)] = selected(a, zb, s, tok[a, zb])
            share(a, j)
            cross[a, zb] = selected(a, zb, across, tok[a, zb])
            across_copy(a, zb).start()

    def unless_own(j, body):
        @pl.when(j != s)
        def _():
            body()

    def experts(j):
        def settle():
            for a in both:
                near_copy(a, j).wait_recv()
                fwd_copy(a, j).wait_recv()

        unless_own(j, settle)
        gate_pre = jnp.dot(held[1, j], w_gate[...], preferred_element_type=jnp.float32)
        up_pre = jnp.dot(held[1, j], w_up[...], preferred_element_type=jnp.float32)
        act_grad = contract_cols(held[0, j], w_down[...])
        gate_clamped = jnp.minimum(gate_pre, CLAMP_LIMIT)
        up_clamped = jnp.clip(up_pre, -CLAMP_LIMIT, CLAMP_LIMIT)
        sigma = jax.nn.sigmoid(SLOPE_ALPHA * gate_clamped)
        gated = gate_clamped * sigma
        act[j] = ((up_clamped + 1.0) * gated).astype(kind)
        inside = (up_pre > -CLAMP_LIMIT) & (up_pre < CLAMP_LIMIT)
        up_g = jnp.where(inside, act_grad * gated, 0.0).astype(kind)
        slope = sigma + SLOPE_ALPHA * gate_clamped * sigma * (1.0 - sigma)
        gate_g = jnp.where(
            gate_pre < CLAMP_LIMIT, act_grad * (up_clamped + 1.0) * slope, 0.0
        ).astype(kind)
        gate_pg[j] = gate_g
        up_pg[j] = up_g
        for q in range(model_width // width):
            mine = pl.ds(q * width, width)
            value = contract_cols(gate_g, w_gate[mine, :]) + contract_cols(up_g, w_up[mine, :])
            part[j, :, mine] = value.astype(kind)
        for_diag(j).start()
        for_near(j).start()

    def add_pair(j):
        for_diag(j).wait_recv()
        mine = part[j, :, lanes(far)].astype(jnp.float32)
        pair[j] = (mine + near_in[1, j].astype(jnp.float32)).astype(kind)
        pair_copy(j).start()

    def whole(j):
        for_near(j).wait_recv()
        pair_copy(j).wait_recv()
        mine = part[j, :, lanes(t)].astype(jnp.float32)
        summed = mine + near_in[0, j].astype(jnp.float32)
        return (summed + far_in[j].astype(jnp.float32)).astype(kind)

    def send_back(j):
        @pl.when(j == s)
        def _():
            ret[s] = whole(j)

        @pl.when(j != s)
        def _():
            total[j] = whole(j)
            back(j).start()

    def forward(j):
        def run():
            for a in both:
                far_copy(a, j).wait_recv()
                fwd_copy(a, j).start()

        unless_own(j, run)

    def flat(value):
        return value.reshape(-1, value.shape[-1])

    def row_grads(k):
        cols = pl.ds(pl.multiple_of(k * 256, 256), 256)
        left = flat(held[1, :, :, cols])
        gate_grad[cols, :] = contract_rows(left, flat(gate_pg[...])).astype(kind)
        up_grad[cols, :] = contract_rows(left, flat(up_pg[...])).astype(kind)

    def act_grads(k):
        cols = pl.ds(pl.multiple_of(k * 512, 512), 512)
        down_grad[:, cols] = contract_rows(flat(act[...]), flat(held[0, :, :, cols])).astype(kind)

    for move in moves:
        move.start()
    meet(steps, True, near, far)
    moves[0].wait()

    def start_own(a):
        src = sources[a]
        for up in both:

            @pl.when(next_is_inner(up))
            def _():
                line_copy(a, z, src.at[:, lanes(t)], up).start()

    def end_own(a):
        for up in both:

            @pl.when(next_is_end(up))
            def _():
                to_end(a, z, sources[a][:, lanes(t)], up)

    start_own(0)
    moves[1].wait()
    moves[2].wait()
    info[pl.ds(0, 2), :] = routes[...].astype(jnp.float32)
    info[pl.ds(2, 2), :] = route_weights[...]
    infos[z] = info[...]
    looped(1, line, lambda dz: info_copy(dz).start())
    row_ids = lax.broadcasted_iota(jnp.int32, (tok_rows, tok_rows), 0)
    col_ids = lax.broadcasted_iota(jnp.int32, (tok_rows, tok_rows), 1)
    before[...] = jnp.where(row_ids < col_ids, 1.0, 0.0).astype(kind)
    table(z)
    end_own(0)
    for move in moves[3:5]:
        move.wait()
    gain = norm_gain[...]

    def normalise(k):
        here = pl.ds(pl.multiple_of(k * 32, 32), 32)
        x = resid[here, :].astype(jnp.float32)
        scale = lax.rsqrt(jnp.mean(x * x, axis=-1, keepdims=True) + 1e-06)
        normed[here, :] = (x * scale * gain).astype(kind)

    looped(0, tok_rows // 32, normalise)
    start_own(1)
    end_own(1)
    for a in both:
        cross[a, z] = selected(a, z, across, sources[a][:, lanes(t)])
        across_copy(a, z).start()
        cross_far[a] = selected(a, z, across, sources[a][:, lanes(far)])
        across_far(a).start()

    def own_chunk(q):
        for a in both:
            held[a, s, :, lanes(q)] = selected(a, z, s, sources[a][:, lanes(q)])

    looped(0, model_width // width, own_chunk)
    for move in moves[5:7]:
        move.wait()
    summed = conv_sum[...].astype(jnp.float32)
    centre = summed - jnp.mean(summed, axis=-1, keepdims=True)
    inv_std = lax.rsqrt(jnp.mean(centre * centre, axis=-1, keepdims=True) + 1e-05)
    pre_act = centre * inv_std * conv_gain[...]
    conv_out = (pre_act * jax.nn.sigmoid(pre_act)).astype(kind)
    side[...] = conv_out
    side_out[0] = conv_out

    def own_picks(e):
        picks[e] = jnp.where(pick(z, e), 1.0, 0.0).astype(kind)

    looped(0, steps, own_picks)
    for move in moves[7:]:
        move.wait()

    codes = line_schedule(line)
    middle = steps // 2

    def slot_code(n):
        code = 0
        for zz in range(line):
            for nn in range(steps):
                code = code + jnp.where((z == zz) & (n == nn), codes[zz][nn], 0)
        return code

    def chunk_at(n):
        code = slot_code(n)
        other = (code // 16) % 2
        return 2 * (code % 16) + y + other * (1 - 2 * y)

    def slot(n):
        code = slot_code(n)
        zb, other = code % 16, (code // 16) % 2
        first, second = (code // 32) % 16, (code // 512) % 16
        meeting = code // 8192
        j = 2 * zb + y + other * (1 - 2 * y)

        @pl.when(meeting > 0)
        def _():
            met = 2 * (meeting - 1) + 1 - y
            for a in both:
                arrival(a, met).wait_recv()
                share(a, met)

        @pl.when(first > 0)
        def _():
            for up in both:
                read_info(first, up)
            for up in both:
                handle(0, first, up)

        @pl.when(second > 0)
        def _():
            for up in both:
                handle(1, second, up)

        @pl.when(n == 1)
        def _():
            for a in both:
                arrival(a, j).wait_recv()
                near_copy(a, j).start()

        @pl.when(n == steps - 2)
        def _():
            looped(1, steps, lambda d: side_copy(d).start())

        forward(j)

        @pl.when(n >= 1)
        def _():
            experts(chunk_at(n - 1))

        @pl.when(n == 1)
        def _():
            add_pair(chunk_at(0))

        @pl.when(n > middle + 1)
        def _():
            add_pair(chunk_at(n - 2))

    def pair_at(n):
        add_pair(chunk_at(n))

    def back_at(n):
        send_back(chunk_at(n))

    looped(0, steps, slot)
    half = model_width // 512
    experts(chunk_at(steps - 1))
    add_pair(chunk_at(steps - 2))
    pair_at(steps - 1)
    looped(1, middle, pair_at)
    looped(middle, steps - 2, back_at)
    looped(0, half // 2, row_grads)
    back_at(steps - 2)
    looped(half // 2, half, row_grads)
    back_at(steps - 1)
    looped(half, half + half // 2, row_grads)
    looped(1, middle, back_at)
    looped(half + half // 2, 2 * half, row_grads)
    looped(0, half, act_grads)
    back_at(0)

    def gather_back(d):
        back_from((s + d) % steps).wait_recv()

    looped(1, steps, gather_back)
    part_grad[...] = contract_rows(flat(picks[...]), flat(ret[...])).astype(kind)

    def finish(j):
        for_near(j).wait_send()
        for_diag(j).wait_send()
        pair_copy(j).wait_send()

        @pl.when(j != s)
        def _():
            back(j).wait_send()
            for a in both:
                near_copy(a, j).wait_send()
                fwd_copy(a, j).wait_send()

        @pl.when(j // 2 != z)
        def _():
            for a in both:
                far_copy(a, j).wait_send()

    def finish_side(d):
        side_copy(d).wait_send()

    def finish_line(m):
        for up in both:
            zb = block_at(m, up)

            @pl.when(valid(m, up) & next_is_inner(up))
            def _():
                for a in both:
                    line_copy(a, zb, tok.at[a, zb], up).wait_send()

            @pl.when(valid(m, up) & next_is_end(up))
            def _():
                for a in both:
                    for col in both:
                        end_copy(a, zb, col, up).wait_send()

    def finish_across(zb):
        for a in both:
            across_copy(a, zb).wait_send()

    def meanwhile():
        looped(1, steps, lambda d: side_copy(d).wait_recv())
        looped(0, steps, finish)
        looped(1, steps, finish_side)
        looped(1, line, lambda dz: info_copy(dz).wait_send())
        looped(0, line, finish_line)
        looped(0, line, finish_across)
        for a in both:
            across_far(a).wait_send()

    settle_body(
        steps, meanwhile, part_grad, grad_out, resid, norm_gain, proj_weight,
        conv_sum, conv_gain, conv_taps, conv_value, conv_gate,
        side_out, feature_cols, proj, value_grad, gate_input_grad,
        full, grads, extended, *settle_sems,
    )


def relay_experts(operands, collective_id):
    routes, resid, w_gate, conv_sum = operands[0], operands[3], operands[5], operands[8]
    steps, tp_count = lax.axis_size("sp"), lax.axis_size("tp")
    line = steps // 2
    tok_rows, model_width = resid.shape
    count = 3 * tok_rows // steps
    width = model_width // tp_count
    hidden = w_gate.shape[1]
    kind = resid.dtype
    block = (steps, count, width)
    channels = conv_sum.shape[1]
    tail_rows = conv_sum.shape[0] + operands[11].shape[0] + 1
    outs = [
        jax.ShapeDtypeStruct((model_width, hidden), kind),
        jax.ShapeDtypeStruct((model_width, hidden), kind),
        jax.ShapeDtypeStruct((hidden, model_width), kind),
        jax.ShapeDtypeStruct((model_width // steps, channels), jnp.float32),
        jax.ShapeDtypeStruct((tok_rows, channels), kind),
        jax.ShapeDtypeStruct((tok_rows, channels), kind),
    ]
    held = pl.BlockSpec(memory_space=pltpu.VMEM)
    outside = pl.BlockSpec(memory_space=pltpu.HBM)

    def sems(*shape):
        return pltpu.SemaphoreType.DMA(shape)

    return pl.pallas_call(
        functools.partial(relay_kernel, steps),
        out_shape=tuple(outs),
        in_specs=[outside] * len(operands),
        out_specs=tuple(held for _ in outs),
        scratch_shapes=[pltpu.VMEM(x.shape, x.dtype) for x in operands]
        + [
            pltpu.VMEM((tok_rows, width), kind),
            pltpu.VMEM((steps,) + conv_sum.shape, kind),
            pltpu.VMEM((steps, tp_count, tok_rows // tp_count, model_width // steps), kind),
            pltpu.VMEM((tok_rows, model_width), kind),
            pltpu.VMEM((tok_rows, model_width), kind),
            pltpu.VMEM((tail_rows, channels), jnp.float32),
            pltpu.VMEM((tok_rows, model_width), kind),
            pltpu.VMEM((2 * routes.shape[0], tok_rows), jnp.float32),
            pltpu.VMEM((line, 2 * routes.shape[0], tok_rows), jnp.float32),
            pltpu.VMEM((line, steps, tok_rows), jnp.float32),
            pltpu.VMEM((line, steps, tok_rows), jnp.float32),
            pltpu.VMEM((tok_rows, tok_rows), kind),
            pltpu.VMEM((steps, count, tok_rows), kind),
            pltpu.VMEM((2, line, tok_rows, width), kind),
            pltpu.VMEM((2, line, 2, count, width), kind),
            pltpu.VMEM((2, line, count, width), kind),
            pltpu.VMEM((2, count, width), kind),
            pltpu.VMEM((2, steps, count, model_width), kind),
        ]
        + [pltpu.VMEM((steps, count, hidden), kind)] * 3
        + [pltpu.VMEM((steps, count, model_width), kind), pltpu.VMEM((2,) + block, kind)]
        + [pltpu.VMEM(block, kind)] * 4
        + [pltpu.VMEM(conv_sum.shape, kind)]
        + [sems(len(operands)), sems(line), sems(line), sems(2, 2, line), sems(2, line), sems(2, 2, line)]
        + [sems(2, line), sems(2, line), sems(2), sems(2, steps)]
        + [sems(2, steps)] * 6
        + [sems(steps)] * 10
        + [sems(tp_count)] * 6
        + [sems(1)]
        + [sems(steps)] * 8
        + [sems(1)] * 2,
        compiler_params=pltpu.CompilerParams(
            collective_id=collective_id, has_side_effects=True, vmem_limit_bytes=42 << 20
        ),
    )(*(pltpu.with_memory_space_constraint(x, pltpu.HBM) for x in operands))


def last_kernel(count, *refs):
    ins, outs, sem = refs[:count], refs[count:-1], refs[-1]
    moves = [pltpu.make_async_copy(a, b, sem.at[i]) for i, (a, b) in enumerate(zip(ins, outs))]
    for move in moves:
        move.start()
    for move in moves:
        move.wait()


def last_stage(results):
    return pl.pallas_call(
        functools.partial(last_kernel, len(results)),
        out_shape=tuple(jax.ShapeDtypeStruct(x.shape, x.dtype) for x in results),
        in_specs=[pl.BlockSpec(memory_space=pltpu.VMEM)] * len(results),
        out_specs=tuple(pl.BlockSpec(memory_space=pl.ANY) for _ in results),
        scratch_shapes=[pltpu.SemaphoreType.DMA((len(results),))],
        compiler_params=pltpu.CompilerParams(vmem_limit_bytes=16 << 20),
    )(*results)


def local(
    grad_out,
    resid,
    norm_gain,
    routes,
    route_weights,
    gate_weight,
    up_weight,
    down_weight,
    proj_weight,
    conv_sum,
    conv_gain,
    conv_taps,
    conv_value,
    conv_gate,
):
    tok_rows, model_width = resid.shape
    sp_count = lax.axis_size("sp")
    tp_count = lax.axis_size("tp")
    capacity = 3 * tok_rows // sp_count
    col_count = model_width // tp_count
    channels = conv_sum.shape[1]
    aligned = capacity % 16 == 0 and model_width % (128 * sp_count) == 0 and channels == GROUP
    if aligned and sp_count % 4 == 0:
        operands = (
            routes.T,
            route_weights.T,
            grad_out,
            resid,
            norm_gain[None],
            gate_weight[0],
            up_weight[0],
            down_weight[0],
            conv_sum,
            conv_gain[None],
            proj_weight,
            conv_taps,
            conv_value,
            conv_gate,
        )
        gate_grad, up_grad, down_grad, *rest = last_stage(relay_experts(operands, 4))
        return (gate_grad[None], up_grad[None], down_grad[None], *rest)
    resid_f = resid.astype(jnp.float32)
    inv_rms = lax.rsqrt(jnp.mean(resid_f * resid_f, axis=-1, keepdims=True) + 1e-06)
    normed = (resid_f * inv_rms * norm_gain).astype(jnp.bfloat16)
    my_sp = lax.axis_index("sp")
    away = (routes - my_sp) % sp_count
    steps_away = jnp.arange(sp_count, dtype=jnp.int32)
    named = away[:, :, None] == steps_away[None, None, :]
    chosen = jnp.any(named, axis=1)
    weight_of = jnp.sum(jnp.where(named, route_weights[:, :, None], 0.0), axis=1)
    token_ids = jnp.arange(tok_rows, dtype=jnp.int32)
    earlier = (token_ids[None, :] < token_ids[:, None]).astype(jnp.bfloat16)
    rank = jnp.dot(earlier, chosen.astype(jnp.bfloat16), preferred_element_type=jnp.float32)
    rank = jnp.where(chosen, rank, -1.0).astype(jnp.int32)
    slots = jnp.arange(capacity, dtype=jnp.int32)
    held = rank.T[:, None, :] == slots[None, :, None]
    slot_weight = jnp.sum(jnp.where(held, weight_of.T[:, None, :], 0.0), axis=2)
    pick = held.astype(jnp.bfloat16).reshape(sp_count * capacity, tok_rows)
    first_col = lax.axis_index("tp") * col_count
    normed_part = lax.dynamic_slice_in_dim(normed, first_col, col_count, 1)
    cots_part = lax.dynamic_slice_in_dim(grad_out, first_col, col_count, 1)
    slot_weight = slot_weight.reshape(-1, 1)
    send_rows = jnp.dot(pick, normed_part, preferred_element_type=jnp.float32).astype(jnp.bfloat16)
    send_cots = jnp.dot(pick, cots_part, preferred_element_type=jnp.float32)
    send_cots = (send_cots * slot_weight).astype(jnp.bfloat16)
    own_pick = pick[:capacity]
    own_rows = jnp.dot(own_pick, normed, preferred_element_type=jnp.float32).astype(jnp.bfloat16)
    own_cots = jnp.dot(own_pick, grad_out, preferred_element_type=jnp.float32)
    own_cots = (own_cots * slot_weight[:capacity]).astype(jnp.bfloat16)
    summed = conv_sum.astype(jnp.float32).reshape(tok_rows, channels // GROUP, GROUP)
    centre = summed - jnp.mean(summed, axis=-1, keepdims=True)
    inv_std = lax.rsqrt(jnp.mean(centre * centre, axis=-1, keepdims=True) + 1e-05)
    grouped = centre * inv_std
    chan_normed = grouped.reshape(tok_rows, channels)
    pre_act = chan_normed * conv_gain
    sigma_conv = jax.nn.sigmoid(pre_act)
    conv_out = (pre_act * sigma_conv).astype(jnp.bfloat16)
    routed_rows, routed_cots = spread(
        (
            send_rows.reshape(sp_count, capacity, col_count),
            send_cots.reshape(sp_count, capacity, col_count),
        ),
        (own_rows, own_cots),
        None,
        True,
        False,
        0,
    )
    routed_rows = routed_rows.reshape(sp_count * capacity, model_width)
    routed_cots = routed_cots.reshape(sp_count * capacity, model_width)
    gate_grad, up_grad, down_grad, partial_value = expert_backward(
        routed_rows, routed_cots, gate_weight[0], up_weight[0], down_weight[0]
    )
    returned = combine(
        partial_value.reshape(sp_count, capacity, model_width).astype(jnp.bfloat16), 1
    ).reshape(sp_count * capacity, col_count)
    normed_part_grad = contract_rows(pick, returned).astype(jnp.bfloat16)
    chunks = 4
    normed_grad, all_out = spread(
        (normed_part_grad.reshape(chunks, tok_rows // chunks, col_count),),
        None,
        conv_out,
        True,
        False,
        2,
    )
    normed_grad = normed_grad.reshape(tok_rows, model_width)
    feature_grad = normed_grad.astype(jnp.float32) * norm_gain
    cubed = inv_rms * inv_rms * inv_rms
    resid_grad = (
        grad_out.astype(jnp.float32)
        + inv_rms * feature_grad
        - resid_f * cubed * jnp.mean(resid_f * feature_grad, axis=-1, keepdims=True)
    ).astype(jnp.bfloat16)
    share = tok_rows // tp_count
    feat_rows = model_width // sp_count
    tokens_part = lax.dynamic_slice_in_dim(resid_grad, lax.axis_index("tp") * share, share, 0)
    by_feature = tokens_part.reshape(share, sp_count, feat_rows).transpose(1, 0, 2)
    own_features = lax.dynamic_slice_in_dim(resid_grad, my_sp * feat_rows, feat_rows, 1)
    (feature_cols,) = spread(
        (by_feature,), (own_features.reshape(tp_count, share, feat_rows),), None, False, True, 3
    )
    proj_grad = contract_rows(
        feature_cols.reshape(sp_count * tok_rows, feat_rows),
        all_out.reshape(sp_count * tok_rows, channels),
    )
    out_grad = jnp.dot(resid_grad, proj_weight, preferred_element_type=jnp.float32)
    normal_grad = (
        out_grad * sigma_conv * (1.0 + pre_act * (1.0 - sigma_conv)) * conv_gain
    ).reshape(tok_rows, channels // GROUP, GROUP)
    sum_grad = inv_std * (
        normal_grad
        - jnp.mean(normal_grad, axis=-1, keepdims=True)
        - grouped * jnp.mean(normal_grad * grouped, axis=-1, keepdims=True)
    )
    sum_grad = sum_grad.reshape(tok_rows, channels)
    following = passed_along(sum_grad[: CONV_K - 1], "sp", -1)
    extended = jnp.concatenate([sum_grad, following], axis=0)
    gated_grad = lax.conv_general_dilated(
        extended[None],
        conv_taps[::-1][:, None, :],
        (1,),
        ((0, 0),),
        dimension_numbers=("NWC", "WIO", "NWC"),
        feature_group_count=channels,
        precision=lax.Precision.HIGHEST,
    )[0]
    sigma_gate = jax.nn.sigmoid(conv_gate.astype(jnp.float32))
    value_grad = (gated_grad * sigma_gate).astype(jnp.bfloat16)
    gate_input_grad = (
        gated_grad * conv_value.astype(jnp.float32) * sigma_gate * (1.0 - sigma_gate)
    ).astype(jnp.bfloat16)
    return (gate_grad[None], up_grad[None], down_grad[None], proj_grad, value_grad, gate_input_grad)


def solution(mesh):
    in_specs = (
        P("sp", None),
        P("sp", None),
        P(),
        P("sp", None),
        P("sp", None),
        P("sp", None, "tp"),
        P("sp", None, "tp"),
        P("sp", "tp", None),
        P(None, "tp"),
        P("sp", "tp"),
        P("tp"),
        P(None, "tp"),
        P("sp", "tp"),
        P("sp", "tp"),
    )
    out_specs = (
        P("sp", None, "tp"),
        P("sp", None, "tp"),
        P("sp", "tp", None),
        P("sp", "tp"),
        P("sp", "tp"),
        P("sp", "tp"),
    )
    return jax.shard_map(local, mesh=mesh, in_specs=in_specs, out_specs=out_specs, check_vma=False)
```
